32 devices in a mesh: sp: 4 (over z), fs: 2 (over y), tp: 4 (over x, core).
Axes of the slice: x: 2, y: 2, z: 4, core: 2. Of those that a mesh axis runs over, the one named last changes fastest.
Arguments:
- tokens: bfloat16 [2, 3072, 2304], P('fs', 'sp'), may hold values from -6 to 6
- norm_gain: float32 [2304], replicated, may hold values from 0.1 to 1.9
- query_weight: bfloat16 [2304, 2048], P(('sp', 'fs'), 'tp'), may hold values from -6 to 6
- key_weight: bfloat16 [2304, 512], P(('sp', 'fs'), 'tp'), may hold values from -6 to 6
- value_weight: bfloat16 [2304, 512], P(('sp', 'fs'), 'tp'), may hold values from -0.125 to 0.125
- outer_weight: bfloat16 [2304, 2048], P(('sp', 'fs'), 'tp'), may hold values from -0.125 to 0.125
- inner_weight: bfloat16 [2304, 2048], P(('sp', 'fs'), 'tp'), may hold values from -0.125 to 0.125
- signal_weight: bfloat16 [2304, 2048], P(('sp', 'fs'), 'tp'), may hold values from -0.125 to 0.125
- conv_taps: float32 [3, 2048], P(None, 'tp'), may hold values from -3 to 3
- sink_logit: float32 [32], P('tp'), may hold values from -4 to 4
Outputs:
- attn_out: bfloat16 [2, 3072, 2048], P('fs', 'sp', 'tp')
- conv_out: bfloat16 [2, 3072, 2048], P('fs', 'sp', 'tp')
- log_total: float32 [2, 32, 3072], P('fs', 'tp', 'sp')
The draws below stay inside these ranges and needn't reach their ends.
All inputs are finite; a program needn't handle non-finite values.
Results may differ from the reference program's by a relative error of at most 0.014.
The reference program's roundings to bfloat16 on the way (of `normed`, `product` and `rounded`) count: a program that leaves them out, or rounds other values in their place, can miss the bound.
Values may be sent and summed in bfloat16 or wider, within the bound.
A program may use at most 64 MiB of HBM per device.

```python
import math
import jax
import jax.numpy as jnp
from jax import lax

D = 2304
HEAD = 64
QHEADS = 32
KVHEADS = 8
CHANNELS = 2048
WINDOW = 128
SEQS = 2
LEN = 3072


def draw_tokens(key, part):
    base = jax.random.normal(jax.random.fold_in(key, 3), (SEQS, LEN, D), jnp.float32)
    return jnp.clip(base, -6.0, 6.0).astype(jnp.bfloat16)


def projection_pair(key):
    scaling = 1.0 / math.sqrt(D)
    query_base = jax.random.normal(jax.random.fold_in(key, 21), (D, QHEADS * HEAD), jnp.float32) * scaling
    key_base = jax.random.normal(jax.random.fold_in(key, 22), (D, KVHEADS * HEAD), jnp.float32) * scaling
    return (jnp.clip(query_base, -6.0, 6.0), jnp.clip(key_base, -6.0, 6.0))


def draw_query_weight(key, part):
    return projection_pair(key)[0].astype(jnp.bfloat16)


def draw_key_weight(key, part):
    return projection_pair(key)[1].astype(jnp.bfloat16)


def block_scale(own_key, shape, shards, smallest, top_value):
    gain, own = 1.0, jax.random.fold_in(own_key, 6)
    for position, blocks in shards:
        draws = jnp.exp(jax.random.uniform(jax.random.fold_in(own, position), (blocks,), jnp.float32, smallest / len(shards), top_value / len(shards)))
        gain = gain * jnp.repeat(draws, shape[position] // blocks).reshape([-1 if axis == position else 1 for axis in range(len(shape))])
    return gain


def normal_values(own_key, dims, scale, reach, cuts=(), held_as=jnp.bfloat16):
    drawn = scale * jax.random.normal(own_key, dims, jnp.float32)
    if cuts:
        drawn = drawn * block_scale(own_key, dims, cuts, -0.22, 0.18)
    return jnp.clip(drawn, -reach, reach).astype(held_as)


def setup_inputs(seed: int = 0) -> dict:
    splits = jax.random.split(jax.random.key(seed), 11)
    return {
        "tokens": draw_tokens(jax.random.fold_in(splits[10], 71), 0),
        "norm_gain": jnp.clip(1.0 + 0.18 * jax.random.normal(splits[1], (D,), jnp.float32), 0.1, 1.9),
        "query_weight": draw_query_weight(jax.random.fold_in(splits[10], 71), 0),
        "key_weight": draw_key_weight(jax.random.fold_in(splits[10], 71), 0),
        "value_weight": normal_values(splits[4], (D, KVHEADS * HEAD), D ** -0.5, 0.125, ((0, 8), (1, 4))),
        "outer_weight": normal_values(splits[5], (D, CHANNELS), D ** -0.5, 0.125, ((0, 8), (1, 4))),
        "inner_weight": normal_values(splits[6], (D, CHANNELS), D ** -0.5, 0.125, ((0, 8), (1, 4))),
        "signal_weight": normal_values(splits[7], (D, CHANNELS), D ** -0.5, 0.125, ((0, 8), (1, 4))),
        "conv_taps": normal_values(splits[8], (3, CHANNELS), 0.6, 3.0, ((1, 4),), jnp.float32),
        "sink_logit": normal_values(splits[9], (QHEADS,), 1.5, 4.0, ((0, 4),), jnp.float32),
    }


EPSILON = 1e-06

def normalized(tokens, norm_gain):
    values = tokens.astype(jnp.float32)
    scaling = lax.rsqrt(lax.optimization_barrier(jnp.mean(values * values, axis=-1, keepdims=True)) + EPSILON)
    return (values * scaling * norm_gain).astype(jnp.bfloat16)

def banded_attention(queries, key_proj, value_proj, sink_logit):
    seq_length = queries.shape[0]
    group_size = QHEADS // KVHEADS
    block_count = seq_length // WINDOW
    query_blocks = queries.astype(jnp.float32).reshape(block_count, WINDOW, KVHEADS, group_size, HEAD)
    key_rows = jnp.pad(key_proj.astype(jnp.float32), ((WINDOW, WINDOW), (0, 0))).reshape(block_count + 2, WINDOW, KVHEADS, HEAD)
    value_rows = jnp.pad(value_proj.astype(jnp.float32), ((WINDOW, WINDOW), (0, 0))).reshape(block_count + 2, WINDOW, KVHEADS, HEAD)
    key_span = jnp.concatenate([key_rows[:-2], key_rows[1:-1], key_rows[2:]], axis=1)
    value_span = jnp.concatenate([value_rows[:-2], value_rows[1:-1], value_rows[2:]], axis=1)
    scores = jnp.einsum('bqkgd,bskd->bkgqs', query_blocks, key_span) * (1.0 / math.sqrt(HEAD))
    distance = jnp.arange(WINDOW)[:, None] - jnp.arange(3 * WINDOW)[None, :] + WINDOW
    key_pos = WINDOW * jnp.arange(block_count)[:, None] - WINDOW + jnp.arange(3 * WINDOW)[None, :]
    inside = (jnp.abs(distance)[None] <= WINDOW) & ((key_pos >= 0) & (key_pos < seq_length))[:, None, :]
    slopes = jnp.exp2(-8.0 * jnp.arange(1, QHEADS + 1, dtype=jnp.float32) / QHEADS)
    scores = scores - slopes.reshape(KVHEADS, group_size, 1, 1) * jnp.abs(distance).astype(jnp.float32)
    scores = jnp.where(inside[:, None, None], scores, -jnp.inf)
    sink_grid = sink_logit.reshape(KVHEADS, group_size, 1, 1)
    row_peak = jnp.maximum(lax.optimization_barrier(jnp.max(scores, axis=-1, keepdims=True)), sink_grid)
    weights = jnp.exp(scores - row_peak)
    row_total = lax.optimization_barrier(jnp.sum(weights, axis=-1, keepdims=True)) + jnp.exp(sink_grid - row_peak)
    rounded = lax.optimization_barrier(weights.astype(jnp.bfloat16)).astype(jnp.float32)
    weighted = jnp.einsum('bkgqs,bskd->bqkgd', rounded, value_span)
    attended = (weighted / row_total.transpose(0, 3, 1, 2, 4)).astype(jnp.bfloat16).reshape(seq_length, QHEADS * HEAD)
    log_total = (row_peak + jnp.log(row_total))[..., 0].transpose(1, 2, 0, 3).reshape(QHEADS, seq_length)
    return (attended, log_total)

def reference(tokens, norm_gain, query_weight, key_weight, value_weight, outer_weight, inner_weight, signal_weight, conv_taps, sink_logit):

    def one_sequence(rows_in):
        normed = normalized(rows_in, norm_gain)

        def project(weight):
            return jnp.dot(normed, weight, preferred_element_type=jnp.float32).astype(jnp.bfloat16)
        queries = project(query_weight)
        key_proj = project(key_weight)
        value_proj = project(value_weight)
        outer_gate = project(outer_weight)
        inner_gate = project(inner_weight)
        signal = project(signal_weight)
        product = (inner_gate.astype(jnp.float32) * signal.astype(jnp.float32)).astype(jnp.bfloat16)
        padded = jnp.pad(product, ((1, 1), (0, 0))).astype(jnp.float32)
        mixed_conv = conv_taps[0] * padded[:-2] + conv_taps[1] * padded[1:-1] + conv_taps[2] * padded[2:]
        conv_out = (outer_gate.astype(jnp.float32) * mixed_conv).astype(jnp.bfloat16)
        attended, log_total = banded_attention(queries, key_proj, value_proj, sink_logit)
        return (attended, conv_out, log_total)
    attn_out, conv_out, log_total = lax.map(one_sequence, tokens)
    return (attn_out, conv_out, log_total)
```

```python
import math

import functools

import jax
import jax.numpy as jnp
from jax import lax
from jax.experimental import pallas as pl
from jax.experimental.pallas import tpu as pltpu
from jax.sharding import PartitionSpec as P

HEAD = 64
WINDOW = 128


EPSILON = 1e-06


def extended(value, sides, width):
    for axis, dim in sides:
        size, length = (lax.axis_size(axis), value.shape[dim])
        up = [(i, (i + 1) % size) for i in range(size - 1)]
        down = [(j, i) for i, j in up]
        last = lax.slice_in_dim(value, length - width, length, axis=dim)
        initial = lax.slice_in_dim(value, 0, width, axis=dim)
        before = lax.ppermute(last, axis, up)
        after = lax.ppermute(initial, axis, down)
        value = jnp.concatenate([before, value, after], axis=dim)
    return value


def normalized(tokens, norm_gain):
    values = tokens.astype(jnp.float32)
    scaling = lax.rsqrt(jnp.mean(values * values, axis=-1, keepdims=True) + EPSILON)
    return (values * scaling * norm_gain).astype(jnp.bfloat16)


def folding(normed):

    def add_portions(running, portions, offset):
        return tuple(
            (jnp.dot(normed, portion, preferred_element_type=jnp.float32) for portion in portions)
        )

    return add_portions


def empty_sums(normed, weights):
    return tuple((jnp.zeros((normed.shape[0], weight.shape[1]), jnp.float32) for weight in weights))


def rounded(results):
    return tuple((result.astype(jnp.bfloat16) for result in results))


def gate_product(inner_gate, signal):
    return (inner_gate.astype(jnp.float32) * signal.astype(jnp.float32)).astype(jnp.bfloat16)


def send_edges(key_proj, value_proj, product):
    stacked = jnp.concatenate([key_proj, value_proj], axis=1)
    window_rows = extended(stacked, (("sp", 0),), WINDOW)
    conv_rows = extended(product, (("sp", 0),), 1)
    return (window_rows, conv_rows)


def banded_attention(queries, window_rows, sink_logit, slopes, first_pos, seq_length):
    tok_count = queries.shape[0]
    kv_cols = window_rows.shape[1] // 2
    kv_heads = kv_cols // HEAD
    group_size = queries.shape[1] // (HEAD * kv_heads)
    block_count = tok_count // WINDOW
    query_blocks = queries.reshape(block_count, WINDOW, kv_heads, group_size, HEAD)
    key_rows = window_rows[:, :kv_cols].reshape(block_count + 2, WINDOW, kv_heads, HEAD)
    value_rows = window_rows[:, kv_cols:].reshape(block_count + 2, WINDOW, kv_heads, HEAD)
    key_span = jnp.concatenate([key_rows[:-2], key_rows[1:-1], key_rows[2:]], axis=1)
    value_span = jnp.concatenate([value_rows[:-2], value_rows[1:-1], value_rows[2:]], axis=1)
    scores = jnp.einsum(
        "bqkgd,bskd->bkgqs", query_blocks, key_span, preferred_element_type=jnp.float32
    ) * (1.0 / math.sqrt(HEAD))
    distance = jnp.arange(WINDOW)[:, None] - jnp.arange(3 * WINDOW)[None, :] + WINDOW
    key_pos = (
        first_pos
        - WINDOW
        + WINDOW * jnp.arange(block_count)[:, None]
        + jnp.arange(3 * WINDOW)[None, :]
    )
    inside = (jnp.abs(distance)[None] <= WINDOW) & ((key_pos >= 0) & (key_pos < seq_length))[
        :, None, :
    ]
    scores = scores - slopes.reshape(kv_heads, group_size, 1, 1) * jnp.abs(distance).astype(
        jnp.float32
    )
    scores = jnp.where(inside[:, None, None], scores, -jnp.inf)
    sink_grid = sink_logit.reshape(kv_heads, group_size, 1, 1)
    row_peak = jnp.maximum(jnp.max(scores, axis=-1, keepdims=True), sink_grid)
    weights = jnp.exp(scores - row_peak)
    row_total = jnp.sum(weights, axis=-1, keepdims=True) + jnp.exp(sink_grid - row_peak)
    weighted = jnp.einsum(
        "bkgqs,bskd->bqkgd",
        weights.astype(jnp.bfloat16),
        value_span,
        preferred_element_type=jnp.float32,
    )
    attended = (
        (weighted / row_total.transpose(0, 3, 1, 2, 4))
        .astype(jnp.bfloat16)
        .reshape(tok_count, kv_heads * group_size * HEAD)
    )
    log_total = (
        (row_peak + jnp.log(row_total))[..., 0]
        .transpose(1, 2, 0, 3)
        .reshape(kv_heads * group_size, tok_count)
    )
    return (attended, log_total)


def per_device(
    tokens,
    norm_gain,
    query_weight,
    key_weight,
    value_weight,
    outer_weight,
    inner_weight,
    signal_weight,
    conv_taps,
    sink_logit,
):
    normed = normalized(tokens[0], norm_gain)
    add_portions = folding(normed)
    all_sums = add_portions(
        empty_sums(
            normed,
            (query_weight, key_weight, value_weight, outer_weight, inner_weight, signal_weight),
        ),
        (
            lax.all_gather(query_weight, ("sp", "fs"), axis=0, tiled=True),
            lax.all_gather(key_weight, ("sp", "fs"), axis=0, tiled=True),
            lax.all_gather(value_weight, ("sp", "fs"), axis=0, tiled=True),
            lax.all_gather(outer_weight, ("sp", "fs"), axis=0, tiled=True),
            lax.all_gather(inner_weight, ("sp", "fs"), axis=0, tiled=True),
            lax.all_gather(signal_weight, ("sp", "fs"), axis=0, tiled=True),
        ),
        jnp.int32(0),
    )
    queries, key_proj, value_proj, outer_gate, inner_gate, signal = rounded(all_sums)
    product = gate_product(inner_gate, signal)
    window_rows, conv_rows = send_edges(key_proj, value_proj, product)
    tok_count = normed.shape[0]
    head_local = queries.shape[1] // HEAD
    head_index = lax.axis_index("tp") * head_local + jnp.arange(1, head_local + 1)
    slopes = jnp.exp2(-8.0 * head_index.astype(jnp.float32) / (head_local * lax.axis_size("tp")))
    first_pos = lax.axis_index("sp") * tok_count
    attended, log_total = banded_attention(
        queries, window_rows, sink_logit, slopes, first_pos, tok_count * lax.axis_size("sp")
    )
    mixed_conv = conv_taps[0] * conv_rows[0:tok_count].astype(jnp.float32)
    mixed_conv = mixed_conv + conv_taps[1] * conv_rows[1 : tok_count + 1].astype(jnp.float32)
    mixed_conv = mixed_conv + conv_taps[2] * conv_rows[2 : tok_count + 2].astype(jnp.float32)
    conv_out = (outer_gate.astype(jnp.float32) * mixed_conv).astype(jnp.bfloat16)
    return (attended[None], conv_out[None], log_total[None])


MESH = pl.DeviceIdType.MESH
GROUPS = 3
FAR = -1e30


def mega_kernel(
    ns,
    tps,
    tokens,
    gain_in,
    qw,
    kw,
    vw,
    ow,
    iw,
    sw,
    taps_in,
    sinks_in,
    attn_out,
    conv_out,
    log_out,
    toks,
    wts,
    stage_w,
    qs,
    kvs,
    bias,
    prod,
    outer,
    attn_st,
    log_st,
    conv_st,
    kv_raw,
    gain_raw,
    gain,
    taps,
    sinks,
    small_sem,
    load_sem,
    stage_sem,
    misc_sem,
    y_send,
    w_recv,
    up_send,
    dn_send,
    tok_send,
    tok_recv,
    kv_send,
    kv_recv,
    pr_send,
    pr_recv,
    ret_send,
    ret_recv,
):
    s, f, t = lax.axis_index("sp"), lax.axis_index("fs"), lax.axis_index("tp")
    other = 1 - f
    core = lax.rem(t, 2)
    mate = t + 1 - 2 * core
    rows = tokens.shape[0]
    half_rows = rows // 2
    depth = qw.shape[0]
    qcols = qs.shape[2]
    heads = qcols // HEAD
    chans = prod.shape[3]
    blocks = rows // WINDOW
    pad = (prod.shape[2] - rows) // 2
    up, down, across, beside = (s + 1, f, t), (s - 1, f, t), (s, other, t), (s, f, mate)
    has_up, has_down = s < ns - 1, s > 0

    barrier = pltpu.get_barrier_semaphore()

    @pl.when(has_up)
    def _():
        pl.semaphore_signal(barrier, inc=1, device_id=up, device_id_type=MESH)

    @pl.when(has_down)
    def _():
        pl.semaphore_signal(barrier, inc=1, device_id=down, device_id_type=MESH)

    pl.semaphore_signal(barrier, inc=1, device_id=across, device_id_type=MESH)
    pl.semaphore_signal(barrier, inc=1, device_id=beside, device_id_type=MESH)

    def block_rows(blk):
        return pl.ds(pl.multiple_of(blk * depth, 16), depth)

    def loads(g, half, dest, sems):
        if g == 0:
            qc = pl.ds(pl.multiple_of(half * qcols, 128), qcols)
            pairs = [(qw.at[:, qc], dest.at[:, pl.ds(0, qcols)])]
        else:
            c = pl.ds(pl.multiple_of(half * (2 * chans) + (g - 1) * chans, 128), chans)
            pairs = [
                (ref.at[:, c], dest.at[:, pl.ds(i * chans, chans)])
                for i, ref in enumerate((iw, sw, ow))
            ]
        return [
            pltpu.make_async_copy(a, b, sems.at[g, i]) for i, (a, b) in enumerate(pairs)
        ]

    mine = s * 2 + f
    theirs = s * 2 + other
    own_loads = [loads(g, f, wts.at[g, block_rows(mine)], load_sem) for g in range(GROUPS)]
    out_loads = [loads(g, other, stage_w.at[g], stage_sem) for g in range(GROUPS)]
    small = [
        pltpu.make_async_copy(a, b, small_sem.at[i])
        for i, (a, b) in enumerate(
            ((kw, kv_raw.at[0]), (vw, kv_raw.at[1]), (gain_in, gain_raw), (taps_in, taps), (sinks_in, sinks))
        )
    ]
    small[0].start()
    small[1].start()
    for g in range(GROUPS):
        for c in out_loads[g] + own_loads[g]:
            c.start()
    for c in small[2:]:
        c.start()
    tok_load = pltpu.make_async_copy(tokens, toks.at[f], misc_sem.at[0])
    tok_load.start()

    pl.semaphore_wait(
        barrier, 2 + jnp.where(has_up, 1, 0) + jnp.where(has_down, 1, 0)
    )

    small[0].wait()
    small[1].wait()
    keys0, vals0 = kv_raw[0], kv_raw[1]
    halves = [
        jnp.concatenate([w[:, i * HEAD : (i + 1) * HEAD] for w in (keys0, vals0)], axis=1)
        for i in range(2)
    ]
    first = f == 0
    stage_w[0, :, pl.ds(qcols, 2 * HEAD)] = jnp.where(first, halves[1], halves[0])
    wts[0, block_rows(mine), pl.ds(qcols, 2 * HEAD)] = jnp.where(first, halves[0], halves[1])

    y_copies = []
    for g in range(GROUPS):
        for c in out_loads[g]:
            c.wait()
        copy = pltpu.make_async_remote_copy(
            src_ref=stage_w.at[g],
            dst_ref=wts.at[g, block_rows(mine)],
            send_sem=y_send.at[g],
            recv_sem=w_recv.at[g, mine],
            device_id=across,
            device_id_type=MESH,
        )
        copy.start()
        y_copies.append(copy)
        for c in own_loads[g]:
            c.wait()
    share = pl.ds(pl.multiple_of(core * half_rows, 16), half_rows)
    rest = pl.ds(pl.multiple_of((1 - core) * half_rows, 16), half_rows)
    tok_copy = pltpu.make_async_remote_copy(
        src_ref=tokens.at[share],
        dst_ref=toks.at[f, share],
        send_sem=tok_send.at[0],
        recv_sem=tok_recv.at[0],
        device_id=across,
        device_id_type=MESH,
    )
    tok_copy.start()

    def incoming(g, blk):
        return pltpu.make_async_remote_copy(
            src_ref=wts.at[g, block_rows(blk)],
            dst_ref=wts.at[g, block_rows(blk)],
            send_sem=up_send.at[g, blk],
            recv_sem=w_recv.at[g, blk],
            device_id=across,
            device_id_type=MESH,
        )

    def forward(g, blk, upward):
        return pltpu.make_async_remote_copy(
            src_ref=wts.at[g, block_rows(blk)],
            dst_ref=wts.at[g, block_rows(blk)],
            send_sem=(up_send if upward else dn_send).at[g, blk],
            recv_sem=w_recv.at[g, blk],
            device_id=up if upward else down,
            device_id_type=MESH,
        )

    def relay_step(g, d, par):
        side = f if par == 0 else other
        if d == 0:
            blk = s * 2 + side
            if par == 1:
                incoming(g, blk).wait_recv()

            @pl.when(has_up)
            def _():
                forward(g, blk, True).start()

            @pl.when(has_down)
            def _():
                forward(g, blk, False).start()

            return

        @pl.when(s - d >= 0)
        def _():
            blk = (s - d) * 2 + side
            incoming(g, blk).wait_recv()

            @pl.when(has_up)
            def _():
                forward(g, blk, True).start()

        @pl.when(s + d < ns)
        def _():
            blk = (s + d) * 2 + side
            incoming(g, blk).wait_recv()

            @pl.when(has_down)
            def _():
                forward(g, blk, False).start()

    def settle():
        for g in range(GROUPS):
            y_copies[g].wait_send()
            for d in range(ns):
                for par in range(2):
                    side = f if par == 0 else other

                    @pl.when((s - d >= 0) & has_up)
                    def _():
                        forward(g, (s - d) * 2 + side, True).wait_send()

                    @pl.when((s + d < ns) & has_down)
                    def _():
                        forward(g, (s + d) * 2 + side, False).wait_send()

    def norm_rows(seq):
        @pl.loop(0, blocks)
        def _(b):
            at = pl.ds(pl.multiple_of(b * WINDOW, WINDOW), WINDOW)
            values = toks[seq, at, :].astype(jnp.float32)
            scaling = lax.rsqrt(jnp.mean(values * values, axis=-1, keepdims=True) + EPSILON)
            toks[seq, at, :] = (values * scaling * gain[...]).astype(jnp.bfloat16)

    mm_rows = rows // 2

    def make_bias():
        for c in small[2:]:
            c.wait()
        for i in range(gain_raw.shape[0]):
            gain[:, i * 128 : (i + 1) * 128] = gain_raw[i : i + 1, :]
        key = lax.broadcasted_iota(jnp.int32, (3 * WINDOW, WINDOW), 0)
        query = lax.broadcasted_iota(jnp.int32, (3 * WINDOW, WINDOW), 1)
        away = jnp.abs(query - key + WINDOW)
        for h in range(heads):
            index = (t * (2 * heads) + f * heads + h + 1).astype(jnp.float32)
            slope = jnp.exp2(jnp.full((1, WINDOW), -8.0 / (2 * heads * tps), jnp.float32) * index)
            bias[h] = jnp.where(away <= WINDOW, -slope * away.astype(jnp.float32), FAR)

    def project_qkv(seq):
        @pl.loop(0, 2)
        def _(b):
            at = pl.multiple_of(b * mm_rows, WINDOW)
            out = jnp.dot(
                toks[seq, pl.ds(at, mm_rows), :], wts[0], preferred_element_type=jnp.float32
            )
            qs[seq, pl.ds(at, mm_rows), :] = out[:, :qcols].astype(jnp.bfloat16)
            kvs[seq, pl.ds(at + WINDOW, mm_rows), :] = out[:, qcols:].astype(jnp.bfloat16)

    def edge_copies(buf, seq, width, sends, recvs, slot):
        length = buf.shape[1] if len(buf.shape) == 3 else buf.shape[2]
        ref = buf.at[seq] if len(buf.shape) == 3 else buf.at[slot // 2, seq]
        climb = pltpu.make_async_remote_copy(
            src_ref=ref.at[pl.ds(length - 2 * width, width)],
            dst_ref=ref.at[pl.ds(0, width)],
            send_sem=sends.at[slot, 0],
            recv_sem=recvs.at[slot, 0],
            device_id=up,
            device_id_type=MESH,
        )
        fall = pltpu.make_async_remote_copy(
            src_ref=ref.at[pl.ds(width, width)],
            dst_ref=ref.at[pl.ds(length - width, width)],
            send_sem=sends.at[slot, 1],
            recv_sem=recvs.at[slot, 1],
            device_id=down,
            device_id_type=MESH,
        )
        return ref, length, climb, fall

    def edges_start(buf, seq, width, sends, recvs, slot):
        ref, length, climb, fall = edge_copies(buf, seq, width, sends, recvs, slot)
        blank = jnp.zeros((width, ref.shape[1]), jnp.bfloat16)

        @pl.when(has_up)
        def _():
            climb.start()

        @pl.when(has_down)
        def _():
            fall.start()

        @pl.when(jnp.logical_not(has_up))
        def _():
            ref[pl.ds(length - width, width), :] = blank

        @pl.when(jnp.logical_not(has_down))
        def _():
            ref[pl.ds(0, width), :] = blank

    def edges_wait(buf, seq, width, sends, recvs, slot):
        _, _, climb, fall = edge_copies(buf, seq, width, sends, recvs, slot)

        @pl.when(has_up)
        def _():
            climb.wait_send()
            fall.wait_recv()

        @pl.when(has_down)
        def _():
            fall.wait_send()
            climb.wait_recv()

    def attend(seq, first, count):
        @pl.loop(first, first + count)
        def _(b):
            at = pl.multiple_of(b * WINDOW, WINDOW)
            kv = kvs[seq, pl.ds(at, 3 * WINDOW), :]
            keys = kv[:, :HEAD]
            values_t = kv.astype(jnp.float32).T[HEAD:, :].astype(jnp.bfloat16)
            queries = qs[seq, pl.ds(at, WINDOW), :]
            low = jnp.where((b == 0) & (s == 0), FAR, 0.0)
            high = jnp.where((b == blocks - 1) & (s == ns - 1), FAR, 0.0)
            outs = []
            for h in range(heads):
                query = queries[:, h * HEAD : (h + 1) * HEAD]
                scores = lax.dot_general(
                    keys, query, (((1,), (1,)), ((), ())), preferred_element_type=jnp.float32
                )
                scores = scores * (1.0 / math.sqrt(HEAD)) + bias[h]
                scores = jnp.concatenate(
                    [
                        scores[:WINDOW] + low,
                        scores[WINDOW : 2 * WINDOW],
                        scores[2 * WINDOW :] + high,
                    ],
                    axis=0,
                )
                sink = sinks[f * heads + h]
                peak = jnp.maximum(jnp.max(scores, axis=0, keepdims=True), sink)
                weights = jnp.exp(scores - peak)
                total = jnp.sum(weights, axis=0, keepdims=True) + jnp.exp(sink - peak)
                mixed = jnp.dot(
                    values_t, weights.astype(jnp.bfloat16), preferred_element_type=jnp.float32
                )
                outs.append(mixed / total)
                log_st[seq, pl.ds(h, 1), pl.ds(at, WINDOW)] = peak + jnp.log(total)
            stacked = jnp.concatenate(outs, axis=0)
            attn_st[seq, pl.ds(at, WINDOW), :] = stacked.T.astype(jnp.bfloat16)

    half_cols = pl.ds(pl.multiple_of(f * qcols, 128), qcols)

    def hand_back(src, dst, slot, seq_is_own):
        if seq_is_own:
            return pltpu.make_async_copy(src, dst, misc_sem.at[1 + slot])
        return pltpu.make_async_remote_copy(
            src_ref=src,
            dst_ref=dst,
            send_sem=ret_send.at[slot],
            recv_sem=ret_recv.at[slot],
            device_id=across,
            device_id_type=MESH,
        )

    def attn_return(own):
        seq = f if own else other
        return [
            hand_back(attn_st.at[seq], attn_out.at[:, half_cols], 0, own),
            hand_back(log_st.at[seq], log_out.at[f], 1, own),
        ]

    def conv_return(g, own):
        seq = f if own else other
        cols = pl.ds(pl.multiple_of(f * (2 * chans) + (g - 1) * chans, 128), chans)
        return [hand_back(conv_st.at[g - 1, seq], conv_out.at[:, cols], 1 + g, own)]

    def project_conv(g, seq):
        @pl.loop(0, 2)
        def _(b):
            at = pl.multiple_of(b * mm_rows, WINDOW)
            out = jnp.dot(
                toks[seq, pl.ds(at, mm_rows), :], wts[g], preferred_element_type=jnp.float32
            )
            inner = out[:, :chans].astype(jnp.bfloat16).astype(jnp.float32)
            signal = out[:, chans : 2 * chans].astype(jnp.bfloat16).astype(jnp.float32)
            prod[g - 1, seq, pl.ds(at + pad, mm_rows), :] = (inner * signal).astype(jnp.bfloat16)
            outer[seq, pl.ds(at, mm_rows), :] = out[:, 2 * chans :].astype(jnp.bfloat16)

    def mix(g, seq):
        cols = pl.ds(pl.multiple_of(f * (2 * chans) + (g - 1) * chans, 128), chans)
        tap = taps[:, cols]
        size = rows + 2 * pad
        full = prod[g - 1, seq].astype(jnp.float32)
        before = pltpu.roll(full, 1, 0)[pad : pad + rows]
        after = pltpu.roll(full, size - 1, 0)[pad : pad + rows]
        mixed = tap[0:1] * before + tap[1:2] * full[pad : pad + rows] + tap[2:3] * after
        conv_st[g - 1, seq] = (outer[seq].astype(jnp.float32) * mixed).astype(jnp.bfloat16)

    def begin(copies):
        for c in copies:
            c.start()

    def pass_tokens():
        return pltpu.make_async_remote_copy(
            src_ref=toks.at[other, share],
            dst_ref=toks.at[other, share],
            send_sem=tok_send.at[1],
            recv_sem=tok_recv.at[1],
            device_id=beside,
            device_id_type=MESH,
        )

    def take_tokens():
        tok_copy.wait_recv()
        pass_tokens().start()

    def ready_tokens():
        pass_tokens().wait_recv()
        pass_tokens().wait_send()
        norm_rows(other)

    def first_own():
        tok_load.wait()
        norm_rows(f)

    def kv_start(seq, slot):
        edges_start(kvs, seq, WINDOW, kv_send, kv_recv, slot)

    def kv_wait(seq, slot):
        edges_wait(kvs, seq, WINDOW, kv_send, kv_recv, slot)

    def pr_start(g, seq, slot):
        edges_start(prod, seq, pad, pr_send, pr_recv, (g - 1) * 2 + slot)

    def pr_wait(g, seq, slot):
        edges_wait(prod, seq, pad, pr_send, pr_recv, (g - 1) * 2 + slot)

    def qkv_own():
        project_qkv(f)
        kv_start(f, 0)

    def qkv_other():
        project_qkv(other)
        kv_start(other, 1)

    def finish_conv(g, own):
        seq, slot = (f, 0) if own else (other, 1)
        pr_wait(g, seq, slot)
        mix(g, seq)
        begin(conv_return(g, own))

    def both_parts(g, own):
        seq, slot = (f, 0) if own else (other, 1)
        project_conv(g, seq)
        pr_start(g, seq, slot)

    third = blocks // 3 if blocks % 3 == 0 else blocks
    parts = blocks // third

    def attend_part(seq, i):
        if i < parts:
            attend(seq, i * third, third)

    plan = {
        (0, 0): [make_bias],
        (0, 2): [first_own],
        (1, 0): [qkv_own],
        (1, 2): [lambda: kv_wait(f, 0), lambda: attend_part(f, 0)],
        (1, 3): [lambda: attend_part(f, 1)],
        (1, 4): [lambda: attend_part(f, 2), lambda: begin(attn_return(True))],
        (1, 7): [take_tokens],
        (2, 0): [lambda: both_parts(1, True)],
        (2, 1): [ready_tokens],
        (2, 2): [qkv_other, lambda: finish_conv(1, True)],
        (2, 3): [lambda: both_parts(1, False)],
        (2, 4): [lambda: kv_wait(other, 1), lambda: attend_part(other, 0)],
        (2, 5): [lambda: attend_part(other, 1)],
        (2, 6): [lambda: attend_part(other, 2), lambda: begin(attn_return(False))],
        (2, 7): [lambda: finish_conv(1, False)],
    }
    spare = dict(plan)
    for g in range(GROUPS):
        for d in range(ns):
            for par in range(2):
                relay_step(g, d, par)
                for piece in spare.pop((g, d * 2 + par), []):
                    piece()
        for key in sorted(k for k in spare if k[0] == g):
            for piece in spare.pop(key):
                piece()

    both_parts(2, False)
    finish_conv(2, False)
    both_parts(2, True)
    finish_conv(2, True)

    tok_copy.wait_send()
    settle()
    for own in (True, False):
        for c in attn_return(own) + conv_return(1, own) + conv_return(2, own):
            c.wait()


def fused_device(
    ns,
    tps,
    tokens,
    norm_gain,
    query_weight,
    key_weight,
    value_weight,
    outer_weight,
    inner_weight,
    signal_weight,
    conv_taps,
    sink_logit,
):
    rows, width = tokens.shape[1:]
    depth, local = query_weight.shape
    qcols = local // 2
    heads = qcols // HEAD
    chans = outer_weight.shape[1] // 4
    head_local = 2 * heads
    group_cols = qcols + 2 * HEAD
    pad = 16
    bf, f32 = jnp.bfloat16, jnp.float32
    dma = pltpu.SemaphoreType.DMA
    hbm = pl.BlockSpec(memory_space=pltpu.HBM)
    anyspace = pl.BlockSpec(memory_space=pl.ANY)
    attended, conv, logs = pl.pallas_call(
        functools.partial(mega_kernel, ns, tps),
        out_shape=(
            jax.ShapeDtypeStruct((rows, local), bf),
            jax.ShapeDtypeStruct((rows, 4 * chans), bf),
            jax.ShapeDtypeStruct((2, heads, rows), f32),
        ),
        in_specs=[hbm] * 10,
        out_specs=(anyspace, anyspace, anyspace),
        scratch_shapes=[
            pltpu.VMEM((2, rows, width), bf),
            pltpu.VMEM((GROUPS, width, group_cols), bf),
            pltpu.VMEM((GROUPS, depth, group_cols), bf),
            pltpu.VMEM((2, rows, qcols), bf),
            pltpu.VMEM((2, rows + 2 * WINDOW, 2 * HEAD), bf),
            pltpu.VMEM((heads, 3 * WINDOW, WINDOW), f32),
            pltpu.VMEM((2, 2, rows + 2 * pad, chans), bf),
            pltpu.VMEM((2, rows, chans), bf),
            pltpu.VMEM((2, rows, qcols), bf),
            pltpu.VMEM((2, heads, rows), f32),
            pltpu.VMEM((2, 2, rows, chans), bf),
            pltpu.VMEM((2, depth, 2 * HEAD), bf),
            pltpu.VMEM((width // 128, 128), f32),
            pltpu.VMEM((1, width), f32),
            pltpu.VMEM((3, 4 * chans), f32),
            pltpu.SMEM((head_local,), f32),
            dma((5,)),
            dma((GROUPS, 3)),
            dma((GROUPS, 3)),
            dma((5,)),
            dma((GROUPS,)),
            dma((GROUPS, 2 * ns)),
            dma((GROUPS, 2 * ns)),
            dma((GROUPS, 2 * ns)),
            dma((2,)),
            dma((2,)),
            dma((2, 2)),
            dma((2, 2)),
            dma((4, 2)),
            dma((4, 2)),
            dma((4,)),
            dma((4,)),
        ],
        compiler_params=pltpu.CompilerParams(
            collective_id=0, has_side_effects=True, vmem_limit_bytes=67043328
        ),
    )(
        tokens[0],
        norm_gain.reshape(width // 128, 128),
        query_weight,
        key_weight,
        value_weight,
        outer_weight,
        inner_weight,
        signal_weight,
        conv_taps,
        sink_logit,
    )
    return (attended[None], conv[None], logs.reshape(1, head_local, rows))


def fits(mesh, args):
    tokens, query_weight, key_weight, outer_weight = (args[i] for i in (0, 2, 3, 5))
    sp, fs, tp = (mesh.shape[a] for a in ("sp", "fs", "tp"))
    rows = tokens.shape[1] // sp
    return (
        fs == 2
        and tokens.shape[0] == fs
        and tp % 2 == 0
        and rows % (2 * WINDOW) == 0
        and key_weight.shape[1] == 2 * HEAD * tp
        and query_weight.shape[1] % (256 * tp) == 0
        and outer_weight.shape[1] == 512 * tp
        and query_weight.shape[1] == 512 * tp
        and query_weight.shape[0] % (16 * sp * fs) == 0
    )


def solution(mesh):
    in_specs = (
        P("fs", "sp", None),
        P(),
        P(("sp", "fs"), "tp"),
        P(("sp", "fs"), "tp"),
        P(("sp", "fs"), "tp"),
        P(("sp", "fs"), "tp"),
        P(("sp", "fs"), "tp"),
        P(("sp", "fs"), "tp"),
        P(None, "tp"),
        P("tp"),
    )
    out_specs = (P("fs", "sp", "tp"), P("fs", "sp", "tp"), P("fs", "tp", "sp"))

    def run(*args):
        body = per_device
        if fits(mesh, args):
            body = functools.partial(fused_device, mesh.shape["sp"], mesh.shape["tp"])
        return jax.shard_map(
            body, mesh=mesh, in_specs=in_specs, out_specs=out_specs, check_vma=False
        )(*args)

    return run
```

```python
import math

import functools

import jax
import jax.numpy as jnp
from jax import lax
from jax.experimental import pallas as pl
from jax.experimental.pallas import tpu as pltpu
from jax.sharding import PartitionSpec as P

HEAD = 64
WINDOW = 128


EPSILON = 1e-06


def extended(value, sides, width):
    for axis, dim in sides:
        size, length = (lax.axis_size(axis), value.shape[dim])
        up = [(i, (i + 1) % size) for i in range(size - 1)]
        down = [(j, i) for i, j in up]
        last = lax.slice_in_dim(value, length - width, length, axis=dim)
        initial = lax.slice_in_dim(value, 0, width, axis=dim)
        before = lax.ppermute(last, axis, up)
        after = lax.ppermute(initial, axis, down)
        value = jnp.concatenate([before, value, after], axis=dim)
    return value


def normalized(tokens, norm_gain):
    values = tokens.astype(jnp.float32)
    scaling = lax.rsqrt(jnp.mean(values * values, axis=-1, keepdims=True) + EPSILON)
    return (values * scaling * norm_gain).astype(jnp.bfloat16)


def folding(normed):

    def add_portions(running, portions, offset):
        return tuple(
            (jnp.dot(normed, portion, preferred_element_type=jnp.float32) for portion in portions)
        )

    return add_portions


def empty_sums(normed, weights):
    return tuple((jnp.zeros((normed.shape[0], weight.shape[1]), jnp.float32) for weight in weights))


def rounded(results):
    return tuple((result.astype(jnp.bfloat16) for result in results))


def gate_product(inner_gate, signal):
    return (inner_gate.astype(jnp.float32) * signal.astype(jnp.float32)).astype(jnp.bfloat16)


def send_edges(key_proj, value_proj, product):
    stacked = jnp.concatenate([key_proj, value_proj], axis=1)
    window_rows = extended(stacked, (("sp", 0),), WINDOW)
    conv_rows = extended(product, (("sp", 0),), 1)
    return (window_rows, conv_rows)


def banded_attention(queries, window_rows, sink_logit, slopes, first_pos, seq_length):
    tok_count = queries.shape[0]
    kv_cols = window_rows.shape[1] // 2
    kv_heads = kv_cols // HEAD
    group_size = queries.shape[1] // (HEAD * kv_heads)
    block_count = tok_count // WINDOW
    query_blocks = queries.reshape(block_count, WINDOW, kv_heads, group_size, HEAD)
    key_rows = window_rows[:, :kv_cols].reshape(block_count + 2, WINDOW, kv_heads, HEAD)
    value_rows = window_rows[:, kv_cols:].reshape(block_count + 2, WINDOW, kv_heads, HEAD)
    key_span = jnp.concatenate([key_rows[:-2], key_rows[1:-1], key_rows[2:]], axis=1)
    value_span = jnp.concatenate([value_rows[:-2], value_rows[1:-1], value_rows[2:]], axis=1)
    scores = jnp.einsum(
        "bqkgd,bskd->bkgqs", query_blocks, key_span, preferred_element_type=jnp.float32
    ) * (1.0 / math.sqrt(HEAD))
    distance = jnp.arange(WINDOW)[:, None] - jnp.arange(3 * WINDOW)[None, :] + WINDOW
    key_pos = (
        first_pos
        - WINDOW
        + WINDOW * jnp.arange(block_count)[:, None]
        + jnp.arange(3 * WINDOW)[None, :]
    )
    inside = (jnp.abs(distance)[None] <= WINDOW) & ((key_pos >= 0) & (key_pos < seq_length))[
        :, None, :
    ]
    scores = scores - slopes.reshape(kv_heads, group_size, 1, 1) * jnp.abs(distance).astype(
        jnp.float32
    )
    scores = jnp.where(inside[:, None, None], scores, -jnp.inf)
    sink_grid = sink_logit.reshape(kv_heads, group_size, 1, 1)
    row_peak = jnp.maximum(jnp.max(scores, axis=-1, keepdims=True), sink_grid)
    weights = jnp.exp(scores - row_peak)
    row_total = jnp.sum(weights, axis=-1, keepdims=True) + jnp.exp(sink_grid - row_peak)
    weighted = jnp.einsum(
        "bkgqs,bskd->bqkgd",
        weights.astype(jnp.bfloat16),
        value_span,
        preferred_element_type=jnp.float32,
    )
    attended = (
        (weighted / row_total.transpose(0, 3, 1, 2, 4))
        .astype(jnp.bfloat16)
        .reshape(tok_count, kv_heads * group_size * HEAD)
    )
    log_total = (
        (row_peak + jnp.log(row_total))[..., 0]
        .transpose(1, 2, 0, 3)
        .reshape(kv_heads * group_size, tok_count)
    )
    return (attended, log_total)


def per_device(
    tokens,
    norm_gain,
    query_weight,
    key_weight,
    value_weight,
    outer_weight,
    inner_weight,
    signal_weight,
    conv_taps,
    sink_logit,
):
    normed = normalized(tokens[0], norm_gain)
    add_portions = folding(normed)
    all_sums = add_portions(
        empty_sums(
            normed,
            (query_weight, key_weight, value_weight, outer_weight, inner_weight, signal_weight),
        ),
        (
            lax.all_gather(query_weight, ("sp", "fs"), axis=0, tiled=True),
            lax.all_gather(key_weight, ("sp", "fs"), axis=0, tiled=True),
            lax.all_gather(value_weight, ("sp", "fs"), axis=0, tiled=True),
            lax.all_gather(outer_weight, ("sp", "fs"), axis=0, tiled=True),
            lax.all_gather(inner_weight, ("sp", "fs"), axis=0, tiled=True),
            lax.all_gather(signal_weight, ("sp", "fs"), axis=0, tiled=True),
        ),
        jnp.int32(0),
    )
    queries, key_proj, value_proj, outer_gate, inner_gate, signal = rounded(all_sums)
    product = gate_product(inner_gate, signal)
    window_rows, conv_rows = send_edges(key_proj, value_proj, product)
    tok_count = normed.shape[0]
    head_local = queries.shape[1] // HEAD
    head_index = lax.axis_index("tp") * head_local + jnp.arange(1, head_local + 1)
    slopes = jnp.exp2(-8.0 * head_index.astype(jnp.float32) / (head_local * lax.axis_size("tp")))
    first_pos = lax.axis_index("sp") * tok_count
    attended, log_total = banded_attention(
        queries, window_rows, sink_logit, slopes, first_pos, tok_count * lax.axis_size("sp")
    )
    mixed_conv = conv_taps[0] * conv_rows[0:tok_count].astype(jnp.float32)
    mixed_conv = mixed_conv + conv_taps[1] * conv_rows[1 : tok_count + 1].astype(jnp.float32)
    mixed_conv = mixed_conv + conv_taps[2] * conv_rows[2 : tok_count + 2].astype(jnp.float32)
    conv_out = (outer_gate.astype(jnp.float32) * mixed_conv).astype(jnp.bfloat16)
    return (attended[None], conv_out[None], log_total[None])


MESH = pl.DeviceIdType.MESH
GROUPS = 3
SPAN = 4
SUBS = 4
FAR = -1e30


def mega_kernel(
    tps,
    tokens,
    gain_in,
    qw,
    kw,
    vw,
    ow,
    iw,
    sw,
    taps_in,
    sinks_in,
    attn_out,
    conv_out,
    log_out,
    toks,
    wts,
    stage_w,
    qs,
    kvs,
    bias,
    prod,
    outer,
    attn_st,
    log_st,
    conv_st,
    kv_raw,
    gain_raw,
    gain,
    taps,
    sinks,
    small_sem,
    load_sem,
    stage_sem,
    misc_sem,
    own_sem,
    y_send,
    w_recv,
    pair_send,
    mid_send,
    tok_y_send,
    tok_z_send,
    tok_t_send,
    tok_recv,
    kv_send,
    kv_recv,
    pr_send,
    pr_recv,
    ret_send,
    ret_recv,
    conv_send,
    conv_recv,
):
    s, f, t = lax.axis_index("sp"), lax.axis_index("fs"), lax.axis_index("tp")
    other = 1 - f
    core = lax.rem(t, 2)
    outward = 1 - lax.rem(s, 2)
    partner = s + 2 * outward - 1
    facing = SPAN - 1 - s
    far = SPAN - 1 - partner
    is_mid = (s == 1) | (s == SPAN - 2)
    is_end = jnp.logical_not(is_mid)
    low_half = s < SPAN // 2
    pair, diag, mid = (partner, f, t), (partner, other, t), (facing, f, t)
    across = (s, other, t)
    mate_t, beyond_t = t + 1 - 2 * core, lax.rem(t + 2, tps)
    mate, beyond = (s, f, mate_t), (s, f, beyond_t)
    rows = tokens.shape[0]
    depth = qw.shape[0]
    qcols = qs.shape[2]
    heads = qcols // HEAD
    chans = prod.shape[3]
    both_rows = outer.shape[2]
    blocks = rows // WINDOW
    pad = (prod.shape[2] - both_rows) // 2
    sub = rows // SUBS
    part = sub // tps
    up, down = (s + 1, f, t), (s - 1, f, t)
    has_up, has_down = s < SPAN - 1, s > 0
    own_off = jnp.where(low_half, rows, 0)
    end_off = rows - own_off

    barrier = pltpu.get_barrier_semaphore()
    for peer in (pair, diag, across, mate, beyond):
        pl.semaphore_signal(barrier, inc=1, device_id=peer, device_id_type=MESH)

    @pl.when(is_mid)
    def _():
        pl.semaphore_signal(barrier, inc=1, device_id=mid, device_id_type=MESH)

    def block_rows(blk):
        return pl.ds(pl.multiple_of(blk * depth, 16), depth)

    def loads(g, half, dest, sems):
        if g == 0:
            qc = pl.ds(pl.multiple_of(half * qcols, 128), qcols)
            pairs = [(qw.at[:, qc], dest.at[:, pl.ds(0, qcols)])]
        else:
            c = pl.ds(pl.multiple_of(half * (2 * chans) + (g - 1) * chans, 128), chans)
            pairs = [
                (ref.at[:, c], dest.at[:, pl.ds(i * chans, chans)])
                for i, ref in enumerate((iw, sw, ow))
            ]
        return [
            pltpu.make_async_copy(a, b, sems.at[g, i]) for i, (a, b) in enumerate(pairs)
        ]

    mine = s * 2 + f
    theirs = s * 2 + other
    own_loads = [loads(g, f, wts.at[g, block_rows(mine)], load_sem) for g in range(GROUPS)]
    out_loads = [loads(g, other, stage_w.at[g], stage_sem) for g in range(GROUPS)]
    small = [
        pltpu.make_async_copy(a, b, small_sem.at[i])
        for i, (a, b) in enumerate(
            (
                (kw, kv_raw.at[0]),
                (vw, kv_raw.at[1]),
                (gain_in, gain_raw),
                (taps_in, taps),
                (sinks_in, sinks),
            )
        )
    ]
    tok_load = pltpu.make_async_copy(tokens, toks.at[f], misc_sem.at[0])

    def begin(copies):
        for c in copies:
            c.start()

    def finish(copies):
        for c in copies:
            c.wait()

    begin(small[:2] + out_loads[0] + own_loads[0] + small[2:])
    tok_load.start()
    begin(out_loads[1] + own_loads[1] + out_loads[2] + own_loads[2])

    def remote(src, dst, send, recv, peer):
        return pltpu.make_async_remote_copy(
            src_ref=src,
            dst_ref=dst,
            send_sem=send,
            recv_sem=recv,
            device_id=peer,
            device_id_type=MESH,
        )

    def y_copy(g):
        return remote(
            stage_w.at[g], wts.at[g, block_rows(mine)], y_send.at[g], w_recv.at[g, mine], across
        )

    def block_copy(g, blk, sends, peer):
        at = wts.at[g, block_rows(blk)]
        return remote(at, at, sends.at[g, blk], w_recv.at[g, blk], peer)

    def to_pair(g, blk):
        return block_copy(g, blk, pair_send, pair)

    def to_mid(g, blk):
        return block_copy(g, blk, mid_send, mid)

    def arrived(g, blk):
        to_pair(g, blk).wait_recv()

    def slot_of(k):
        return (other, 2 + f, 2 + other)[k]

    def piece(slot, j, q):
        return toks.at[slot, pl.ds(pl.multiple_of(j * sub + q * part, 16), part)]

    def tok_y(k, j):
        slot = f if k == 0 else 2 + f
        at = piece(slot, j, t)
        return remote(at, at, tok_y_send.at[k, j], tok_recv.at[2 if k else 0, j, 0], across)

    def tok_z(k, j):
        seq = f if k == 0 else other
        return remote(
            piece(seq, j, t),
            piece(2 + seq, j, t),
            tok_z_send.at[k, j],
            tok_recv.at[1 + k, j, 0],
            pair,
        )

    def tok_share(k, j, kind):
        q = beyond_t if kind == 2 else t
        at = piece(slot_of(k), j, q)
        return remote(
            at, at, tok_t_send.at[k, j, kind], tok_recv.at[k, j, kind + 1],
            beyond if kind == 1 else mate,
        )

    def tok_wait(k, j, kind):
        at = piece(slot_of(k), j, t)
        remote(at, at, tok_t_send.at[k, j, 0], tok_recv.at[k, j, kind], mate).wait_recv()

    def take(k, j):
        tok_wait(k, j, 0)
        tok_share(k, j, 1).start()
        tok_share(k, j, 0).start()

    def hand(k, j):
        tok_wait(k, j, 2)
        tok_share(k, j, 2).start()

    def have(k, j):
        tok_wait(k, j, 1)
        tok_wait(k, j, 3)

    def norm_own():
        @pl.loop(0, blocks)
        def _(b):
            at = pl.ds(pl.multiple_of(b * WINDOW, WINDOW), WINDOW)
            values = toks[f, at, :].astype(jnp.float32)
            scaling = lax.rsqrt(jnp.mean(values * values, axis=-1, keepdims=True) + EPSILON)
            toks[f, at, :] = (values * scaling * gain[...]).astype(jnp.bfloat16)

    mm_rows = rows // 2

    def make_bias():
        key = lax.broadcasted_iota(jnp.int32, (3 * WINDOW, WINDOW), 0)
        query = lax.broadcasted_iota(jnp.int32, (3 * WINDOW, WINDOW), 1)
        away = jnp.abs(query - key + WINDOW)
        for h in range(heads):
            index = (t * (2 * heads) + f * heads + h + 1).astype(jnp.float32)
            slope = jnp.exp2(jnp.full((1, WINDOW), -8.0 / (2 * heads * tps), jnp.float32) * index)
            bias[h] = jnp.where(away <= WINDOW, -slope * away.astype(jnp.float32), FAR)

    def project_qkv(seq):
        @pl.loop(0, 2)
        def _(b):
            at = pl.multiple_of(b * mm_rows, WINDOW)
            out = jnp.dot(
                toks[seq, pl.ds(at, mm_rows), :], wts[0], preferred_element_type=jnp.float32
            )
            qs[seq, pl.ds(at, mm_rows), :] = out[:, :qcols].astype(jnp.bfloat16)
            kvs[seq, pl.ds(at + WINDOW, mm_rows), :] = out[:, qcols:].astype(jnp.bfloat16)

    kv_len = kvs.shape[1]

    def kv_copies(seq, slot):
        ref = kvs.at[seq]
        climb = remote(
            ref.at[pl.ds(kv_len - 2 * WINDOW, WINDOW)],
            ref.at[pl.ds(0, WINDOW)],
            kv_send.at[slot, 0],
            kv_recv.at[slot, 0],
            up,
        )
        fall = remote(
            ref.at[pl.ds(WINDOW, WINDOW)],
            ref.at[pl.ds(kv_len - WINDOW, WINDOW)],
            kv_send.at[slot, 1],
            kv_recv.at[slot, 1],
            down,
        )
        return climb, fall

    def kv_start(seq, slot):
        climb, fall = kv_copies(seq, slot)
        blank = jnp.zeros((WINDOW, 2 * HEAD), jnp.bfloat16)

        @pl.when(has_up)
        def _():
            climb.start()

        @pl.when(has_down)
        def _():
            fall.start()

        @pl.when(jnp.logical_not(has_up))
        def _():
            kvs[seq, pl.ds(kv_len - WINDOW, WINDOW), :] = blank

        @pl.when(jnp.logical_not(has_down))
        def _():
            kvs[seq, pl.ds(0, WINDOW), :] = blank

    def kv_wait(seq, slot):
        climb, fall = kv_copies(seq, slot)

        @pl.when(has_up)
        def _():
            climb.wait_send()
            fall.wait_recv()

        @pl.when(has_down)
        def _():
            fall.wait_send()
            climb.wait_recv()

    def attend(seq, first, count, step=1):
        @pl.loop(0, count)
        def _(i):
            b = first + i * step
            at = pl.multiple_of(b * WINDOW, WINDOW)
            kv = kvs[seq, pl.ds(at, 3 * WINDOW), :]
            keys = kv[:, :HEAD]
            values_t = kv.astype(jnp.float32).T[HEAD:, :].astype(jnp.bfloat16)
            queries = qs[seq, pl.ds(at, WINDOW), :]
            low = jnp.where((b == 0) & (s == 0), FAR, 0.0)
            high = jnp.where((b == blocks - 1) & (s == SPAN - 1), FAR, 0.0)
            outs = []
            for h in range(heads):
                query = queries[:, h * HEAD : (h + 1) * HEAD]
                scores = lax.dot_general(
                    keys, query, (((1,), (1,)), ((), ())), preferred_element_type=jnp.float32
                )
                scores = scores * (1.0 / math.sqrt(HEAD)) + bias[h]
                scores = jnp.concatenate(
                    [
                        scores[:WINDOW] + low,
                        scores[WINDOW : 2 * WINDOW],
                        scores[2 * WINDOW :] + high,
                    ],
                    axis=0,
                )
                sink = sinks[f * heads + h]
                peak = jnp.maximum(jnp.max(scores, axis=0, keepdims=True), sink)
                weights = jnp.exp(scores - peak)
                total = jnp.sum(weights, axis=0, keepdims=True) + jnp.exp(sink - peak)
                mixed = jnp.dot(
                    values_t, weights.astype(jnp.bfloat16), preferred_element_type=jnp.float32
                )
                outs.append(mixed / total)
                log_st[seq, pl.ds(h, 1), pl.ds(at, WINDOW)] = peak + jnp.log(total)
            stacked = jnp.concatenate(outs, axis=0)
            attn_st[seq, pl.ds(at, WINDOW), :] = stacked.T.astype(jnp.bfloat16)

    half_cols = pl.ds(pl.multiple_of(f * qcols, 128), qcols)

    def attn_return(own):
        seq = f if own else other
        pairs = [
            (attn_st.at[seq], attn_out.at[:, half_cols]),
            (log_st.at[seq], log_out.at[f]),
        ]
        if own:
            return [pltpu.make_async_copy(a, b, misc_sem.at[1 + i]) for i, (a, b) in enumerate(pairs)]
        return [
            remote(a, b, ret_send.at[i], ret_recv.at[i], across) for i, (a, b) in enumerate(pairs)
        ]

    def conv_cols(g):
        return pl.ds(pl.multiple_of(f * (2 * chans) + (g - 1) * chans, 128), chans)

    def conv_return(g, own_seq, own_rows):
        seq = f if own_seq else other
        off = own_off if own_rows else end_off
        src = conv_st.at[g - 1, seq, pl.ds(pl.multiple_of(off, WINDOW), rows)]
        dst = conv_out.at[:, conv_cols(g)]
        if own_seq and own_rows:
            return pltpu.make_async_copy(src, dst, own_sem.at[g - 1])
        which = 0 if own_seq else 1
        kind = 0 if own_seq else (2 if own_rows else 1)
        peer = pair if own_seq else (across if own_rows else diag)
        return remote(src, dst, conv_send.at[g - 1, kind], conv_recv.at[g - 1, which], peer)

    def project_conv(g, seq, own_rows):
        slot, off = (seq, own_off) if own_rows else (2 + seq, end_off)

        @pl.loop(0, 2)
        def _(b):
            at = pl.multiple_of(b * mm_rows, WINDOW)
            to = pl.multiple_of(off + b * mm_rows, WINDOW)
            out = jnp.dot(
                toks[slot, pl.ds(at, mm_rows), :], wts[g], preferred_element_type=jnp.float32
            )
            inner = out[:, :chans].astype(jnp.bfloat16).astype(jnp.float32)
            signal = out[:, chans : 2 * chans].astype(jnp.bfloat16).astype(jnp.float32)
            prod[g - 1, seq, pl.ds(to + pad, mm_rows), :] = (inner * signal).astype(jnp.bfloat16)
            outer[g - 1, seq, pl.ds(to, mm_rows), :] = out[:, 2 * chans :].astype(jnp.bfloat16)

    def pr_copies(g, seq, slot):
        ref = prod.at[g - 1, seq]
        climb = remote(
            ref.at[pl.ds(both_rows, pad)],
            ref.at[pl.ds(0, pad)],
            pr_send.at[g - 1, slot],
            pr_recv.at[g - 1, slot],
            mid,
        )
        fall = remote(
            ref.at[pl.ds(pad, pad)],
            ref.at[pl.ds(both_rows + pad, pad)],
            pr_send.at[g - 1, slot],
            pr_recv.at[g - 1, slot],
            mid,
        )
        return climb, fall

    def pr_start(g, seq, slot):
        climb, fall = pr_copies(g, seq, slot)
        blank = jnp.zeros((pad, chans), jnp.bfloat16)

        @pl.when(low_half)
        def _():
            climb.start()
            prod[g - 1, seq, pl.ds(0, pad), :] = blank

        @pl.when(jnp.logical_not(low_half))
        def _():
            fall.start()
            prod[g - 1, seq, pl.ds(both_rows + pad, pad), :] = blank

    def pr_wait(g, seq, slot):
        climb, fall = pr_copies(g, seq, slot)

        @pl.when(low_half)
        def _():
            climb.wait_send()
            fall.wait_recv()

        @pl.when(jnp.logical_not(low_half))
        def _():
            fall.wait_send()
            climb.wait_recv()

    def mix(g, seq, own_rows):
        off = pl.multiple_of(own_off if own_rows else end_off, WINDOW)
        tap = taps[:, conv_cols(g)]
        size = rows + 2 * pad
        full = prod[g - 1, seq, pl.ds(off, size), :].astype(jnp.float32)
        before = pltpu.roll(full, 1, 0)[pad : pad + rows]
        after = pltpu.roll(full, size - 1, 0)[pad : pad + rows]
        mixed = tap[0:1] * before + tap[1:2] * full[pad : pad + rows] + tap[2:3] * after
        gate = outer[g - 1, seq, pl.ds(off, rows), :].astype(jnp.float32)
        conv_st[g - 1, seq, pl.ds(off, rows), :] = (gate * mixed).astype(jnp.bfloat16)

    finish(small[:2])
    keys0, vals0 = kv_raw[0], kv_raw[1]
    halves = [
        jnp.concatenate([w[:, i * HEAD : (i + 1) * HEAD] for w in (keys0, vals0)], axis=1)
        for i in range(2)
    ]
    first = f == 0
    stage_w[0, :, pl.ds(qcols, 2 * HEAD)] = jnp.where(first, halves[1], halves[0])
    wts[0, block_rows(mine), pl.ds(qcols, 2 * HEAD)] = jnp.where(first, halves[0], halves[1])

    pl.semaphore_wait(barrier, jnp.where(is_mid, 6, 5))

    finish(own_loads[0])
    to_pair(0, mine).start()

    @pl.when(is_mid)
    def _():
        to_mid(0, mine).start()

    finish(out_loads[0])
    y_copy(0).start()
    finish(out_loads[1])
    y_copy(1).start()
    finish(own_loads[1])

    @pl.when(is_mid)
    def _():
        to_mid(1, mine).start()

    finish(small[2:])
    for i in range(gain_raw.shape[0]):
        gain[:, i * 128 : (i + 1) * 128] = gain_raw[i : i + 1, :]
    tok_load.wait()
    norm_own()
    for j in range(SUBS // 2):
        tok_y(0, j).start()
    finish(out_loads[2] + own_loads[2])
    y_copy(2).start()
    for j in range(SUBS // 2, SUBS):
        tok_y(0, j).start()

    def relay(g, blk, onward):
        arrived(g, blk)
        onward(g, blk).start()

    pt = [partner * 2 + f, partner * 2 + other]
    ct = [facing * 2 + f, facing * 2 + other]
    ft = [far * 2 + f, far * 2 + other]

    def end_program():
        tok_z(0, 0).start()
        relay(0, theirs, to_pair)
        tok_z(0, 1).start()
        to_pair(1, mine).start()
        relay(1, theirs, to_pair)
        tok_z(0, 2).start()
        tok_z(0, 3).start()
        to_pair(2, mine).start()
        make_bias()
        take(0, 0)
        take(0, 1)
        hand(0, 0)
        relay(2, theirs, to_pair)
        hand(0, 1)
        take(0, 2)
        tok_z(1, 2).start()
        hand(0, 2)
        take(0, 3)
        tok_z(1, 3).start()
        for blk in pt + ct + ft:
            arrived(0, blk)
        project_qkv(f)
        kv_start(f, 0)
        hand(0, 3)
        for j in range(SUBS):
            have(0, j)
        project_qkv(other)
        kv_start(other, 1)
        attend(f, 1, blocks - 2)
        kv_wait(f, 0)
        attend(f, 0, 2, blocks - 1)
        begin(attn_return(True))
        attend(other, 1, blocks - 2)
        kv_wait(other, 1)
        attend(other, 0, 2, blocks - 1)
        begin(attn_return(False))
        for g in (1, 2):
            for own_seq in (True, False):
                conv_return(g, own_seq, False).wait_recv()
        for g in range(GROUPS):
            to_pair(g, mine).wait_send()
            to_pair(g, theirs).wait_send()
        for j in range(SUBS):
            tok_z(0, j).wait_send()
        for j in range(SUBS // 2, SUBS):
            tok_z(1, j).wait_send()

    def conv_own(g, own_seq):
        seq, slot = (f, 0) if own_seq else (other, 1)
        project_conv(g, seq, True)
        pr_start(g, seq, slot)

    def conv_end(g, own_seq):
        seq = f if own_seq else other
        project_conv(g, seq, False)
        mix(g, seq, False)
        conv_return(g, own_seq, False).start()

    def conv_close(g, own_seq):
        seq, slot = (f, 0) if own_seq else (other, 1)
        pr_wait(g, seq, slot)
        mix(g, seq, True)
        conv_return(g, own_seq, True).start()

    def mid_program():
        make_bias()
        relay(0, theirs, to_mid)
        to_pair(0, theirs).start()
        relay(1, theirs, to_mid)
        relay(0, ct[0], to_pair)
        relay(0, pt[0], to_mid)
        take(1, 0)
        tok_y(1, 0).start()
        take(0, 0)
        relay(0, pt[1], to_mid)
        to_mid(2, mine).start()
        relay(0, ct[1], to_pair)
        hand(1, 0)
        take(1, 1)
        tok_y(1, 1).start()
        take(0, 1)
        hand(0, 0)
        relay(2, theirs, to_mid)
        relay(1, pt[0], to_mid)
        hand(1, 1)
        relay(0, ft[0], to_pair)
        take(2, 0)
        hand(0, 1)
        relay(1, pt[1], to_mid)
        relay(0, ft[1], to_pair)
        project_qkv(f)
        kv_start(f, 0)
        take(0, 2)
        take(2, 1)
        hand(2, 0)
        attend(f, 1, (blocks - 2) // 2)
        take(0, 3)
        take(1, 2)
        hand(0, 2)
        hand(2, 1)
        attend(f, 1 + (blocks - 2) // 2, (blocks - 2) // 2)
        take(1, 3)
        hand(0, 3)
        hand(1, 2)
        for j in range(SUBS):
            have(0, j)
        project_qkv(other)
        kv_start(other, 1)
        relay(2, pt[0], to_mid)
        hand(1, 3)
        kv_wait(f, 0)
        attend(f, 0, 2, blocks - 1)
        begin(attn_return(True))
        relay(2, pt[1], to_mid)
        attend(other, 1, blocks - 2)
        kv_wait(other, 1)
        attend(other, 0, 2, blocks - 1)
        begin(attn_return(False))
        for blk in ct + ft:
            arrived(1, blk)
        conv_own(1, True)
        conv_own(1, False)
        take(2, 2)
        for j in range(SUBS):
            have(1, j)
        conv_end(1, True)
        hand(2, 2)
        take(2, 3)
        conv_close(1, True)
        hand(2, 3)
        for blk in ct + ft:
            arrived(2, blk)
        conv_own(2, True)
        conv_own(2, False)
        conv_end(2, True)
        conv_close(2, True)
        for j in range(SUBS):
            have(2, j)
        conv_end(1, False)
        conv_end(2, False)
        conv_close(1, False)
        conv_close(2, False)
        for g in (1, 2):
            conv_return(g, False, True).wait_recv()
            conv_return(g, True, True).wait()
            conv_return(g, False, True).wait_send()
            for own_seq in (True, False):
                conv_return(g, own_seq, False).wait_send()
        for blk in [mine, theirs] + ct + ft:
            to_pair(0, blk).wait_send()
        for g in range(GROUPS):
            for blk in [mine, theirs] + pt:
                to_mid(g, blk).wait_send()
        for j in range(SUBS // 2):
            tok_y(1, j).wait_send()
        for k in (1, 2):
            for j in range(SUBS):
                for kind in range(3):
                    tok_share(k, j, kind).wait_send()

    pl.when(is_end)(end_program)
    pl.when(is_mid)(mid_program)

    for g in range(GROUPS):
        y_copy(g).wait_send()
    for j in range(SUBS):
        tok_y(0, j).wait_send()
        for kind in range(3):
            tok_share(0, j, kind).wait_send()
    for own in (True, False):
        finish(attn_return(own))


def fused_device(
    tps,
    tokens,
    norm_gain,
    query_weight,
    key_weight,
    value_weight,
    outer_weight,
    inner_weight,
    signal_weight,
    conv_taps,
    sink_logit,
):
    rows, width = tokens.shape[1:]
    depth, local = query_weight.shape
    qcols = local // 2
    heads = qcols // HEAD
    chans = outer_weight.shape[1] // 4
    head_local = 2 * heads
    group_cols = qcols + 2 * HEAD
    pad = 16
    bf, f32 = jnp.bfloat16, jnp.float32
    dma = pltpu.SemaphoreType.DMA
    hbm = pl.BlockSpec(memory_space=pltpu.HBM)
    anyspace = pl.BlockSpec(memory_space=pl.ANY)
    attended, conv, logs = pl.pallas_call(
        functools.partial(mega_kernel, tps),
        out_shape=(
            jax.ShapeDtypeStruct((rows, local), bf),
            jax.ShapeDtypeStruct((rows, 4 * chans), bf),
            jax.ShapeDtypeStruct((2, heads, rows), f32),
        ),
        in_specs=[hbm] * 10,
        out_specs=(anyspace, anyspace, anyspace),
        scratch_shapes=[
            pltpu.VMEM((4, rows, width), bf),
            pltpu.VMEM((GROUPS, width, group_cols), bf),
            pltpu.VMEM((GROUPS, depth, group_cols), bf),
            pltpu.VMEM((2, rows, qcols), bf),
            pltpu.VMEM((2, rows + 2 * WINDOW, 2 * HEAD), bf),
            pltpu.VMEM((heads, 3 * WINDOW, WINDOW), f32),
            pltpu.VMEM((2, 2, 2 * rows + 2 * pad, chans), bf),
            pltpu.VMEM((2, 2, 2 * rows, chans), bf),
            pltpu.VMEM((2, rows, qcols), bf),
            pltpu.VMEM((2, heads, rows), f32),
            pltpu.VMEM((2, 2, 2 * rows, chans), bf),
            pltpu.VMEM((2, depth, 2 * HEAD), bf),
            pltpu.VMEM((width // 128, 128), f32),
            pltpu.VMEM((1, width), f32),
            pltpu.VMEM((3, 4 * chans), f32),
            pltpu.SMEM((head_local,), f32),
            dma((5,)),
            dma((GROUPS, 3)),
            dma((GROUPS, 3)),
            dma((3,)),
            dma((2,)),
            dma((GROUPS,)),
            dma((GROUPS, 2 * SPAN)),
            dma((GROUPS, 2 * SPAN)),
            dma((GROUPS, 2 * SPAN)),
            dma((2, SUBS)),
            dma((2, SUBS)),
            dma((3, SUBS, 3)),
            dma((3, SUBS, 4)),
            dma((2, 2)),
            dma((2, 2)),
            dma((2, 2)),
            dma((2, 2)),
            dma((2,)),
            dma((2,)),
            dma((2, 3)),
            dma((2, 2)),
        ],
        compiler_params=pltpu.CompilerParams(
            collective_id=0, has_side_effects=True, vmem_limit_bytes=67043328
        ),
    )(
        tokens[0],
        norm_gain.reshape(width // 128, 128),
        query_weight,
        key_weight,
        value_weight,
        outer_weight,
        inner_weight,
        signal_weight,
        conv_taps,
        sink_logit,
    )
    return (attended[None], conv[None], logs.reshape(1, head_local, rows))


def fits(mesh, args):
    tokens, query_weight, key_weight, outer_weight = (args[i] for i in (0, 2, 3, 5))
    sp, fs, tp = (mesh.shape[a] for a in ("sp", "fs", "tp"))
    rows = tokens.shape[1] // sp
    return (
        fs == 2
        and sp == SPAN
        and tokens.shape[0] == fs
        and tp == 4
        and rows % (2 * WINDOW) == 0
        and rows // WINDOW % 2 == 0
        and rows % (16 * SUBS * tp) == 0
        and key_weight.shape[1] == 2 * HEAD * tp
        and query_weight.shape[1] % (256 * tp) == 0
        and outer_weight.shape[1] == 512 * tp
        and query_weight.shape[1] == 512 * tp
        and query_weight.shape[0] % (16 * sp * fs) == 0
    )


def solution(mesh):
    in_specs = (
        P("fs", "sp", None),
        P(),
        P(("sp", "fs"), "tp"),
        P(("sp", "fs"), "tp"),
        P(("sp", "fs"), "tp"),
        P(("sp", "fs"), "tp"),
        P(("sp", "fs"), "tp"),
        P(("sp", "fs"), "tp"),
        P(None, "tp"),
        P("tp"),
    )
    out_specs = (P("fs", "sp", "tp"), P("fs", "sp", "tp"), P("fs", "tp", "sp"))

    def run(*args):
        body = per_device
        if fits(mesh, args):
            body = functools.partial(fused_device, mesh.shape["tp"])
        return jax.shard_map(
            body, mesh=mesh, in_specs=in_specs, out_specs=out_specs, check_vma=False
        )(*args)

    return run
```

```python
import math

import functools

import jax
import jax.numpy as jnp
from jax import lax
from jax.experimental import pallas as pl
from jax.experimental.pallas import tpu as pltpu
from jax.sharding import PartitionSpec as P

HEAD = 64
WINDOW = 128


EPSILON = 1e-06


def extended(value, sides, width):
    for axis, dim in sides:
        size, length = (lax.axis_size(axis), value.shape[dim])
        up = [(i, (i + 1) % size) for i in range(size - 1)]
        down = [(j, i) for i, j in up]
        last = lax.slice_in_dim(value, length - width, length, axis=dim)
        initial = lax.slice_in_dim(value, 0, width, axis=dim)
        before = lax.ppermute(last, axis, up)
        after = lax.ppermute(initial, axis, down)
        value = jnp.concatenate([before, value, after], axis=dim)
    return value


def normalized(tokens, norm_gain):
    values = tokens.astype(jnp.float32)
    scaling = lax.rsqrt(jnp.mean(values * values, axis=-1, keepdims=True) + EPSILON)
    return (values * scaling * norm_gain).astype(jnp.bfloat16)


def folding(normed):

    def add_portions(running, portions, offset):
        return tuple(
            (jnp.dot(normed, portion, preferred_element_type=jnp.float32) for portion in portions)
        )

    return add_portions


def empty_sums(normed, weights):
    return tuple((jnp.zeros((normed.shape[0], weight.shape[1]), jnp.float32) for weight in weights))


def rounded(results):
    return tuple((result.astype(jnp.bfloat16) for result in results))


def gate_product(inner_gate, signal):
    return (inner_gate.astype(jnp.float32) * signal.astype(jnp.float32)).astype(jnp.bfloat16)


def send_edges(key_proj, value_proj, product):
    stacked = jnp.concatenate([key_proj, value_proj], axis=1)
    window_rows = extended(stacked, (("sp", 0),), WINDOW)
    conv_rows = extended(product, (("sp", 0),), 1)
    return (window_rows, conv_rows)


def banded_attention(queries, window_rows, sink_logit, slopes, first_pos, seq_length):
    tok_count = queries.shape[0]
    kv_cols = window_rows.shape[1] // 2
    kv_heads = kv_cols // HEAD
    group_size = queries.shape[1] // (HEAD * kv_heads)
    block_count = tok_count // WINDOW
    query_blocks = queries.reshape(block_count, WINDOW, kv_heads, group_size, HEAD)
    key_rows = window_rows[:, :kv_cols].reshape(block_count + 2, WINDOW, kv_heads, HEAD)
    value_rows = window_rows[:, kv_cols:].reshape(block_count + 2, WINDOW, kv_heads, HEAD)
    key_span = jnp.concatenate([key_rows[:-2], key_rows[1:-1], key_rows[2:]], axis=1)
    value_span = jnp.concatenate([value_rows[:-2], value_rows[1:-1], value_rows[2:]], axis=1)
    scores = jnp.einsum(
        "bqkgd,bskd->bkgqs", query_blocks, key_span, preferred_element_type=jnp.float32
    ) * (1.0 / math.sqrt(HEAD))
    distance = jnp.arange(WINDOW)[:, None] - jnp.arange(3 * WINDOW)[None, :] + WINDOW
    key_pos = (
        first_pos
        - WINDOW
        + WINDOW * jnp.arange(block_count)[:, None]
        + jnp.arange(3 * WINDOW)[None, :]
    )
    inside = (jnp.abs(distance)[None] <= WINDOW) & ((key_pos >= 0) & (key_pos < seq_length))[
        :, None, :
    ]
    scores = scores - slopes.reshape(kv_heads, group_size, 1, 1) * jnp.abs(distance).astype(
        jnp.float32
    )
    scores = jnp.where(inside[:, None, None], scores, -jnp.inf)
    sink_grid = sink_logit.reshape(kv_heads, group_size, 1, 1)
    row_peak = jnp.maximum(jnp.max(scores, axis=-1, keepdims=True), sink_grid)
    weights = jnp.exp(scores - row_peak)
    row_total = jnp.sum(weights, axis=-1, keepdims=True) + jnp.exp(sink_grid - row_peak)
    weighted = jnp.einsum(
        "bkgqs,bskd->bqkgd",
        weights.astype(jnp.bfloat16),
        value_span,
        preferred_element_type=jnp.float32,
    )
    attended = (
        (weighted / row_total.transpose(0, 3, 1, 2, 4))
        .astype(jnp.bfloat16)
        .reshape(tok_count, kv_heads * group_size * HEAD)
    )
    log_total = (
        (row_peak + jnp.log(row_total))[..., 0]
        .transpose(1, 2, 0, 3)
        .reshape(kv_heads * group_size, tok_count)
    )
    return (attended, log_total)


def per_device(
    tokens,
    norm_gain,
    query_weight,
    key_weight,
    value_weight,
    outer_weight,
    inner_weight,
    signal_weight,
    conv_taps,
    sink_logit,
):
    normed = normalized(tokens[0], norm_gain)
    add_portions = folding(normed)
    all_sums = add_portions(
        empty_sums(
            normed,
            (query_weight, key_weight, value_weight, outer_weight, inner_weight, signal_weight),
        ),
        (
            lax.all_gather(query_weight, ("sp", "fs"), axis=0, tiled=True),
            lax.all_gather(key_weight, ("sp", "fs"), axis=0, tiled=True),
            lax.all_gather(value_weight, ("sp", "fs"), axis=0, tiled=True),
            lax.all_gather(outer_weight, ("sp", "fs"), axis=0, tiled=True),
            lax.all_gather(inner_weight, ("sp", "fs"), axis=0, tiled=True),
            lax.all_gather(signal_weight, ("sp", "fs"), axis=0, tiled=True),
        ),
        jnp.int32(0),
    )
    queries, key_proj, value_proj, outer_gate, inner_gate, signal = rounded(all_sums)
    product = gate_product(inner_gate, signal)
    window_rows, conv_rows = send_edges(key_proj, value_proj, product)
    tok_count = normed.shape[0]
    head_local = queries.shape[1] // HEAD
    head_index = lax.axis_index("tp") * head_local + jnp.arange(1, head_local + 1)
    slopes = jnp.exp2(-8.0 * head_index.astype(jnp.float32) / (head_local * lax.axis_size("tp")))
    first_pos = lax.axis_index("sp") * tok_count
    attended, log_total = banded_attention(
        queries, window_rows, sink_logit, slopes, first_pos, tok_count * lax.axis_size("sp")
    )
    mixed_conv = conv_taps[0] * conv_rows[0:tok_count].astype(jnp.float32)
    mixed_conv = mixed_conv + conv_taps[1] * conv_rows[1 : tok_count + 1].astype(jnp.float32)
    mixed_conv = mixed_conv + conv_taps[2] * conv_rows[2 : tok_count + 2].astype(jnp.float32)
    conv_out = (outer_gate.astype(jnp.float32) * mixed_conv).astype(jnp.bfloat16)
    return (attended[None], conv_out[None], log_total[None])


MESH = pl.DeviceIdType.MESH
GROUPS = 3
SPAN = 4
SUBS = 4
FAR = -1e30


def mega_kernel(
    tps,
    tokens,
    gain_in,
    qw,
    kw,
    vw,
    ow,
    iw,
    sw,
    taps_in,
    sinks_in,
    attn_out,
    conv_out,
    log_out,
    toks,
    wts,
    stage_w,
    qs,
    kvs,
    bias,
    prod,
    outer,
    attn_st,
    log_st,
    conv_st,
    acc,
    kv_raw,
    gain_raw,
    gain,
    taps,
    sinks,
    small_sem,
    load_sem,
    stage_sem,
    misc_sem,
    own_sem,
    y_send,
    w_recv,
    pair_send,
    mid_send,
    tok_y_send,
    tok_z_send,
    tok_t_send,
    tok_recv,
    kv_send,
    kv_recv,
    pr_send,
    pr_recv,
    ret_send,
    ret_recv,
    conv_send,
    conv_recv,
):
    s, f, t = lax.axis_index("sp"), lax.axis_index("fs"), lax.axis_index("tp")
    other = 1 - f
    core = lax.rem(t, 2)
    outward = 1 - lax.rem(s, 2)
    partner = s + 2 * outward - 1
    facing = SPAN - 1 - s
    far = SPAN - 1 - partner
    is_mid = (s == 1) | (s == SPAN - 2)
    is_end = jnp.logical_not(is_mid)
    low_half = s < SPAN // 2
    pair, diag, mid = (partner, f, t), (partner, other, t), (facing, f, t)
    across = (s, other, t)
    mate_t, beyond_t = t + 1 - 2 * core, lax.rem(t + 2, tps)
    mate, beyond = (s, f, mate_t), (s, f, beyond_t)
    rows = tokens.shape[0]
    depth = qw.shape[0]
    qcols = qs.shape[2]
    heads = qcols // HEAD
    chans = prod.shape[3]
    both_rows = outer.shape[2]
    blocks = rows // WINDOW
    pad = (prod.shape[2] - both_rows) // 2
    sub = rows // SUBS
    part = sub // tps
    up, down = (s + 1, f, t), (s - 1, f, t)
    has_up, has_down = s < SPAN - 1, s > 0
    own_off = jnp.where(low_half, rows, 0)
    end_off = rows - own_off

    barrier = pltpu.get_barrier_semaphore()
    for peer in (pair, diag, across, mate, beyond):
        pl.semaphore_signal(barrier, inc=1, device_id=peer, device_id_type=MESH)

    @pl.when(is_mid)
    def _():
        pl.semaphore_signal(barrier, inc=1, device_id=mid, device_id_type=MESH)

    def block_rows(blk):
        return pl.ds(pl.multiple_of(blk * depth, 16), depth)

    def loads(g, half, dest, sems):
        if g == 0:
            qc = pl.ds(pl.multiple_of(half * qcols, 128), qcols)
            pairs = [(qw.at[:, qc], dest.at[:, pl.ds(0, qcols)])]
        else:
            c = pl.ds(pl.multiple_of(half * (2 * chans) + (g - 1) * chans, 128), chans)
            pairs = [
                (ref.at[:, c], dest.at[:, pl.ds(i * chans, chans)])
                for i, ref in enumerate((iw, sw, ow))
            ]
        return [
            pltpu.make_async_copy(a, b, sems.at[g, i]) for i, (a, b) in enumerate(pairs)
        ]

    mine = s * 2 + f
    theirs = s * 2 + other
    own_loads = [loads(g, f, wts.at[g, block_rows(mine)], load_sem) for g in range(GROUPS)]
    out_loads = [loads(g, other, stage_w.at[g], stage_sem) for g in range(GROUPS)]
    small = [
        pltpu.make_async_copy(a, b, small_sem.at[i])
        for i, (a, b) in enumerate(
            (
                (kw, kv_raw.at[0]),
                (vw, kv_raw.at[1]),
                (gain_in, gain_raw),
                (taps_in, taps),
                (sinks_in, sinks),
            )
        )
    ]
    tok_load = pltpu.make_async_copy(tokens, toks.at[f], misc_sem.at[0])

    def begin(copies):
        for c in copies:
            c.start()

    def finish(copies):
        for c in copies:
            c.wait()

    begin(small[:2] + out_loads[0] + own_loads[0] + small[2:])
    tok_load.start()
    begin(out_loads[1] + own_loads[1] + out_loads[2] + own_loads[2])

    def remote(src, dst, send, recv, peer):
        return pltpu.make_async_remote_copy(
            src_ref=src,
            dst_ref=dst,
            send_sem=send,
            recv_sem=recv,
            device_id=peer,
            device_id_type=MESH,
        )

    def y_copy(g):
        return remote(
            stage_w.at[g], wts.at[g, block_rows(mine)], y_send.at[g], w_recv.at[g, mine], across
        )

    def block_copy(g, blk, sends, peer):
        at = wts.at[g, block_rows(blk)]
        return remote(at, at, sends.at[g, blk], w_recv.at[g, blk], peer)

    def to_pair(g, blk):
        return block_copy(g, blk, pair_send, pair)

    def to_mid(g, blk):
        return block_copy(g, blk, mid_send, mid)

    def arrived(g, blk):
        to_pair(g, blk).wait_recv()

    def slot_of(k):
        return (other, 2 + f, 2 + other)[k]

    def piece(slot, j, q):
        return toks.at[slot, pl.ds(pl.multiple_of(j * sub + q * part, 16), part)]

    def tok_y(k, j):
        slot = f if k == 0 else 2 + f
        at = piece(slot, j, beyond_t if k == 2 else t)
        kind = 2 if k == 2 else 0
        return remote(at, at, tok_y_send.at[k, j], tok_recv.at[2 if k else 0, j, kind], across)

    def tok_z(k, j):
        seq = f if k == 0 else other
        return remote(
            piece(seq, j, t),
            piece(2 + seq, j, t),
            tok_z_send.at[k, j],
            tok_recv.at[1 + k, j, 0],
            pair,
        )

    def tok_share(k, j, kind):
        q = beyond_t if kind == 2 else t
        at = piece(slot_of(k), j, q)
        return remote(
            at, at, tok_t_send.at[k, j, kind], tok_recv.at[k, j, kind + 1],
            beyond if kind == 1 else mate,
        )

    def tok_wait(k, j, kind):
        at = piece(slot_of(k), j, t)
        remote(at, at, tok_t_send.at[k, j, 0], tok_recv.at[k, j, kind], mate).wait_recv()

    def take(k, j):
        tok_wait(k, j, 0)
        if k < 2 or j >= SUBS // 2:
            tok_share(k, j, 1).start()
        tok_share(k, j, 0).start()
        if k == 1 and j < SUBS // 2:
            tok_y(1, j).start()

    def hand(k, j):
        tok_wait(k, j, 2)
        tok_share(k, j, 2).start()
        if k == 1 and j < SUBS // 2:
            tok_y(2, j).start()

    def have(k, j):
        tok_wait(k, j, 1)
        tok_wait(k, j, 3)

    def norm_own():
        @pl.loop(0, blocks)
        def _(b):
            at = pl.ds(pl.multiple_of(b * WINDOW, WINDOW), WINDOW)
            values = toks[f, at, :].astype(jnp.float32)
            scaling = lax.rsqrt(jnp.mean(values * values, axis=-1, keepdims=True) + EPSILON)
            toks[f, at, :] = (values * scaling * gain[...]).astype(jnp.bfloat16)

    mm_rows = rows // 2

    def make_bias():
        key = lax.broadcasted_iota(jnp.int32, (3 * WINDOW, WINDOW), 0)
        query = lax.broadcasted_iota(jnp.int32, (3 * WINDOW, WINDOW), 1)
        away = jnp.abs(query - key + WINDOW)
        for h in range(heads):
            index = (t * (2 * heads) + f * heads + h + 1).astype(jnp.float32)
            slope = jnp.exp2(jnp.full((1, WINDOW), -8.0 / (2 * heads * tps), jnp.float32) * index)
            bias[h] = jnp.where(away <= WINDOW, -slope * away.astype(jnp.float32), FAR)

    half_k = depth * SPAN
    near_k = pl.multiple_of(jnp.where(low_half, 0, half_k), 128)
    far_k = pl.multiple_of(half_k - near_k, 128)

    def partial(g, slot, at, k_off):
        return jnp.dot(
            toks[slot, pl.ds(at, mm_rows), pl.ds(k_off, half_k)],
            wts[g, pl.ds(k_off, half_k), :],
            preferred_element_type=jnp.float32,
        )

    def sums(g, slot):
        return slot if g == 0 else slot + 4 * g - 2

    def near(g, slot, lo=0, hi=2):
        @pl.loop(lo, hi)
        def _(b):
            at = pl.multiple_of(b * mm_rows, WINDOW)
            acc[sums(g, slot), pl.ds(at, mm_rows), :] = partial(g, slot, at, near_k)

    def total(g, slot, at):
        return acc[sums(g, slot), pl.ds(at, mm_rows), :] + partial(g, slot, at, far_k)

    def project_qkv(seq):
        @pl.loop(0, 2)
        def _(b):
            at = pl.multiple_of(b * mm_rows, WINDOW)
            out = total(0, seq, at)
            qs[seq, pl.ds(at, mm_rows), :] = out[:, :qcols].astype(jnp.bfloat16)
            kvs[seq, pl.ds(at + WINDOW, mm_rows), :] = out[:, qcols:].astype(jnp.bfloat16)

    kv_len = kvs.shape[1]

    def kv_copies(seq, slot):
        ref = kvs.at[seq]
        climb = remote(
            ref.at[pl.ds(kv_len - 2 * WINDOW, WINDOW)],
            ref.at[pl.ds(0, WINDOW)],
            kv_send.at[slot, 0],
            kv_recv.at[slot, 0],
            up,
        )
        fall = remote(
            ref.at[pl.ds(WINDOW, WINDOW)],
            ref.at[pl.ds(kv_len - WINDOW, WINDOW)],
            kv_send.at[slot, 1],
            kv_recv.at[slot, 1],
            down,
        )
        return climb, fall

    def kv_start(seq, slot):
        climb, fall = kv_copies(seq, slot)
        blank = jnp.zeros((WINDOW, 2 * HEAD), jnp.bfloat16)

        @pl.when(has_up)
        def _():
            climb.start()

        @pl.when(has_down)
        def _():
            fall.start()

        @pl.when(jnp.logical_not(has_up))
        def _():
            kvs[seq, pl.ds(kv_len - WINDOW, WINDOW), :] = blank

        @pl.when(jnp.logical_not(has_down))
        def _():
            kvs[seq, pl.ds(0, WINDOW), :] = blank

    def kv_wait(seq, slot):
        climb, fall = kv_copies(seq, slot)

        @pl.when(has_up)
        def _():
            climb.wait_send()
            fall.wait_recv()

        @pl.when(has_down)
        def _():
            fall.wait_send()
            climb.wait_recv()

    def attend(seq, first, count, step=1):
        @pl.loop(0, count)
        def _(i):
            b = first + i * step
            at = pl.multiple_of(b * WINDOW, WINDOW)
            kv = kvs[seq, pl.ds(at, 3 * WINDOW), :]
            keys = kv[:, :HEAD]
            values_t = kv.astype(jnp.float32).T[HEAD:, :].astype(jnp.bfloat16)
            queries = qs[seq, pl.ds(at, WINDOW), :]
            low = jnp.where((b == 0) & (s == 0), FAR, 0.0)
            high = jnp.where((b == blocks - 1) & (s == SPAN - 1), FAR, 0.0)
            outs = []
            for h in range(heads):
                query = queries[:, h * HEAD : (h + 1) * HEAD]
                scores = lax.dot_general(
                    keys, query, (((1,), (1,)), ((), ())), preferred_element_type=jnp.float32
                )
                scores = scores * (1.0 / math.sqrt(HEAD)) + bias[h]
                scores = jnp.concatenate(
                    [
                        scores[:WINDOW] + low,
                        scores[WINDOW : 2 * WINDOW],
                        scores[2 * WINDOW :] + high,
                    ],
                    axis=0,
                )
                sink = sinks[f * heads + h]
                peak = jnp.maximum(jnp.max(scores, axis=0, keepdims=True), sink)
                weights = jnp.exp(scores - peak)
                total = jnp.sum(weights, axis=0, keepdims=True) + jnp.exp(sink - peak)
                mixed = jnp.dot(
                    values_t, weights.astype(jnp.bfloat16), preferred_element_type=jnp.float32
                )
                outs.append(mixed / total)
                log_st[seq, pl.ds(h, 1), pl.ds(at, WINDOW)] = peak + jnp.log(total)
            stacked = jnp.concatenate(outs, axis=0)
            attn_st[seq, pl.ds(at, WINDOW), :] = stacked.T.astype(jnp.bfloat16)

    half_cols = pl.ds(pl.multiple_of(f * qcols, 128), qcols)

    def attn_return(own):
        seq = f if own else other
        pairs = [
            (attn_st.at[seq], attn_out.at[:, half_cols]),
            (log_st.at[seq], log_out.at[f]),
        ]
        if own:
            return [pltpu.make_async_copy(a, b, misc_sem.at[1 + i]) for i, (a, b) in enumerate(pairs)]
        return [
            remote(a, b, ret_send.at[i], ret_recv.at[i], across) for i, (a, b) in enumerate(pairs)
        ]

    def conv_cols(g):
        return pl.ds(pl.multiple_of(f * (2 * chans) + (g - 1) * chans, 128), chans)

    split = mm_rows - pad

    def conv_return(g, own_seq, own_rows, tail=0):
        seq = f if own_seq else other
        off = own_off if own_rows else end_off
        lo, count = 0, rows
        if not own_seq and not own_rows:
            lo, count = (split, rows - split) if tail else (0, split)
        src = conv_st.at[g - 1, seq, pl.ds(pl.multiple_of(off + lo, pad), count)]
        dst = conv_out.at[pl.ds(lo, count), conv_cols(g)]
        if own_seq and own_rows:
            return pltpu.make_async_copy(src, dst, own_sem.at[g - 1])
        if own_seq:
            return remote(src, dst, conv_send.at[g - 1, 0], conv_recv.at[g - 1, 0], pair)
        if own_rows:
            return remote(src, dst, conv_send.at[g - 1, 1], conv_recv.at[g - 1, 1], across)
        return remote(
            src, dst, conv_send.at[g - 1, 2 + tail], conv_recv.at[g - 1, 1 + tail], diag
        )

    def project_conv(g, seq, own_rows, lo=0, hi=2):
        slot, off = (seq, own_off) if own_rows else (2 + seq, end_off)

        @pl.loop(lo, hi)
        def _(b):
            at = pl.multiple_of(b * mm_rows, WINDOW)
            to = pl.multiple_of(off + b * mm_rows, WINDOW)
            out = total(g, slot, at)
            inner = out[:, :chans].astype(jnp.bfloat16).astype(jnp.float32)
            signal = out[:, chans : 2 * chans].astype(jnp.bfloat16).astype(jnp.float32)
            prod[g - 1, seq, pl.ds(to + pad, mm_rows), :] = (inner * signal).astype(jnp.bfloat16)
            outer[g - 1, seq, pl.ds(to, mm_rows), :] = out[:, 2 * chans :].astype(jnp.bfloat16)

    def pr_copies(g, seq, slot):
        ref = prod.at[g - 1, seq]
        climb = remote(
            ref.at[pl.ds(both_rows, pad)],
            ref.at[pl.ds(0, pad)],
            pr_send.at[g - 1, slot],
            pr_recv.at[g - 1, slot],
            mid,
        )
        fall = remote(
            ref.at[pl.ds(pad, pad)],
            ref.at[pl.ds(both_rows + pad, pad)],
            pr_send.at[g - 1, slot],
            pr_recv.at[g - 1, slot],
            mid,
        )
        return climb, fall

    def pr_start(g, seq, slot):
        climb, fall = pr_copies(g, seq, slot)
        blank = jnp.zeros((pad, chans), jnp.bfloat16)

        @pl.when(low_half)
        def _():
            climb.start()
            prod[g - 1, seq, pl.ds(0, pad), :] = blank

        @pl.when(jnp.logical_not(low_half))
        def _():
            fall.start()
            prod[g - 1, seq, pl.ds(both_rows + pad, pad), :] = blank

    def pr_wait(g, seq, slot):
        climb, fall = pr_copies(g, seq, slot)

        @pl.when(low_half)
        def _():
            climb.wait_send()
            fall.wait_recv()

        @pl.when(jnp.logical_not(low_half))
        def _():
            fall.wait_send()
            climb.wait_recv()

    def mix(g, seq, own_rows, lo=0, hi=None):
        count = (rows if hi is None else hi) - lo
        off = pl.multiple_of((own_off if own_rows else end_off) + lo, pad)
        tap = taps[:, conv_cols(g)]
        size = count + 2 * pad
        full = prod[g - 1, seq, pl.ds(off, size), :].astype(jnp.float32)
        before = pltpu.roll(full, 1, 0)[pad : pad + count]
        after = pltpu.roll(full, size - 1, 0)[pad : pad + count]
        mixed = tap[0:1] * before + tap[1:2] * full[pad : pad + count] + tap[2:3] * after
        gate = outer[g - 1, seq, pl.ds(off, count), :].astype(jnp.float32)
        conv_st[g - 1, seq, pl.ds(off, count), :] = (gate * mixed).astype(jnp.bfloat16)

    finish(small[:2])
    keys0, vals0 = kv_raw[0], kv_raw[1]
    halves = [
        jnp.concatenate([w[:, i * HEAD : (i + 1) * HEAD] for w in (keys0, vals0)], axis=1)
        for i in range(2)
    ]
    first = f == 0
    stage_w[0, :, pl.ds(qcols, 2 * HEAD)] = jnp.where(first, halves[1], halves[0])
    wts[0, block_rows(mine), pl.ds(qcols, 2 * HEAD)] = jnp.where(first, halves[0], halves[1])

    pl.semaphore_wait(barrier, jnp.where(is_mid, 6, 5))

    finish(own_loads[0])
    to_pair(0, mine).start()

    @pl.when(is_mid)
    def _():
        to_mid(0, mine).start()

    finish(out_loads[0])
    y_copy(0).start()
    finish(own_loads[1])

    @pl.when(is_mid)
    def _():
        to_mid(1, mine).start()

    finish(small[2:])
    for i in range(gain_raw.shape[0]):
        gain[:, i * 128 : (i + 1) * 128] = gain_raw[i : i + 1, :]
    tok_load.wait()
    norm_own()
    for j in range(SUBS):
        tok_y(0, j).start()
    finish(out_loads[1] + out_loads[2] + own_loads[2])
    y_copy(1).start()
    y_copy(2).start()

    def relay(g, blk, onward):
        arrived(g, blk)
        onward(g, blk).start()

    pt = [partner * 2 + f, partner * 2 + other]
    ct = [facing * 2 + f, facing * 2 + other]
    ft = [far * 2 + f, far * 2 + other]

    def end_program():
        tok_z(0, 0).start()
        make_bias()
        relay(0, theirs, to_pair)
        tok_z(0, 1).start()
        to_pair(1, mine).start()
        tok_z(0, 2).start()
        take(0, 0)
        take(0, 1)
        for blk in pt:
            arrived(0, blk)
        near(0, f)
        hand(0, 0)
        take(0, 2)
        hand(0, 1)
        take(0, 3)
        hand(0, 2)
        relay(1, theirs, to_pair)
        tok_z(0, 3).start()
        hand(0, 3)
        for j in range(SUBS):
            have(0, j)
        near(0, other)
        for blk in ct + ft:
            arrived(0, blk)
        project_qkv(f)
        kv_start(f, 0)
        project_qkv(other)
        kv_start(other, 1)
        to_pair(2, mine).start()
        relay(2, theirs, to_pair)
        tok_z(1, 2).start()
        tok_z(1, 3).start()
        attend(f, 1, blocks - 2)
        attend(other, 1, blocks - 2)
        kv_wait(f, 0)
        attend(f, 0, 2, blocks - 1)
        begin(attn_return(True))
        kv_wait(other, 1)
        attend(other, 0, 2, blocks - 1)
        begin(attn_return(False))
        for g in (1, 2):
            conv_return(g, True, False).wait_recv()
            conv_return(g, False, False).wait_recv()
            conv_return(g, False, False, 1).wait_recv()
        for g in range(GROUPS):
            to_pair(g, mine).wait_send()
            to_pair(g, theirs).wait_send()
        for j in range(SUBS):
            tok_z(0, j).wait_send()
        for j in range(SUBS // 2, SUBS):
            tok_z(1, j).wait_send()

    def conv_own(g, own_seq):
        seq, slot = (f, 0) if own_seq else (other, 1)
        project_conv(g, seq, True)
        pr_start(g, seq, slot)

    def conv_close(g, own_seq):
        seq, slot = (f, 0) if own_seq else (other, 1)
        pr_wait(g, seq, slot)
        mix(g, seq, True)
        conv_return(g, own_seq, True).start()

    def conv_end(g):
        project_conv(g, f, False)
        mix(g, f, False)
        conv_return(g, True, False).start()

    def conv_end_head(g):
        project_conv(g, other, False, 0, 1)
        mix(g, other, False, 0, split)
        conv_return(g, False, False).start()

    def conv_end_tail(g):
        project_conv(g, other, False, 1, 2)
        mix(g, other, False, split, rows)
        conv_return(g, False, False, 1).start()

    def mid_program():
        half = (blocks - 2) // 2
        make_bias()
        relay(0, theirs, to_mid)
        to_pair(0, theirs).start()
        relay(0, ct[0], to_pair)
        relay(0, pt[0], to_mid)
        take(0, 0)
        take(0, 1)
        relay(0, ct[1], to_pair)
        relay(0, pt[1], to_mid)
        to_mid(2, mine).start()
        near(0, f)
        hand(0, 0)
        relay(0, ft[0], to_pair)
        take(0, 2)
        hand(0, 1)
        take(0, 3)
        take(1, 0)
        relay(0, ft[1], to_pair)
        project_qkv(f)
        kv_start(f, 0)
        hand(0, 2)
        take(1, 1)
        relay(1, pt[0], to_mid)
        attend(f, 1, half)
        relay(1, theirs, to_mid)
        hand(0, 3)
        for j in range(SUBS):
            have(0, j)
        near(0, other)
        project_qkv(other)
        kv_start(other, 1)
        relay(2, theirs, to_mid)
        take(1, 2)
        attend(f, 1 + half, half)
        hand(1, 0)
        relay(1, pt[1], to_mid)
        attend(other, 1, half)
        near(1, f)
        hand(1, 1)
        near(1, other)
        take(1, 3)
        attend(other, 1 + half, half)
        kv_wait(f, 0)
        attend(f, 0, 2, blocks - 1)
        begin(attn_return(True))
        hand(1, 2)
        take(2, 0)
        take(2, 1)
        relay(2, pt[0], to_mid)
        kv_wait(other, 1)
        attend(other, 0, 2, blocks - 1)
        begin(attn_return(False))
        for blk in ct + ft:
            arrived(1, blk)
        conv_own(1, True)
        hand(1, 3)
        hand(2, 0)
        conv_own(1, False)
        relay(2, pt[1], to_mid)
        for j in range(SUBS):
            have(1, j)
        near(1, 2 + f)
        conv_end(1)
        near(2, 2 + f)
        hand(2, 1)
        conv_close(1, True)
        for j in range(SUBS // 2):
            have(2, j)
        near(1, 2 + other, 0, 1)
        conv_end_head(1)
        take(2, 2)
        near(2, f)
        near(2, other)
        near(2, 2 + other, 0, 1)
        for blk in ct + ft:
            arrived(2, blk)
        conv_own(2, True)
        take(2, 3)
        conv_own(2, False)
        conv_end(2)
        hand(2, 2)
        conv_end_head(2)
        conv_close(2, True)
        hand(2, 3)
        for j in range(SUBS // 2, SUBS):
            have(2, j)
        near(1, 2 + other, 1, 2)
        conv_end_tail(1)
        near(2, 2 + other, 1, 2)
        conv_end_tail(2)
        conv_close(1, False)
        conv_close(2, False)
        for g in (1, 2):
            conv_return(g, False, True).wait_recv()
            conv_return(g, True, True).wait()
            conv_return(g, False, True).wait_send()
            conv_return(g, True, False).wait_send()
            conv_return(g, False, False).wait_send()
            conv_return(g, False, False, 1).wait_send()
        for blk in [mine, theirs] + ct + ft:
            to_pair(0, blk).wait_send()
        for g in range(GROUPS):
            for blk in [mine, theirs] + pt:
                to_mid(g, blk).wait_send()
        for j in range(SUBS // 2):
            tok_y(1, j).wait_send()
            tok_y(2, j).wait_send()
        for k in (1, 2):
            for j in range(SUBS):
                for kind in range(3):
                    if k < 2 or j >= SUBS // 2 or kind != 1:
                        tok_share(k, j, kind).wait_send()

    pl.when(is_end)(end_program)
    pl.when(is_mid)(mid_program)

    for g in range(GROUPS):
        y_copy(g).wait_send()
    for j in range(SUBS):
        tok_y(0, j).wait_send()
        for kind in range(3):
            tok_share(0, j, kind).wait_send()
    for own in (True, False):
        finish(attn_return(own))


def fused_device(
    tps,
    tokens,
    norm_gain,
    query_weight,
    key_weight,
    value_weight,
    outer_weight,
    inner_weight,
    signal_weight,
    conv_taps,
    sink_logit,
):
    rows, width = tokens.shape[1:]
    depth, local = query_weight.shape
    qcols = local // 2
    heads = qcols // HEAD
    chans = outer_weight.shape[1] // 4
    head_local = 2 * heads
    group_cols = qcols + 2 * HEAD
    pad = 16
    bf, f32 = jnp.bfloat16, jnp.float32
    dma = pltpu.SemaphoreType.DMA
    hbm = pl.BlockSpec(memory_space=pltpu.HBM)
    anyspace = pl.BlockSpec(memory_space=pl.ANY)
    attended, conv, logs = pl.pallas_call(
        functools.partial(mega_kernel, tps),
        out_shape=(
            jax.ShapeDtypeStruct((rows, local), bf),
            jax.ShapeDtypeStruct((rows, 4 * chans), bf),
            jax.ShapeDtypeStruct((2, heads, rows), f32),
        ),
        in_specs=[hbm] * 10,
        out_specs=(anyspace, anyspace, anyspace),
        scratch_shapes=[
            pltpu.VMEM((4, rows, width), bf),
            pltpu.VMEM((GROUPS, width, group_cols), bf),
            pltpu.VMEM((GROUPS, depth, group_cols), bf),
            pltpu.VMEM((2, rows, qcols), bf),
            pltpu.VMEM((2, rows + 2 * WINDOW, 2 * HEAD), bf),
            pltpu.VMEM((heads, 3 * WINDOW, WINDOW), f32),
            pltpu.VMEM((2, 2, 2 * rows + 2 * pad, chans), bf),
            pltpu.VMEM((2, 2, 2 * rows, chans), bf),
            pltpu.VMEM((2, rows, qcols), bf),
            pltpu.VMEM((2, heads, rows), f32),
            pltpu.VMEM((2, 2, 2 * rows, chans), bf),
            pltpu.VMEM((10, rows, group_cols), f32),
            pltpu.VMEM((2, depth, 2 * HEAD), bf),
            pltpu.VMEM((width // 128, 128), f32),
            pltpu.VMEM((1, width), f32),
            pltpu.VMEM((3, 4 * chans), f32),
            pltpu.SMEM((head_local,), f32),
            dma((5,)),
            dma((GROUPS, 3)),
            dma((GROUPS, 3)),
            dma((3,)),
            dma((2,)),
            dma((GROUPS,)),
            dma((GROUPS, 2 * SPAN)),
            dma((GROUPS, 2 * SPAN)),
            dma((GROUPS, 2 * SPAN)),
            dma((3, SUBS)),
            dma((2, SUBS)),
            dma((3, SUBS, 3)),
            dma((3, SUBS, 4)),
            dma((2, 2)),
            dma((2, 2)),
            dma((2, 2)),
            dma((2, 2)),
            dma((2,)),
            dma((2,)),
            dma((2, 4)),
            dma((2, 3)),
        ],
        compiler_params=pltpu.CompilerParams(
            collective_id=0, has_side_effects=True, vmem_limit_bytes=67043328
        ),
    )(
        tokens[0],
        norm_gain.reshape(width // 128, 128),
        query_weight,
        key_weight,
        value_weight,
        outer_weight,
        inner_weight,
        signal_weight,
        conv_taps,
        sink_logit,
    )
    return (attended[None], conv[None], logs.reshape(1, head_local, rows))


def fits(mesh, args):
    tokens, query_weight, key_weight, outer_weight = (args[i] for i in (0, 2, 3, 5))
    sp, fs, tp = (mesh.shape[a] for a in ("sp", "fs", "tp"))
    rows = tokens.shape[1] // sp
    return (
        fs == 2
        and sp == SPAN
        and tokens.shape[0] == fs
        and tp == 4
        and rows % (2 * WINDOW) == 0
        and rows // WINDOW % 2 == 0
        and rows % (16 * SUBS * tp) == 0
        and key_weight.shape[1] == 2 * HEAD * tp
        and query_weight.shape[1] % (256 * tp) == 0
        and outer_weight.shape[1] == 512 * tp
        and query_weight.shape[1] == 512 * tp
        and query_weight.shape[0] % (16 * sp * fs) == 0
    )


def solution(mesh):
    in_specs = (
        P("fs", "sp", None),
        P(),
        P(("sp", "fs"), "tp"),
        P(("sp", "fs"), "tp"),
        P(("sp", "fs"), "tp"),
        P(("sp", "fs"), "tp"),
        P(("sp", "fs"), "tp"),
        P(("sp", "fs"), "tp"),
        P(None, "tp"),
        P("tp"),
    )
    out_specs = (P("fs", "sp", "tp"), P("fs", "sp", "tp"), P("fs", "tp", "sp"))

    def run(*args):
        body = per_device
        if fits(mesh, args):
            body = functools.partial(fused_device, mesh.shape["tp"])
        return jax.shard_map(
            body, mesh=mesh, in_specs=in_specs, out_specs=out_specs, check_vma=False
        )(*args)

    return run
```

```python
import math

import functools

import jax
import jax.numpy as jnp
from jax import lax
from jax.experimental import pallas as pl
from jax.experimental.pallas import tpu as pltpu
from jax.sharding import PartitionSpec as P

HEAD = 64
WINDOW = 128


EPSILON = 1e-06


def extended(value, sides, width):
    for axis, dim in sides:
        size, length = (lax.axis_size(axis), value.shape[dim])
        up = [(i, (i + 1) % size) for i in range(size - 1)]
        down = [(j, i) for i, j in up]
        last = lax.slice_in_dim(value, length - width, length, axis=dim)
        initial = lax.slice_in_dim(value, 0, width, axis=dim)
        before = lax.ppermute(last, axis, up)
        after = lax.ppermute(initial, axis, down)
        value = jnp.concatenate([before, value, after], axis=dim)
    return value


def normalized(tokens, norm_gain):
    values = tokens.astype(jnp.float32)
    scaling = lax.rsqrt(jnp.mean(values * values, axis=-1, keepdims=True) + EPSILON)
    return (values * scaling * norm_gain).astype(jnp.bfloat16)


def folding(normed):

    def add_portions(running, portions, offset):
        return tuple(
            (jnp.dot(normed, portion, preferred_element_type=jnp.float32) for portion in portions)
        )

    return add_portions


def empty_sums(normed, weights):
    return tuple((jnp.zeros((normed.shape[0], weight.shape[1]), jnp.float32) for weight in weights))


def rounded(results):
    return tuple((result.astype(jnp.bfloat16) for result in results))


def gate_product(inner_gate, signal):
    return (inner_gate.astype(jnp.float32) * signal.astype(jnp.float32)).astype(jnp.bfloat16)


def send_edges(key_proj, value_proj, product):
    stacked = jnp.concatenate([key_proj, value_proj], axis=1)
    window_rows = extended(stacked, (("sp", 0),), WINDOW)
    conv_rows = extended(product, (("sp", 0),), 1)
    return (window_rows, conv_rows)


def banded_attention(queries, window_rows, sink_logit, slopes, first_pos, seq_length):
    tok_count = queries.shape[0]
    kv_cols = window_rows.shape[1] // 2
    kv_heads = kv_cols // HEAD
    group_size = queries.shape[1] // (HEAD * kv_heads)
    block_count = tok_count // WINDOW
    query_blocks = queries.reshape(block_count, WINDOW, kv_heads, group_size, HEAD)
    key_rows = window_rows[:, :kv_cols].reshape(block_count + 2, WINDOW, kv_heads, HEAD)
    value_rows = window_rows[:, kv_cols:].reshape(block_count + 2, WINDOW, kv_heads, HEAD)
    key_span = jnp.concatenate([key_rows[:-2], key_rows[1:-1], key_rows[2:]], axis=1)
    value_span = jnp.concatenate([value_rows[:-2], value_rows[1:-1], value_rows[2:]], axis=1)
    scores = jnp.einsum(
        "bqkgd,bskd->bkgqs", query_blocks, key_span, preferred_element_type=jnp.float32
    ) * (1.0 / math.sqrt(HEAD))
    distance = jnp.arange(WINDOW)[:, None] - jnp.arange(3 * WINDOW)[None, :] + WINDOW
    key_pos = (
        first_pos
        - WINDOW
        + WINDOW * jnp.arange(block_count)[:, None]
        + jnp.arange(3 * WINDOW)[None, :]
    )
    inside = (jnp.abs(distance)[None] <= WINDOW) & ((key_pos >= 0) & (key_pos < seq_length))[
        :, None, :
    ]
    scores = scores - slopes.reshape(kv_heads, group_size, 1, 1) * jnp.abs(distance).astype(
        jnp.float32
    )
    scores = jnp.where(inside[:, None, None], scores, -jnp.inf)
    sink_grid = sink_logit.reshape(kv_heads, group_size, 1, 1)
    row_peak = jnp.maximum(jnp.max(scores, axis=-1, keepdims=True), sink_grid)
    weights = jnp.exp(scores - row_peak)
    row_total = jnp.sum(weights, axis=-1, keepdims=True) + jnp.exp(sink_grid - row_peak)
    weighted = jnp.einsum(
        "bkgqs,bskd->bqkgd",
        weights.astype(jnp.bfloat16),
        value_span,
        preferred_element_type=jnp.float32,
    )
    attended = (
        (weighted / row_total.transpose(0, 3, 1, 2, 4))
        .astype(jnp.bfloat16)
        .reshape(tok_count, kv_heads * group_size * HEAD)
    )
    log_total = (
        (row_peak + jnp.log(row_total))[..., 0]
        .transpose(1, 2, 0, 3)
        .reshape(kv_heads * group_size, tok_count)
    )
    return (attended, log_total)


def per_device(
    tokens,
    norm_gain,
    query_weight,
    key_weight,
    value_weight,
    outer_weight,
    inner_weight,
    signal_weight,
    conv_taps,
    sink_logit,
):
    normed = normalized(tokens[0], norm_gain)
    add_portions = folding(normed)
    all_sums = add_portions(
        empty_sums(
            normed,
            (query_weight, key_weight, value_weight, outer_weight, inner_weight, signal_weight),
        ),
        (
            lax.all_gather(query_weight, ("sp", "fs"), axis=0, tiled=True),
            lax.all_gather(key_weight, ("sp", "fs"), axis=0, tiled=True),
            lax.all_gather(value_weight, ("sp", "fs"), axis=0, tiled=True),
            lax.all_gather(outer_weight, ("sp", "fs"), axis=0, tiled=True),
            lax.all_gather(inner_weight, ("sp", "fs"), axis=0, tiled=True),
            lax.all_gather(signal_weight, ("sp", "fs"), axis=0, tiled=True),
        ),
        jnp.int32(0),
    )
    queries, key_proj, value_proj, outer_gate, inner_gate, signal = rounded(all_sums)
    product = gate_product(inner_gate, signal)
    window_rows, conv_rows = send_edges(key_proj, value_proj, product)
    tok_count = normed.shape[0]
    head_local = queries.shape[1] // HEAD
    head_index = lax.axis_index("tp") * head_local + jnp.arange(1, head_local + 1)
    slopes = jnp.exp2(-8.0 * head_index.astype(jnp.float32) / (head_local * lax.axis_size("tp")))
    first_pos = lax.axis_index("sp") * tok_count
    attended, log_total = banded_attention(
        queries, window_rows, sink_logit, slopes, first_pos, tok_count * lax.axis_size("sp")
    )
    mixed_conv = conv_taps[0] * conv_rows[0:tok_count].astype(jnp.float32)
    mixed_conv = mixed_conv + conv_taps[1] * conv_rows[1 : tok_count + 1].astype(jnp.float32)
    mixed_conv = mixed_conv + conv_taps[2] * conv_rows[2 : tok_count + 2].astype(jnp.float32)
    conv_out = (outer_gate.astype(jnp.float32) * mixed_conv).astype(jnp.bfloat16)
    return (attended[None], conv_out[None], log_total[None])


MESH = pl.DeviceIdType.MESH
GROUPS = 3
SPAN = 4
SUBS = 4
FAR = -1e30


def mega_kernel(
    tps,
    tokens,
    gain_in,
    qw,
    kw,
    vw,
    ow,
    iw,
    sw,
    taps_in,
    sinks_in,
    attn_out,
    conv_out,
    log_out,
    toks,
    wts,
    stage_w,
    qs,
    kvs,
    bias,
    prod,
    outer,
    attn_st,
    log_st,
    conv_st,
    acc,
    kv_raw,
    gain_raw,
    gain,
    taps,
    sinks,
    small_sem,
    load_sem,
    stage_sem,
    misc_sem,
    own_sem,
    y_send,
    w_recv,
    pair_send,
    mid_send,
    tok_y_send,
    tok_z_send,
    tok_t_send,
    tok_recv,
    kv_send,
    kv_recv,
    pr_send,
    pr_recv,
    ret_send,
    ret_recv,
    conv_send,
    conv_recv,
):
    s, f, t = lax.axis_index("sp"), lax.axis_index("fs"), lax.axis_index("tp")
    other = 1 - f
    core = lax.rem(t, 2)
    outward = 1 - lax.rem(s, 2)
    partner = s + 2 * outward - 1
    facing = SPAN - 1 - s
    far = SPAN - 1 - partner
    is_mid = (s == 1) | (s == SPAN - 2)
    is_end = jnp.logical_not(is_mid)
    low_half = s < SPAN // 2
    pair, diag, mid = (partner, f, t), (partner, other, t), (facing, f, t)
    across = (s, other, t)
    mate_t, beyond_t = t + 1 - 2 * core, lax.rem(t + 2, tps)
    mate, beyond = (s, f, mate_t), (s, f, beyond_t)
    rows = tokens.shape[0]
    depth = qw.shape[0]
    qcols = qs.shape[2]
    heads = qcols // HEAD
    chans = prod.shape[3]
    both_rows = outer.shape[2]
    blocks = rows // WINDOW
    pad = (prod.shape[2] - both_rows) // 2
    sub = rows // SUBS
    part = sub // tps
    up, down = (s + 1, f, t), (s - 1, f, t)
    has_up, has_down = s < SPAN - 1, s > 0
    own_off = jnp.where(low_half, rows, 0)
    end_off = rows - own_off

    barrier = pltpu.get_barrier_semaphore()
    for peer in (pair, diag, across, mate, beyond):
        pl.semaphore_signal(barrier, inc=1, device_id=peer, device_id_type=MESH)

    @pl.when(is_mid)
    def _():
        pl.semaphore_signal(barrier, inc=1, device_id=mid, device_id_type=MESH)

    def block_rows(blk):
        return pl.ds(pl.multiple_of(blk * depth, 16), depth)

    def loads(g, half, dest, sems):
        if g == 0:
            qc = pl.ds(pl.multiple_of(half * qcols, 128), qcols)
            pairs = [(qw.at[:, qc], dest.at[:, pl.ds(0, qcols)])]
        else:
            c = pl.ds(pl.multiple_of(half * (2 * chans) + (g - 1) * chans, 128), chans)
            pairs = [
                (ref.at[:, c], dest.at[:, pl.ds(i * chans, chans)])
                for i, ref in enumerate((iw, sw, ow))
            ]
        return [
            pltpu.make_async_copy(a, b, sems.at[g, i]) for i, (a, b) in enumerate(pairs)
        ]

    mine = s * 2 + f
    theirs = s * 2 + other
    own_loads = [loads(g, f, wts.at[g, block_rows(mine)], load_sem) for g in range(GROUPS)]
    out_loads = [loads(g, other, stage_w.at[g], stage_sem) for g in range(GROUPS)]
    small = [
        pltpu.make_async_copy(a, b, small_sem.at[i])
        for i, (a, b) in enumerate(
            (
                (kw, kv_raw.at[0]),
                (vw, kv_raw.at[1]),
                (gain_in, gain_raw),
                (taps_in, taps),
                (sinks_in, sinks),
            )
        )
    ]
    tok_load = pltpu.make_async_copy(tokens, toks.at[f], misc_sem.at[0])

    def begin(copies):
        for c in copies:
            c.start()

    def finish(copies):
        for c in copies:
            c.wait()

    begin(small[:2] + out_loads[0] + own_loads[0] + small[2:])
    tok_load.start()
    begin(out_loads[1] + own_loads[1] + out_loads[2] + own_loads[2])

    def remote(src, dst, send, recv, peer):
        return pltpu.make_async_remote_copy(
            src_ref=src,
            dst_ref=dst,
            send_sem=send,
            recv_sem=recv,
            device_id=peer,
            device_id_type=MESH,
        )

    def y_copy(g):
        return remote(
            stage_w.at[g], wts.at[g, block_rows(mine)], y_send.at[g], w_recv.at[g, mine], across
        )

    def block_copy(g, blk, sends, peer):
        at = wts.at[g, block_rows(blk)]
        return remote(at, at, sends.at[g, blk], w_recv.at[g, blk], peer)

    def to_pair(g, blk):
        return block_copy(g, blk, pair_send, pair)

    def to_mid(g, blk):
        return block_copy(g, blk, mid_send, mid)

    def arrived(g, blk):
        to_pair(g, blk).wait_recv()

    def slot_of(k):
        return (other, 2 + f, 2 + other)[k]

    def piece(slot, j, q):
        place = jnp.where(low_half, SUBS - 1 - j, j)
        return toks.at[slot, pl.ds(pl.multiple_of(place * sub + q * part, 16), part)]

    def tok_y(k, j):
        slot = f if k == 0 else 2 + f
        at = piece(slot, j, beyond_t if k == 2 else t)
        kind = 2 if k == 2 else 0
        return remote(at, at, tok_y_send.at[k, j], tok_recv.at[2 if k else 0, j, kind], across)

    def tok_z(k, j):
        seq = f if k == 0 else other
        return remote(
            piece(seq, j, t),
            piece(2 + seq, j, t),
            tok_z_send.at[k, j],
            tok_recv.at[1 + k, j, 0],
            pair,
        )

    def tok_share(k, j, kind):
        q = beyond_t if kind == 2 else t
        at = piece(slot_of(k), j, q)
        return remote(
            at, at, tok_t_send.at[k, j, kind], tok_recv.at[k, j, kind + 1],
            beyond if kind == 1 else mate,
        )

    def tok_wait(k, j, kind):
        at = piece(slot_of(k), j, t)
        remote(at, at, tok_t_send.at[k, j, 0], tok_recv.at[k, j, kind], mate).wait_recv()

    def take(k, j):
        tok_wait(k, j, 0)
        if k < 2 or j >= SUBS // 2:
            tok_share(k, j, 1).start()
        tok_share(k, j, 0).start()
        if k == 1 and j < SUBS // 2:
            tok_y(1, j).start()

    def hand(k, j):
        tok_wait(k, j, 2)
        tok_share(k, j, 2).start()
        if k == 1 and j < SUBS // 2:
            tok_y(2, j).start()

    def have(k, j):
        tok_wait(k, j, 1)
        tok_wait(k, j, 3)

    def norm_own():
        @pl.loop(0, blocks)
        def _(b):
            at = pl.ds(pl.multiple_of(b * WINDOW, WINDOW), WINDOW)
            values = toks[f, at, :].astype(jnp.float32)
            scaling = lax.rsqrt(jnp.mean(values * values, axis=-1, keepdims=True) + EPSILON)
            toks[f, at, :] = (values * scaling * gain[...]).astype(jnp.bfloat16)

    mm_rows = rows // 2

    def make_bias():
        key = lax.broadcasted_iota(jnp.int32, (3 * WINDOW, WINDOW), 0)
        query = lax.broadcasted_iota(jnp.int32, (3 * WINDOW, WINDOW), 1)
        away = jnp.abs(query - key + WINDOW)
        for h in range(heads):
            index = (t * (2 * heads) + f * heads + h + 1).astype(jnp.float32)
            slope = jnp.exp2(jnp.full((1, WINDOW), -8.0 / (2 * heads * tps), jnp.float32) * index)
            bias[h] = jnp.where(away <= WINDOW, -slope * away.astype(jnp.float32), FAR)

    half_k = depth * SPAN
    near_k = pl.multiple_of(jnp.where(low_half, 0, half_k), 128)
    far_k = pl.multiple_of(half_k - near_k, 128)

    def partial(g, slot, at, k_off):
        return jnp.dot(
            toks[slot, pl.ds(at, mm_rows), pl.ds(k_off, half_k)],
            wts[g, pl.ds(k_off, half_k), :],
            preferred_element_type=jnp.float32,
        )

    def sums(g, slot):
        return slot if g == 0 else slot + 4 * g - 2

    def halves_of(b):
        return pl.loop(0, 2) if b is None else lambda body: body(b)

    def near(g, slot, only=None):
        @halves_of(only)
        def _(b):
            at = pl.multiple_of(b * mm_rows, WINDOW)
            acc[sums(g, slot), pl.ds(at, mm_rows), :] = partial(g, slot, at, near_k)

    def total(g, slot, at):
        return acc[sums(g, slot), pl.ds(at, mm_rows), :] + partial(g, slot, at, far_k)

    def project_qkv(seq):
        @pl.loop(0, 2)
        def _(b):
            at = pl.multiple_of(b * mm_rows, WINDOW)
            out = total(0, seq, at)
            qs[seq, pl.ds(at, mm_rows), :] = out[:, :qcols].astype(jnp.bfloat16)
            kvs[seq, pl.ds(at + WINDOW, mm_rows), :] = out[:, qcols:].astype(jnp.bfloat16)

    kv_len = kvs.shape[1]

    def kv_copies(seq, slot):
        ref = kvs.at[seq]
        climb = remote(
            ref.at[pl.ds(kv_len - 2 * WINDOW, WINDOW)],
            ref.at[pl.ds(0, WINDOW)],
            kv_send.at[slot, 0],
            kv_recv.at[slot, 0],
            up,
        )
        fall = remote(
            ref.at[pl.ds(WINDOW, WINDOW)],
            ref.at[pl.ds(kv_len - WINDOW, WINDOW)],
            kv_send.at[slot, 1],
            kv_recv.at[slot, 1],
            down,
        )
        return climb, fall

    def kv_start(seq, slot):
        climb, fall = kv_copies(seq, slot)
        blank = jnp.zeros((WINDOW, 2 * HEAD), jnp.bfloat16)

        @pl.when(has_up)
        def _():
            climb.start()

        @pl.when(has_down)
        def _():
            fall.start()

        @pl.when(jnp.logical_not(has_up))
        def _():
            kvs[seq, pl.ds(kv_len - WINDOW, WINDOW), :] = blank

        @pl.when(jnp.logical_not(has_down))
        def _():
            kvs[seq, pl.ds(0, WINDOW), :] = blank

    def kv_wait(seq, slot):
        climb, fall = kv_copies(seq, slot)

        @pl.when(has_up)
        def _():
            climb.wait_send()
            fall.wait_recv()

        @pl.when(has_down)
        def _():
            fall.wait_send()
            climb.wait_recv()

    def attend(seq, first, count, step=1):
        @pl.loop(0, count)
        def _(i):
            b = first + i * step
            at = pl.multiple_of(b * WINDOW, WINDOW)
            kv = kvs[seq, pl.ds(at, 3 * WINDOW), :]
            keys = kv[:, :HEAD]
            values_t = kv.astype(jnp.float32).T[HEAD:, :].astype(jnp.bfloat16)
            queries = qs[seq, pl.ds(at, WINDOW), :]
            low = jnp.where((b == 0) & (s == 0), FAR, 0.0)
            high = jnp.where((b == blocks - 1) & (s == SPAN - 1), FAR, 0.0)
            outs = []
            for h in range(heads):
                query = queries[:, h * HEAD : (h + 1) * HEAD]
                scores = lax.dot_general(
                    keys, query, (((1,), (1,)), ((), ())), preferred_element_type=jnp.float32
                )
                scores = scores * (1.0 / math.sqrt(HEAD)) + bias[h]
                scores = jnp.concatenate(
                    [
                        scores[:WINDOW] + low,
                        scores[WINDOW : 2 * WINDOW],
                        scores[2 * WINDOW :] + high,
                    ],
                    axis=0,
                )
                sink = sinks[f * heads + h]
                peak = jnp.maximum(jnp.max(scores, axis=0, keepdims=True), sink)
                weights = jnp.exp(scores - peak)
                total = jnp.sum(weights, axis=0, keepdims=True) + jnp.exp(sink - peak)
                mixed = jnp.dot(
                    values_t, weights.astype(jnp.bfloat16), preferred_element_type=jnp.float32
                )
                outs.append(mixed / total)
                log_st[seq, pl.ds(h, 1), pl.ds(at, WINDOW)] = peak + jnp.log(total)
            stacked = jnp.concatenate(outs, axis=0)
            attn_st[seq, pl.ds(at, WINDOW), :] = stacked.T.astype(jnp.bfloat16)

    half_cols = pl.ds(pl.multiple_of(f * qcols, 128), qcols)

    def attn_return(own):
        seq = f if own else other
        pairs = [
            (attn_st.at[seq], attn_out.at[:, half_cols]),
            (log_st.at[seq], log_out.at[f]),
        ]
        if own:
            return [pltpu.make_async_copy(a, b, misc_sem.at[1 + i]) for i, (a, b) in enumerate(pairs)]
        return [
            remote(a, b, ret_send.at[i], ret_recv.at[i], across) for i, (a, b) in enumerate(pairs)
        ]

    def conv_cols(g):
        return pl.ds(pl.multiple_of(f * (2 * chans) + (g - 1) * chans, 128), chans)

    split = mm_rows - pad
    head_b = jnp.where(low_half, 1, 0)
    spans = {
        None: (0, rows),
        "head": (jnp.where(low_half, rows - split, 0), split),
        "tail": (jnp.where(low_half, 0, split), rows - split),
    }

    def conv_return(g, own_seq, own_rows, span=None):
        seq = f if own_seq else other
        off = own_off if own_rows else end_off
        lo, count = spans[span]
        src = conv_st.at[g - 1, seq, pl.ds(pl.multiple_of(off + lo, pad), count)]
        dst = conv_out.at[pl.ds(pl.multiple_of(lo, pad), count), conv_cols(g)]
        if own_seq and own_rows:
            return pltpu.make_async_copy(src, dst, own_sem.at[g - 1])
        if own_seq:
            return remote(src, dst, conv_send.at[g - 1, 0], conv_recv.at[g - 1, 0], pair)
        if own_rows:
            return remote(src, dst, conv_send.at[g - 1, 1], conv_recv.at[g - 1, 1], across)
        last = 1 if span == "tail" else 0
        return remote(
            src, dst, conv_send.at[g - 1, 2 + last], conv_recv.at[g - 1, 1 + last], diag
        )

    def project_conv(g, seq, own_rows, only=None):
        slot, off = (seq, own_off) if own_rows else (2 + seq, end_off)

        @halves_of(only)
        def _(b):
            at = pl.multiple_of(b * mm_rows, WINDOW)
            to = pl.multiple_of(off + b * mm_rows, WINDOW)
            out = total(g, slot, at)
            inner = out[:, :chans].astype(jnp.bfloat16).astype(jnp.float32)
            signal = out[:, chans : 2 * chans].astype(jnp.bfloat16).astype(jnp.float32)
            prod[g - 1, seq, pl.ds(to + pad, mm_rows), :] = (inner * signal).astype(jnp.bfloat16)
            outer[g - 1, seq, pl.ds(to, mm_rows), :] = out[:, 2 * chans :].astype(jnp.bfloat16)

    def pr_copies(g, seq, slot):
        ref = prod.at[g - 1, seq]
        climb = remote(
            ref.at[pl.ds(both_rows, pad)],
            ref.at[pl.ds(0, pad)],
            pr_send.at[g - 1, slot],
            pr_recv.at[g - 1, slot],
            mid,
        )
        fall = remote(
            ref.at[pl.ds(pad, pad)],
            ref.at[pl.ds(both_rows + pad, pad)],
            pr_send.at[g - 1, slot],
            pr_recv.at[g - 1, slot],
            mid,
        )
        return climb, fall

    def pr_start(g, seq, slot):
        climb, fall = pr_copies(g, seq, slot)
        blank = jnp.zeros((pad, chans), jnp.bfloat16)

        @pl.when(low_half)
        def _():
            climb.start()
            prod[g - 1, seq, pl.ds(0, pad), :] = blank

        @pl.when(jnp.logical_not(low_half))
        def _():
            fall.start()
            prod[g - 1, seq, pl.ds(both_rows + pad, pad), :] = blank

    def pr_wait(g, seq, slot):
        climb, fall = pr_copies(g, seq, slot)

        @pl.when(low_half)
        def _():
            climb.wait_send()
            fall.wait_recv()

        @pl.when(jnp.logical_not(low_half))
        def _():
            fall.wait_send()
            climb.wait_recv()

    def mix(g, seq, own_rows, span=None):
        lo, count = spans[span]
        off = pl.multiple_of((own_off if own_rows else end_off) + lo, pad)
        tap = taps[:, conv_cols(g)]
        size = count + 2 * pad
        full = prod[g - 1, seq, pl.ds(off, size), :].astype(jnp.float32)
        before = pltpu.roll(full, 1, 0)[pad : pad + count]
        after = pltpu.roll(full, size - 1, 0)[pad : pad + count]
        mixed = tap[0:1] * before + tap[1:2] * full[pad : pad + count] + tap[2:3] * after
        gate = outer[g - 1, seq, pl.ds(off, count), :].astype(jnp.float32)
        conv_st[g - 1, seq, pl.ds(off, count), :] = (gate * mixed).astype(jnp.bfloat16)

    finish(small[:2])
    keys0, vals0 = kv_raw[0], kv_raw[1]
    halves = [
        jnp.concatenate([w[:, i * HEAD : (i + 1) * HEAD] for w in (keys0, vals0)], axis=1)
        for i in range(2)
    ]
    first = f == 0
    stage_w[0, :, pl.ds(qcols, 2 * HEAD)] = jnp.where(first, halves[1], halves[0])
    wts[0, block_rows(mine), pl.ds(qcols, 2 * HEAD)] = jnp.where(first, halves[0], halves[1])

    pl.semaphore_wait(barrier, jnp.where(is_mid, 6, 5))

    finish(own_loads[0])
    to_pair(0, mine).start()

    @pl.when(is_mid)
    def _():
        to_mid(0, mine).start()

    finish(out_loads[0])
    y_copy(0).start()
    finish(own_loads[1])

    @pl.when(is_mid)
    def _():
        to_mid(1, mine).start()

    finish(small[2:])
    for i in range(gain_raw.shape[0]):
        gain[:, i * 128 : (i + 1) * 128] = gain_raw[i : i + 1, :]
    tok_load.wait()
    norm_own()
    for j in range(SUBS):
        tok_y(0, j).start()
    finish(out_loads[1] + out_loads[2] + own_loads[2])
    y_copy(1).start()
    y_copy(2).start()

    def relay(g, blk, onward):
        arrived(g, blk)
        onward(g, blk).start()

    pt = [partner * 2 + f, partner * 2 + other]
    ct = [facing * 2 + f, facing * 2 + other]
    ft = [far * 2 + f, far * 2 + other]

    def end_program():
        tok_z(0, 0).start()
        make_bias()
        relay(0, theirs, to_pair)
        tok_z(0, 1).start()
        to_pair(1, mine).start()
        tok_z(0, 2).start()
        take(0, 0)
        take(0, 1)
        for blk in pt:
            arrived(0, blk)
        near(0, f)
        hand(0, 0)
        take(0, 2)
        hand(0, 1)
        take(0, 3)
        hand(0, 2)
        relay(1, theirs, to_pair)
        tok_z(0, 3).start()
        hand(0, 3)
        for j in range(SUBS):
            have(0, j)
        near(0, other)
        for blk in ct + ft:
            arrived(0, blk)
        project_qkv(f)
        kv_start(f, 0)
        project_qkv(other)
        kv_start(other, 1)
        to_pair(2, mine).start()
        relay(2, theirs, to_pair)
        tok_z(1, 2).start()
        tok_z(1, 3).start()
        attend(f, 1, blocks - 2)
        attend(other, 1, blocks - 2)
        kv_wait(f, 0)
        attend(f, 0, 2, blocks - 1)
        begin(attn_return(True))
        kv_wait(other, 1)
        attend(other, 0, 2, blocks - 1)
        begin(attn_return(False))
        for g in (1, 2):
            conv_return(g, True, False).wait_recv()
            conv_return(g, False, False, "head").wait_recv()
            conv_return(g, False, False, "tail").wait_recv()
        for g in range(GROUPS):
            to_pair(g, mine).wait_send()
            to_pair(g, theirs).wait_send()
        for j in range(SUBS):
            tok_z(0, j).wait_send()
        for j in range(SUBS // 2, SUBS):
            tok_z(1, j).wait_send()

    def conv_own(g, own_seq):
        seq, slot = (f, 0) if own_seq else (other, 1)
        project_conv(g, seq, True)
        pr_start(g, seq, slot)

    def conv_close(g, own_seq):
        seq, slot = (f, 0) if own_seq else (other, 1)
        pr_wait(g, seq, slot)
        mix(g, seq, True)
        conv_return(g, own_seq, True).start()

    def conv_end(g):
        project_conv(g, f, False)
        mix(g, f, False)
        conv_return(g, True, False).start()

    def conv_end_part(g, span):
        project_conv(g, other, False, head_b if span == "head" else 1 - head_b)
        mix(g, other, False, span)
        conv_return(g, False, False, span).start()

    def mid_program():
        half = (blocks - 2) // 2
        make_bias()
        relay(0, theirs, to_mid)
        to_pair(0, theirs).start()
        relay(0, ct[0], to_pair)
        relay(0, pt[0], to_mid)
        take(0, 0)
        take(0, 1)
        relay(0, ct[1], to_pair)
        relay(0, pt[1], to_mid)
        to_mid(2, mine).start()
        near(0, f)
        hand(0, 0)
        relay(0, ft[0], to_pair)
        take(0, 2)
        hand(0, 1)
        take(0, 3)
        take(1, 0)
        relay(0, ft[1], to_pair)
        project_qkv(f)
        kv_start(f, 0)
        hand(0, 2)
        take(1, 1)
        relay(1, pt[0], to_mid)
        attend(f, 1, half)
        relay(1, theirs, to_mid)
        hand(0, 3)
        for j in range(SUBS):
            have(0, j)
        near(0, other)
        project_qkv(other)
        kv_start(other, 1)
        relay(2, theirs, to_mid)
        take(1, 2)
        attend(f, 1 + half, half)
        hand(1, 0)
        relay(1, pt[1], to_mid)
        attend(other, 1, half)
        near(1, f)
        hand(1, 1)
        near(1, other)
        take(1, 3)
        attend(other, 1 + half, half)
        kv_wait(f, 0)
        attend(f, 0, 2, blocks - 1)
        begin(attn_return(True))
        hand(1, 2)
        take(2, 0)
        take(2, 1)
        relay(2, pt[0], to_mid)
        kv_wait(other, 1)
        attend(other, 0, 2, blocks - 1)
        begin(attn_return(False))
        for blk in ct + ft:
            arrived(1, blk)
        conv_own(1, True)
        hand(1, 3)
        hand(2, 0)
        conv_own(1, False)
        relay(2, pt[1], to_mid)
        for j in range(SUBS):
            have(1, j)
        near(1, 2 + f)
        conv_end(1)
        near(2, 2 + f)
        hand(2, 1)
        take(2, 2)
        conv_close(1, True)
        for j in range(SUBS // 2):
            have(2, j)
        near(1, 2 + other, head_b)
        conv_end_part(1, "head")
        conv_close(1, False)
        near(2, f)
        near(2, other)
        take(2, 3)
        near(2, 2 + other, head_b)
        for blk in ct + ft:
            arrived(2, blk)
        conv_own(2, True)
        conv_own(2, False)
        hand(2, 2)
        conv_end(2)
        conv_end_part(2, "head")
        conv_close(2, False)
        hand(2, 3)
        for j in range(SUBS // 2, SUBS):
            have(2, j)
        near(1, 2 + other, 1 - head_b)
        conv_end_part(1, "tail")
        near(2, 2 + other, 1 - head_b)
        conv_end_part(2, "tail")
        conv_close(2, True)
        for g in (1, 2):
            conv_return(g, False, True).wait_recv()
            conv_return(g, True, True).wait()
            conv_return(g, False, True).wait_send()
            conv_return(g, True, False).wait_send()
            conv_return(g, False, False, "head").wait_send()
            conv_return(g, False, False, "tail").wait_send()
        for blk in [mine, theirs] + ct + ft:
            to_pair(0, blk).wait_send()
        for g in range(GROUPS):
            for blk in [mine, theirs] + pt:
                to_mid(g, blk).wait_send()
        for j in range(SUBS // 2):
            tok_y(1, j).wait_send()
            tok_y(2, j).wait_send()
        for k in (1, 2):
            for j in range(SUBS):
                for kind in range(3):
                    if k < 2 or j >= SUBS // 2 or kind != 1:
                        tok_share(k, j, kind).wait_send()

    pl.when(is_end)(end_program)
    pl.when(is_mid)(mid_program)

    for g in range(GROUPS):
        y_copy(g).wait_send()
    for j in range(SUBS):
        tok_y(0, j).wait_send()
        for kind in range(3):
            tok_share(0, j, kind).wait_send()
    for own in (True, False):
        finish(attn_return(own))


def fused_device(
    tps,
    tokens,
    norm_gain,
    query_weight,
    key_weight,
    value_weight,
    outer_weight,
    inner_weight,
    signal_weight,
    conv_taps,
    sink_logit,
):
    rows, width = tokens.shape[1:]
    depth, local = query_weight.shape
    qcols = local // 2
    heads = qcols // HEAD
    chans = outer_weight.shape[1] // 4
    head_local = 2 * heads
    group_cols = qcols + 2 * HEAD
    pad = 16
    bf, f32 = jnp.bfloat16, jnp.float32
    dma = pltpu.SemaphoreType.DMA
    hbm = pl.BlockSpec(memory_space=pltpu.HBM)
    anyspace = pl.BlockSpec(memory_space=pl.ANY)
    attended, conv, logs = pl.pallas_call(
        functools.partial(mega_kernel, tps),
        out_shape=(
            jax.ShapeDtypeStruct((rows, local), bf),
            jax.ShapeDtypeStruct((rows, 4 * chans), bf),
            jax.ShapeDtypeStruct((2, heads, rows), f32),
        ),
        in_specs=[hbm] * 10,
        out_specs=(anyspace, anyspace, anyspace),
        scratch_shapes=[
            pltpu.VMEM((4, rows, width), bf),
            pltpu.VMEM((GROUPS, width, group_cols), bf),
            pltpu.VMEM((GROUPS, depth, group_cols), bf),
            pltpu.VMEM((2, rows, qcols), bf),
            pltpu.VMEM((2, rows + 2 * WINDOW, 2 * HEAD), bf),
            pltpu.VMEM((heads, 3 * WINDOW, WINDOW), f32),
            pltpu.VMEM((2, 2, 2 * rows + 2 * pad, chans), bf),
            pltpu.VMEM((2, 2, 2 * rows, chans), bf),
            pltpu.VMEM((2, rows, qcols), bf),
            pltpu.VMEM((2, heads, rows), f32),
            pltpu.VMEM((2, 2, 2 * rows, chans), bf),
            pltpu.VMEM((10, rows, group_cols), f32),
            pltpu.VMEM((2, depth, 2 * HEAD), bf),
            pltpu.VMEM((width // 128, 128), f32),
            pltpu.VMEM((1, width), f32),
            pltpu.VMEM((3, 4 * chans), f32),
            pltpu.SMEM((head_local,), f32),
            dma((5,)),
            dma((GROUPS, 3)),
            dma((GROUPS, 3)),
            dma((3,)),
            dma((2,)),
            dma((GROUPS,)),
            dma((GROUPS, 2 * SPAN)),
            dma((GROUPS, 2 * SPAN)),
            dma((GROUPS, 2 * SPAN)),
            dma((3, SUBS)),
            dma((2, SUBS)),
            dma((3, SUBS, 3)),
            dma((3, SUBS, 4)),
            dma((2, 2)),
            dma((2, 2)),
            dma((2, 2)),
            dma((2, 2)),
            dma((2,)),
            dma((2,)),
            dma((2, 4)),
            dma((2, 3)),
        ],
        compiler_params=pltpu.CompilerParams(
            collective_id=0, has_side_effects=True, vmem_limit_bytes=48 << 20
        ),
    )(
        *(
            pltpu.with_memory_space_constraint(x, pltpu.HBM)
            for x in (
                tokens[0],
                norm_gain.reshape(width // 128, 128),
                query_weight,
                key_weight,
                value_weight,
                outer_weight,
                inner_weight,
                signal_weight,
                conv_taps,
                sink_logit,
            )
        )
    )
    return (attended[None], conv[None], logs.reshape(1, head_local, rows))


def fits(mesh, args):
    tokens, query_weight, key_weight, outer_weight = (args[i] for i in (0, 2, 3, 5))
    sp, fs, tp = (mesh.shape[a] for a in ("sp", "fs", "tp"))
    rows = tokens.shape[1] // sp
    return (
        fs == 2
        and sp == SPAN
        and tokens.shape[0] == fs
        and tp == 4
        and rows % (2 * WINDOW) == 0
        and rows // WINDOW % 2 == 0
        and rows % (16 * SUBS * tp) == 0
        and key_weight.shape[1] == 2 * HEAD * tp
        and query_weight.shape[1] % (256 * tp) == 0
        and outer_weight.shape[1] == 512 * tp
        and query_weight.shape[1] == 512 * tp
        and query_weight.shape[0] % (16 * sp * fs) == 0
    )


def solution(mesh):
    in_specs = (
        P("fs", "sp", None),
        P(),
        P(("sp", "fs"), "tp"),
        P(("sp", "fs"), "tp"),
        P(("sp", "fs"), "tp"),
        P(("sp", "fs"), "tp"),
        P(("sp", "fs"), "tp"),
        P(("sp", "fs"), "tp"),
        P(None, "tp"),
        P("tp"),
    )
    out_specs = (P("fs", "sp", "tp"), P("fs", "sp", "tp"), P("fs", "tp", "sp"))

    def run(*args):
        body = per_device
        if fits(mesh, args):
            body = functools.partial(fused_device, mesh.shape["tp"])
        return jax.shard_map(
            body, mesh=mesh, in_specs=in_specs, out_specs=out_specs, check_vma=False
        )(*args)

    return run
```

```python
import math

import functools

import jax
import jax.numpy as jnp
from jax import lax
from jax.experimental import pallas as pl
from jax.experimental.pallas import tpu as pltpu
from jax.sharding import PartitionSpec as P

HEAD = 64
WINDOW = 128


EPSILON = 1e-06


def extended(value, sides, width):
    for axis, dim in sides:
        size, length = (lax.axis_size(axis), value.shape[dim])
        up = [(i, (i + 1) % size) for i in range(size - 1)]
        down = [(j, i) for i, j in up]
        last = lax.slice_in_dim(value, length - width, length, axis=dim)
        initial = lax.slice_in_dim(value, 0, width, axis=dim)
        before = lax.ppermute(last, axis, up)
        after = lax.ppermute(initial, axis, down)
        value = jnp.concatenate([before, value, after], axis=dim)
    return value


def normalized(tokens, norm_gain):
    values = tokens.astype(jnp.float32)
    scaling = lax.rsqrt(jnp.mean(values * values, axis=-1, keepdims=True) + EPSILON)
    return (values * scaling * norm_gain).astype(jnp.bfloat16)


def folding(normed):

    def add_portions(running, portions, offset):
        return tuple(
            (jnp.dot(normed, portion, preferred_element_type=jnp.float32) for portion in portions)
        )

    return add_portions


def empty_sums(normed, weights):
    return tuple((jnp.zeros((normed.shape[0], weight.shape[1]), jnp.float32) for weight in weights))


def rounded(results):
    return tuple((result.astype(jnp.bfloat16) for result in results))


def gate_product(inner_gate, signal):
    return (inner_gate.astype(jnp.float32) * signal.astype(jnp.float32)).astype(jnp.bfloat16)


def send_edges(key_proj, value_proj, product):
    stacked = jnp.concatenate([key_proj, value_proj], axis=1)
    window_rows = extended(stacked, (("sp", 0),), WINDOW)
    conv_rows = extended(product, (("sp", 0),), 1)
    return (window_rows, conv_rows)


def banded_attention(queries, window_rows, sink_logit, slopes, first_pos, seq_length):
    tok_count = queries.shape[0]
    kv_cols = window_rows.shape[1] // 2
    kv_heads = kv_cols // HEAD
    group_size = queries.shape[1] // (HEAD * kv_heads)
    block_count = tok_count // WINDOW
    query_blocks = queries.reshape(block_count, WINDOW, kv_heads, group_size, HEAD)
    key_rows = window_rows[:, :kv_cols].reshape(block_count + 2, WINDOW, kv_heads, HEAD)
    value_rows = window_rows[:, kv_cols:].reshape(block_count + 2, WINDOW, kv_heads, HEAD)
    key_span = jnp.concatenate([key_rows[:-2], key_rows[1:-1], key_rows[2:]], axis=1)
    value_span = jnp.concatenate([value_rows[:-2], value_rows[1:-1], value_rows[2:]], axis=1)
    scores = jnp.einsum(
        "bqkgd,bskd->bkgqs", query_blocks, key_span, preferred_element_type=jnp.float32
    ) * (1.0 / math.sqrt(HEAD))
    distance = jnp.arange(WINDOW)[:, None] - jnp.arange(3 * WINDOW)[None, :] + WINDOW
    key_pos = (
        first_pos
        - WINDOW
        + WINDOW * jnp.arange(block_count)[:, None]
        + jnp.arange(3 * WINDOW)[None, :]
    )
    inside = (jnp.abs(distance)[None] <= WINDOW) & ((key_pos >= 0) & (key_pos < seq_length))[
        :, None, :
    ]
    scores = scores - slopes.reshape(kv_heads, group_size, 1, 1) * jnp.abs(distance).astype(
        jnp.float32
    )
    scores = jnp.where(inside[:, None, None], scores, -jnp.inf)
    sink_grid = sink_logit.reshape(kv_heads, group_size, 1, 1)
    row_peak = jnp.maximum(jnp.max(scores, axis=-1, keepdims=True), sink_grid)
    weights = jnp.exp(scores - row_peak)
    row_total = jnp.sum(weights, axis=-1, keepdims=True) + jnp.exp(sink_grid - row_peak)
    weighted = jnp.einsum(
        "bkgqs,bskd->bqkgd",
        weights.astype(jnp.bfloat16),
        value_span,
        preferred_element_type=jnp.float32,
    )
    attended = (
        (weighted / row_total.transpose(0, 3, 1, 2, 4))
        .astype(jnp.bfloat16)
        .reshape(tok_count, kv_heads * group_size * HEAD)
    )
    log_total = (
        (row_peak + jnp.log(row_total))[..., 0]
        .transpose(1, 2, 0, 3)
        .reshape(kv_heads * group_size, tok_count)
    )
    return (attended, log_total)


def per_device(
    tokens,
    norm_gain,
    query_weight,
    key_weight,
    value_weight,
    outer_weight,
    inner_weight,
    signal_weight,
    conv_taps,
    sink_logit,
):
    normed = normalized(tokens[0], norm_gain)
    add_portions = folding(normed)
    all_sums = add_portions(
        empty_sums(
            normed,
            (query_weight, key_weight, value_weight, outer_weight, inner_weight, signal_weight),
        ),
        (
            lax.all_gather(query_weight, ("sp", "fs"), axis=0, tiled=True),
            lax.all_gather(key_weight, ("sp", "fs"), axis=0, tiled=True),
            lax.all_gather(value_weight, ("sp", "fs"), axis=0, tiled=True),
            lax.all_gather(outer_weight, ("sp", "fs"), axis=0, tiled=True),
            lax.all_gather(inner_weight, ("sp", "fs"), axis=0, tiled=True),
            lax.all_gather(signal_weight, ("sp", "fs"), axis=0, tiled=True),
        ),
        jnp.int32(0),
    )
    queries, key_proj, value_proj, outer_gate, inner_gate, signal = rounded(all_sums)
    product = gate_product(inner_gate, signal)
    window_rows, conv_rows = send_edges(key_proj, value_proj, product)
    tok_count = normed.shape[0]
    head_local = queries.shape[1] // HEAD
    head_index = lax.axis_index("tp") * head_local + jnp.arange(1, head_local + 1)
    slopes = jnp.exp2(-8.0 * head_index.astype(jnp.float32) / (head_local * lax.axis_size("tp")))
    first_pos = lax.axis_index("sp") * tok_count
    attended, log_total = banded_attention(
        queries, window_rows, sink_logit, slopes, first_pos, tok_count * lax.axis_size("sp")
    )
    mixed_conv = conv_taps[0] * conv_rows[0:tok_count].astype(jnp.float32)
    mixed_conv = mixed_conv + conv_taps[1] * conv_rows[1 : tok_count + 1].astype(jnp.float32)
    mixed_conv = mixed_conv + conv_taps[2] * conv_rows[2 : tok_count + 2].astype(jnp.float32)
    conv_out = (outer_gate.astype(jnp.float32) * mixed_conv).astype(jnp.bfloat16)
    return (attended[None], conv_out[None], log_total[None])


MESH = pl.DeviceIdType.MESH
GROUPS = 3
SPAN = 4
SUBS = 4
Y_PAIRS = 1
Z_FIRST = 3
FAR = -1e30


def mega_kernel(
    tps,
    tokens,
    gain_in,
    qw,
    kw,
    vw,
    ow,
    iw,
    sw,
    taps_in,
    sinks_in,
    attn_out,
    conv_out,
    log_out,
    toks,
    wts,
    stage_w,
    qs,
    kvs,
    bias,
    sink_row,
    prod,
    outer,
    attn_st,
    log_st,
    conv_st,
    acc,
    kv_raw,
    gain_raw,
    gain,
    taps,
    sinks,
    small_sem,
    load_sem,
    stage_sem,
    misc_sem,
    own_sem,
    y_send,
    w_recv,
    pair_send,
    mid_send,
    tok_y_send,
    tok_z_send,
    tok_t_send,
    tok_recv,
    tok_have,
    kv_send,
    kv_recv,
    pr_send,
    pr_recv,
    ret_send,
    ret_recv,
    conv_send,
    conv_recv,
):
    s, f, t = lax.axis_index("sp"), lax.axis_index("fs"), lax.axis_index("tp")
    other = 1 - f
    core = lax.rem(t, 2)
    outward = 1 - lax.rem(s, 2)
    partner = s + 2 * outward - 1
    facing = SPAN - 1 - s
    far = SPAN - 1 - partner
    is_mid = (s == 1) | (s == SPAN - 2)
    is_end = jnp.logical_not(is_mid)
    low_half = s < SPAN // 2
    pair, diag, mid = (partner, f, t), (partner, other, t), (facing, f, t)
    across = (s, other, t)
    mate_t, beyond_t = t + 1 - 2 * core, lax.rem(t + 2, tps)
    mate, beyond = (s, f, mate_t), (s, f, beyond_t)
    rows = tokens.shape[0]
    depth = qw.shape[0]
    qcols = qs.shape[2]
    heads = qcols // HEAD
    chans = prod.shape[3]
    both_rows = outer.shape[2]
    blocks = rows // WINDOW
    pad = (prod.shape[2] - both_rows) // 2
    sub = rows // SUBS
    part = sub // tps
    up, down = (s + 1, f, t), (s - 1, f, t)
    has_up, has_down = s < SPAN - 1, s > 0
    own_off = jnp.where(low_half, rows, 0)
    end_off = rows - own_off

    barrier = pltpu.get_barrier_semaphore()
    for peer in (pair, diag, across, mate, beyond):
        pl.semaphore_signal(barrier, inc=1, device_id=peer, device_id_type=MESH)

    @pl.when(is_mid)
    def _():
        pl.semaphore_signal(barrier, inc=1, device_id=mid, device_id_type=MESH)

    def block_rows(blk):
        return pl.ds(pl.multiple_of(blk * depth, 16), depth)

    def loads(g, half, dest, sems):
        if g == 0:
            qc = pl.ds(pl.multiple_of(half * qcols, 128), qcols)
            pairs = [(qw.at[:, qc], dest.at[:, pl.ds(0, qcols)])]
        else:
            c = pl.ds(pl.multiple_of(half * (2 * chans) + (g - 1) * chans, 128), chans)
            pairs = [
                (ref.at[:, c], dest.at[:, pl.ds(i * chans, chans)])
                for i, ref in enumerate((iw, sw, ow))
            ]
        return [pltpu.make_async_copy(a, b, sems.at[g]) for a, b in pairs]

    def loaded(g, dest, sems):
        whole = dest.at[:, pl.ds(0, qcols)] if g == 0 else dest
        pltpu.make_async_copy(whole, whole, sems.at[g]).wait()

    mine = s * 2 + f
    theirs = s * 2 + other
    own_dest = [wts.at[g, block_rows(mine)] for g in range(GROUPS)]
    own_loads = [loads(g, f, own_dest[g], load_sem) for g in range(GROUPS)]
    out_loads = [loads(g, other, stage_w.at[g], stage_sem) for g in range(GROUPS)]
    small = [
        pltpu.make_async_copy(a, b, small_sem.at[i])
        for i, (a, b) in enumerate(
            (
                (kw, kv_raw.at[0]),
                (vw, kv_raw.at[1]),
                (gain_in, gain_raw),
                (taps_in, taps),
                (sinks_in, sinks),
            )
        )
    ]
    tok_load = pltpu.make_async_copy(tokens, toks.at[f], misc_sem.at[0])

    def begin(copies):
        for c in copies:
            c.start()

    def finish(copies):
        for c in copies:
            c.wait()

    begin(small[:2] + out_loads[0] + own_loads[0] + small[2:])
    tok_load.start()
    begin(out_loads[1] + own_loads[1] + out_loads[2] + own_loads[2])

    def remote(src, dst, send, recv, peer):
        return pltpu.make_async_remote_copy(
            src_ref=src,
            dst_ref=dst,
            send_sem=send,
            recv_sem=recv,
            device_id=peer,
            device_id_type=MESH,
        )

    def y_copy(g):
        return remote(
            stage_w.at[g], wts.at[g, block_rows(mine)], y_send.at[g], w_recv.at[g, mine], across
        )

    def block_copy(g, blk, send, peer):
        at = wts.at[g, block_rows(blk)]
        return remote(at, at, send, w_recv.at[g, blk], peer)

    def to_pair(g, blk):
        return block_copy(g, blk, pair_send.at[0], pair)

    def to_mid(g, blk):
        return block_copy(g, blk, mid_send.at[g], mid)

    def blocks_sent(send, count):
        at = wts.at[0, pl.ds(0, count * depth)]
        remote(at, at, send, w_recv.at[0, 0], across).wait_send()

    def arrived(g, blk):
        to_pair(g, blk).wait_recv()

    def slot_of(k):
        return (other, 2 + f, 2 + other)[k]

    def piece(slot, j, q):
        place = jnp.where(low_half, SUBS - 1 - j, j)
        return toks.at[slot, pl.ds(pl.multiple_of(place * sub + q * part, 16), part)]

    def tok_y(k, j):
        slot = f if k == 0 else 2 + f
        at = piece(slot, j, beyond_t if k == 2 else t)
        return remote(
            at, at, tok_y_send.at[1 if k else 0], tok_recv.at[2 if k else 0, j, k // 2], across
        )

    def tok_z(k, j):
        seq = f if k == 0 else other
        return remote(
            piece(seq, j, t), piece(2 + seq, j, t), tok_z_send.at[0], tok_recv.at[1 + k, j, 0], pair
        )

    def have_slot(k, j):
        if k == 0:
            return j // (SUBS // 2)
        return 2 if k == 1 else 3 + max(0, j - 1)

    def tok_share(k, j, kind):
        at = piece(slot_of(k), j, beyond_t if kind == 2 else t)
        if kind == 1:
            return remote(at, at, tok_t_send.at[k], tok_recv.at[k, j, 1], beyond)
        return remote(at, at, tok_t_send.at[k], tok_have.at[have_slot(k, j)], mate)

    def tok_wait(k, j, kind):
        at = piece(slot_of(k), j, t)
        remote(at, at, tok_t_send.at[k], tok_recv.at[k, j, kind], mate).wait_recv()

    def take(k, j):
        tok_wait(k, j, 0)
        if k < 2 or j >= Y_PAIRS:
            tok_share(k, j, 1).start()
        tok_share(k, j, 0).start()
        if k == 1 and j < Z_FIRST:
            tok_y(1, j).start()

    def hand(k, j):
        tok_wait(k, j, 1)
        tok_share(k, j, 2).start()

    def have(index, pieces):
        at = toks.at[0, pl.ds(0, pieces * part)]
        remote(at, at, tok_t_send.at[0], tok_have.at[index], mate).wait_recv()

    def pieces_sent(send, pieces):
        at = toks.at[0, pl.ds(0, pieces * part)]
        remote(at, at, send, tok_have.at[0], mate).wait_send()

    def norm_own():
        @pl.loop(0, blocks)
        def _(b):
            at = pl.ds(pl.multiple_of(b * WINDOW, WINDOW), WINDOW)
            values = toks[f, at, :].astype(jnp.float32)
            scaling = lax.rsqrt(jnp.mean(values * values, axis=-1, keepdims=True) + EPSILON)
            toks[f, at, :] = (values * scaling * gain[...]).astype(jnp.bfloat16)

    mm_rows = rows // 2

    def make_bias():
        key = lax.broadcasted_iota(jnp.int32, (3 * WINDOW, WINDOW), 0)
        query = lax.broadcasted_iota(jnp.int32, (3 * WINDOW, WINDOW), 1)
        away = jnp.abs(query - key + WINDOW)
        for h in range(heads):
            index = (t * (2 * heads) + f * heads + h + 1).astype(jnp.float32)
            slope = jnp.exp2(jnp.full((1, WINDOW), -8.0 / (2 * heads * tps), jnp.float32) * index)
            cols = pl.ds(h * WINDOW, WINDOW)
            bias[:, cols] = jnp.where(away <= WINDOW, -slope * away.astype(jnp.float32), FAR)
            sink_row[:, cols] = jnp.full((1, WINDOW), sinks[f * heads + h], jnp.float32)

    scale = 1.0 / math.sqrt(HEAD)
    half_k = depth * SPAN
    near_k = pl.multiple_of(jnp.where(low_half, 0, half_k), 128)
    far_k = pl.multiple_of(half_k - near_k, 128)

    def partial(g, slot, at, k_off):
        return jnp.dot(
            toks[slot, pl.ds(at, mm_rows), pl.ds(k_off, half_k)],
            wts[g, pl.ds(k_off, half_k), :],
            preferred_element_type=jnp.float32,
        )

    def sums(g, slot):
        return slot if g == 0 else slot + 4 * g - 2

    def halves_of(b):
        return pl.loop(0, 2) if b is None else lambda body: body(b)

    def near(g, slot, only=None):
        @halves_of(only)
        def _(b):
            at = pl.multiple_of(b * mm_rows, WINDOW)
            acc[sums(g, slot), pl.ds(at, mm_rows), :] = partial(g, slot, at, near_k)

    def total(g, slot, at):
        return acc[sums(g, slot), pl.ds(at, mm_rows), :] + partial(g, slot, at, far_k)

    def project_qkv(seq):
        @pl.loop(0, 2)
        def _(b):
            at = pl.multiple_of(b * mm_rows, WINDOW)
            out = total(0, seq, at)
            qs[seq, pl.ds(at, mm_rows), :] = (out[:, :qcols] * scale).astype(jnp.bfloat16)
            kvs[seq, pl.ds(at + WINDOW, mm_rows), :] = out[:, qcols:].astype(jnp.bfloat16)

    kv_len = kvs.shape[1]

    def kv_copies(seq, slot):
        ref = kvs.at[seq]
        climb = remote(
            ref.at[pl.ds(kv_len - 2 * WINDOW, WINDOW)],
            ref.at[pl.ds(0, WINDOW)],
            kv_send.at[slot, 0],
            kv_recv.at[slot, 0],
            up,
        )
        fall = remote(
            ref.at[pl.ds(WINDOW, WINDOW)],
            ref.at[pl.ds(kv_len - WINDOW, WINDOW)],
            kv_send.at[slot, 1],
            kv_recv.at[slot, 1],
            down,
        )
        return climb, fall

    def kv_start(seq, slot):
        climb, fall = kv_copies(seq, slot)
        blank = jnp.zeros((WINDOW, 2 * HEAD), jnp.bfloat16)

        @pl.when(has_up)
        def _():
            climb.start()

        @pl.when(has_down)
        def _():
            fall.start()

        @pl.when(jnp.logical_not(has_up))
        def _():
            kvs[seq, pl.ds(kv_len - WINDOW, WINDOW), :] = blank

        @pl.when(jnp.logical_not(has_down))
        def _():
            kvs[seq, pl.ds(0, WINDOW), :] = blank

    def kv_wait(seq, slot):
        climb, fall = kv_copies(seq, slot)

        @pl.when(has_up)
        def _():
            climb.wait_send()
            fall.wait_recv()

        @pl.when(has_down)
        def _():
            fall.wait_send()
            climb.wait_recv()

    def attend(seq, first, count, step=1, closed=False):
        @pl.loop(0, count)
        def _(i):
            b = first + i * step
            at = pl.multiple_of(b * WINDOW, WINDOW)
            kv = kvs[seq, pl.ds(at, 3 * WINDOW), :]
            keys = kv[:, :HEAD]
            values_t = kv.astype(jnp.float32).T[HEAD:, :].astype(jnp.bfloat16)
            queries = qs[seq, pl.ds(at, WINDOW), :]
            stacked = jnp.concatenate(
                [queries[:, h * HEAD : (h + 1) * HEAD] for h in range(heads)], axis=0
            )
            scores = lax.dot_general(
                keys, stacked, (((1,), (1,)), ((), ())), preferred_element_type=jnp.float32
            )
            scores = scores + bias[...]
            if closed:
                low = jnp.where((b == 0) & (s == 0), FAR, 0.0)
                high = jnp.where((b == blocks - 1) & (s == SPAN - 1), FAR, 0.0)
                scores = jnp.concatenate(
                    [
                        scores[:WINDOW] + low,
                        scores[WINDOW : 2 * WINDOW],
                        scores[2 * WINDOW :] + high,
                    ],
                    axis=0,
                )
            sink = sink_row[...]
            peak = jnp.maximum(jnp.max(scores, axis=0, keepdims=True), sink)
            weights = jnp.exp(scores - peak)
            total = jnp.sum(weights, axis=0, keepdims=True) + jnp.exp(sink - peak)
            mixed = jnp.dot(
                values_t, weights.astype(jnp.bfloat16), preferred_element_type=jnp.float32
            )
            mixed = mixed / total
            logs = peak + jnp.log(total)
            outs = []
            for h in range(heads):
                cols = slice(h * WINDOW, (h + 1) * WINDOW)
                outs.append(mixed[:, cols])
                log_st[seq, pl.ds(h, 1), pl.ds(at, WINDOW)] = logs[:, cols]
            attn_st[seq, pl.ds(at, WINDOW), :] = (
                jnp.concatenate(outs, axis=0).T.astype(jnp.bfloat16)
            )

    half_cols = pl.ds(pl.multiple_of(f * qcols, 128), qcols)

    def attn_return(own):
        seq = f if own else other
        pairs = [
            (attn_st.at[seq], attn_out.at[:, half_cols]),
            (log_st.at[seq], log_out.at[f]),
        ]
        if own:
            return [pltpu.make_async_copy(a, b, misc_sem.at[1 + i]) for i, (a, b) in enumerate(pairs)]
        return [
            remote(a, b, ret_send.at[i], ret_recv.at[i], across) for i, (a, b) in enumerate(pairs)
        ]

    def conv_cols(g):
        return pl.ds(pl.multiple_of(f * (2 * chans) + (g - 1) * chans, 128), chans)

    split = mm_rows - pad
    head_b = jnp.where(low_half, 1, 0)
    spans = {
        None: (0, rows),
        "head": (jnp.where(low_half, rows - split, 0), split),
        "tail": (jnp.where(low_half, 0, split), rows - split),
    }

    def conv_return(g, own_seq, own_rows, span=None):
        seq = f if own_seq else other
        off = own_off if own_rows else end_off
        lo, count = spans[span]
        src = conv_st.at[g - 1, seq, pl.ds(pl.multiple_of(off + lo, pad), count)]
        dst = conv_out.at[pl.ds(pl.multiple_of(lo, pad), count), conv_cols(g)]
        if own_seq and own_rows:
            return pltpu.make_async_copy(src, dst, own_sem.at[g - 1])
        if own_seq:
            return remote(src, dst, conv_send.at[g - 1, 0], conv_recv.at[g - 1, 0], pair)
        if own_rows:
            return remote(src, dst, conv_send.at[g - 1, 1], conv_recv.at[g - 1, 1], across)
        last = 1 if span == "tail" else 0
        return remote(
            src, dst, conv_send.at[g - 1, 2 + last], conv_recv.at[g - 1, 1 + last], diag
        )

    def project_conv(g, seq, own_rows, only=None):
        slot, off = (seq, own_off) if own_rows else (2 + seq, end_off)

        @halves_of(only)
        def _(b):
            at = pl.multiple_of(b * mm_rows, WINDOW)
            to = pl.multiple_of(off + b * mm_rows, WINDOW)
            out = total(g, slot, at)
            inner = out[:, :chans].astype(jnp.bfloat16).astype(jnp.float32)
            signal = out[:, chans : 2 * chans].astype(jnp.bfloat16).astype(jnp.float32)
            prod[g - 1, seq, pl.ds(to + pad, mm_rows), :] = (inner * signal).astype(jnp.bfloat16)
            outer[g - 1, seq, pl.ds(to, mm_rows), :] = out[:, 2 * chans :].astype(jnp.bfloat16)

    def project_tail(g, j):
        at = pl.multiple_of(jnp.where(low_half, SUBS - 1 - j, j) * sub, 16)
        out = jnp.dot(
            toks[2 + other, pl.ds(at, sub), :], wts[g], preferred_element_type=jnp.float32
        )
        inner = out[:, :chans].astype(jnp.bfloat16).astype(jnp.float32)
        signal = out[:, chans : 2 * chans].astype(jnp.bfloat16).astype(jnp.float32)
        to = pl.multiple_of(end_off + at, 16)
        prod[g - 1, other, pl.ds(to + pad, sub), :] = (inner * signal).astype(jnp.bfloat16)
        outer[g - 1, other, pl.ds(to, sub), :] = out[:, 2 * chans :].astype(jnp.bfloat16)

    def pr_copies(g, seq, slot):
        ref = prod.at[g - 1, seq]
        climb = remote(
            ref.at[pl.ds(both_rows, pad)],
            ref.at[pl.ds(0, pad)],
            pr_send.at[g - 1, slot],
            pr_recv.at[g - 1, slot],
            mid,
        )
        fall = remote(
            ref.at[pl.ds(pad, pad)],
            ref.at[pl.ds(both_rows + pad, pad)],
            pr_send.at[g - 1, slot],
            pr_recv.at[g - 1, slot],
            mid,
        )
        return climb, fall

    def pr_start(g, seq, slot):
        climb, fall = pr_copies(g, seq, slot)
        blank = jnp.zeros((pad, chans), jnp.bfloat16)

        @pl.when(low_half)
        def _():
            climb.start()
            prod[g - 1, seq, pl.ds(0, pad), :] = blank

        @pl.when(jnp.logical_not(low_half))
        def _():
            fall.start()
            prod[g - 1, seq, pl.ds(both_rows + pad, pad), :] = blank

    def pr_wait(g, seq, slot):
        climb, fall = pr_copies(g, seq, slot)

        @pl.when(low_half)
        def _():
            climb.wait_send()
            fall.wait_recv()

        @pl.when(jnp.logical_not(low_half))
        def _():
            fall.wait_send()
            climb.wait_recv()

    def mix(g, seq, own_rows, span=None):
        lo, count = spans[span]
        off = pl.multiple_of((own_off if own_rows else end_off) + lo, pad)
        tap = taps[:, conv_cols(g)]
        size = count + 2 * pad
        full = prod[g - 1, seq, pl.ds(off, size), :].astype(jnp.float32)
        before = pltpu.roll(full, 1, 0)[pad : pad + count]
        after = pltpu.roll(full, size - 1, 0)[pad : pad + count]
        mixed = tap[0:1] * before + tap[1:2] * full[pad : pad + count] + tap[2:3] * after
        gate = outer[g - 1, seq, pl.ds(off, count), :].astype(jnp.float32)
        conv_st[g - 1, seq, pl.ds(off, count), :] = (gate * mixed).astype(jnp.bfloat16)

    finish(small[:2])
    keys0, vals0 = kv_raw[0], kv_raw[1]
    halves = [
        jnp.concatenate([w[:, i * HEAD : (i + 1) * HEAD] for w in (keys0, vals0)], axis=1)
        for i in range(2)
    ]
    first = f == 0
    stage_w[0, :, pl.ds(qcols, 2 * HEAD)] = jnp.where(first, halves[1], halves[0])
    wts[0, block_rows(mine), pl.ds(qcols, 2 * HEAD)] = jnp.where(first, halves[0], halves[1])

    pl.semaphore_wait(barrier, jnp.where(is_mid, 6, 5))

    loaded(0, own_dest[0], load_sem)
    to_pair(0, mine).start()

    @pl.when(is_mid)
    def _():
        to_mid(0, mine).start()

    loaded(0, stage_w.at[0], stage_sem)
    loaded(1, stage_w.at[1], stage_sem)

    @pl.when(is_end)
    def _():
        y_copy(0).start()
        y_copy(1).start()

    loaded(1, own_dest[1], load_sem)

    @pl.when(is_mid)
    def _():
        to_mid(1, mine).start()

    finish(small[2:])
    for i in range(gain_raw.shape[0]):
        gain[:, i * 128 : (i + 1) * 128] = gain_raw[i : i + 1, :]
    tok_load.wait()
    norm_own()
    tok_y(0, 0).start()

    @pl.when(is_mid)
    def _():
        y_copy(0).start()

    for j in range(1, SUBS):
        tok_y(0, j).start()

    @pl.when(is_mid)
    def _():
        y_copy(1).start()

    loaded(2, stage_w.at[2], stage_sem)
    y_copy(2).start()
    loaded(2, own_dest[2], load_sem)

    def relay(g, blk, onward):
        arrived(g, blk)
        onward(g, blk).start()

    pt = [partner * 2 + f, partner * 2 + other]
    ct = [facing * 2 + f, facing * 2 + other]
    ft = [far * 2 + f, far * 2 + other]

    def end_program():
        tok_z(0, 0).start()
        make_bias()
        relay(0, theirs, to_pair)
        tok_z(0, 1).start()
        to_pair(1, mine).start()
        relay(1, theirs, to_pair)
        tok_z(0, 2).start()
        tok_z(0, 3).start()
        take(0, 0)
        for blk in pt:
            arrived(0, blk)
        near(0, f)
        take(0, 1)
        hand(0, 0)
        take(0, 2)
        hand(0, 1)
        take(0, 3)
        hand(0, 2)
        have(0, 2 * (SUBS // 2))
        near(0, other, head_b)
        for blk in ct + ft:
            arrived(0, blk)
        project_qkv(f)
        kv_start(f, 0)
        to_pair(2, mine).start()
        hand(0, 3)
        have(1, 2 * (SUBS // 2))
        near(0, other, 1 - head_b)
        project_qkv(other)
        kv_start(other, 1)
        relay(2, theirs, to_pair)
        for j in range(Z_FIRST, SUBS):
            tok_z(1, j).start()
        attend(f, 1, blocks - 2)
        attend(other, 1, blocks - 2)
        kv_wait(f, 0)
        attend(f, 0, 2, blocks - 1, True)
        begin(attn_return(True))
        kv_wait(other, 1)
        attend(other, 0, 2, blocks - 1, True)
        begin(attn_return(False))
        for g in (1, 2):
            conv_return(g, True, False).wait_recv()
            conv_return(g, False, False, "head").wait_recv()
            conv_return(g, False, False, "tail").wait_recv()
        blocks_sent(pair_send.at[0], 2 * GROUPS)
        pieces_sent(tok_z_send.at[0], 2 * SUBS - Z_FIRST)

    def conv_own(g, own_seq):
        seq, slot = (f, 0) if own_seq else (other, 1)
        project_conv(g, seq, True)
        pr_start(g, seq, slot)

    def conv_close(g, own_seq):
        seq, slot = (f, 0) if own_seq else (other, 1)
        pr_wait(g, seq, slot)
        mix(g, seq, True)
        conv_return(g, own_seq, True).start()

    def conv_end(g):
        project_conv(g, f, False)
        mix(g, f, False)
        conv_return(g, True, False).start()

    def conv_end_close(g, span):
        mix(g, other, False, span)
        conv_return(g, False, False, span).start()

    def mid_program():
        half = (blocks - 2) // 2
        make_bias()
        relay(0, ct[0], to_pair)
        relay(0, pt[0], to_mid)
        take(0, 0)
        take(1, 0)
        relay(0, theirs, to_mid)
        to_pair(0, theirs).start()
        hand(0, 0)
        relay(0, pt[1], to_mid)
        to_mid(2, mine).start()
        near(0, f)
        take(0, 1)
        relay(0, ct[1], to_pair)
        hand(1, 0)
        take(0, 2)
        relay(0, ft[0], to_pair)
        take(1, 1)
        hand(0, 1)
        have(0, 2 * (SUBS // 2))
        near(0, other, head_b)
        relay(0, ft[1], to_pair)
        take(0, 3)
        relay(1, pt[0], to_mid)
        project_qkv(f)
        kv_start(f, 0)
        hand(0, 2)
        attend(f, 1, half)
        relay(1, theirs, to_mid)
        attend(f, 1 + half, half)
        relay(1, pt[1], to_mid)
        near(1, f)
        hand(0, 3)
        have(1, 2 * (SUBS // 2))
        near(0, other, 1 - head_b)
        project_qkv(other)
        kv_start(other, 1)
        relay(2, theirs, to_mid)
        take(1, 2)
        tok_y(2, 0).start()
        attend(other, 1, half)
        hand(1, 1)
        attend(other, 1 + half, half)
        near(1, other)
        take(1, 3)
        kv_wait(f, 0)
        attend(f, 0, 2, blocks - 1)
        begin(attn_return(True))
        hand(1, 2)
        take(2, 0)
        relay(2, pt[0], to_mid)
        for blk in ct + ft:
            arrived(1, blk)
        conv_own(1, True)
        take(2, 1)
        conv_own(1, False)
        kv_wait(other, 1)
        attend(other, 0, 2, blocks - 1)
        begin(attn_return(False))
        hand(1, 3)
        relay(2, pt[1], to_mid)
        have(2, 2 * SUBS)
        near(1, 2 + f)
        take(2, 2)
        conv_end(1)
        near(2, 2 + f)
        conv_close(1, True)
        hand(2, 1)
        near(2, f)
        hand(2, 0)
        take(2, 3)
        have(3, 4)
        near(1, 2 + other, head_b)
        project_conv(1, other, False, head_b)
        conv_end_close(1, "head")
        conv_close(1, False)
        near(2, other)
        hand(2, 2)
        near(2, 2 + other, head_b)
        for blk in ct + ft:
            arrived(2, blk)
        conv_own(2, True)
        conv_end(2)
        have(4, 2)
        project_tail(1, 2)
        hand(2, 3)
        conv_own(2, False)
        project_conv(2, other, False, head_b)
        conv_end_close(2, "head")
        conv_close(2, False)
        have(5, 2)
        project_tail(1, 3)
        conv_end_close(1, "tail")
        project_tail(2, 2)
        project_tail(2, 3)
        conv_end_close(2, "tail")
        conv_close(2, True)
        for g in (1, 2):
            conv_return(g, False, True).wait_recv()
            conv_return(g, True, True).wait()
            conv_return(g, False, True).wait_send()
            conv_return(g, True, False).wait_send()
            conv_return(g, False, False, "head").wait_send()
            conv_return(g, False, False, "tail").wait_send()
            pieces_sent(tok_t_send.at[g], 3 * SUBS if g == 1 else 3 * SUBS - Y_PAIRS)
        blocks_sent(pair_send.at[0], 6)
        for g in range(GROUPS):
            blocks_sent(mid_send.at[g], 4)
        pieces_sent(tok_y_send.at[1], Z_FIRST + Y_PAIRS)

    pl.when(is_end)(end_program)
    pl.when(is_mid)(mid_program)

    for g in range(GROUPS):
        y_copy(g).wait_send()
    pieces_sent(tok_y_send.at[0], SUBS)
    pieces_sent(tok_t_send.at[0], 3 * SUBS)
    for own in (True, False):
        finish(attn_return(own))


def fused_device(
    tps,
    tokens,
    norm_gain,
    query_weight,
    key_weight,
    value_weight,
    outer_weight,
    inner_weight,
    signal_weight,
    conv_taps,
    sink_logit,
):
    rows, width = tokens.shape[1:]
    depth, local = query_weight.shape
    qcols = local // 2
    heads = qcols // HEAD
    chans = outer_weight.shape[1] // 4
    head_local = 2 * heads
    group_cols = qcols + 2 * HEAD
    pad = 16
    bf, f32 = jnp.bfloat16, jnp.float32
    dma = pltpu.SemaphoreType.DMA
    hbm = pl.BlockSpec(memory_space=pltpu.HBM)
    anyspace = pl.BlockSpec(memory_space=pl.ANY)
    attended, conv, logs = pl.pallas_call(
        functools.partial(mega_kernel, tps),
        out_shape=(
            jax.ShapeDtypeStruct((rows, local), bf),
            jax.ShapeDtypeStruct((rows, 4 * chans), bf),
            jax.ShapeDtypeStruct((2, heads, rows), f32),
        ),
        in_specs=[hbm] * 10,
        out_specs=(anyspace, anyspace, anyspace),
        scratch_shapes=[
            pltpu.VMEM((4, rows, width), bf),
            pltpu.VMEM((GROUPS, width, group_cols), bf),
            pltpu.VMEM((GROUPS, depth, group_cols), bf),
            pltpu.VMEM((2, rows, qcols), bf),
            pltpu.VMEM((2, rows + 2 * WINDOW, 2 * HEAD), bf),
            pltpu.VMEM((3 * WINDOW, heads * WINDOW), f32),
            pltpu.VMEM((1, heads * WINDOW), f32),
            pltpu.VMEM((2, 2, 2 * rows + 2 * pad, chans), bf),
            pltpu.VMEM((2, 2, 2 * rows, chans), bf),
            pltpu.VMEM((2, rows, qcols), bf),
            pltpu.VMEM((2, heads, rows), f32),
            pltpu.VMEM((2, 2, 2 * rows, chans), bf),
            pltpu.VMEM((10, rows, group_cols), f32),
            pltpu.VMEM((2, depth, 2 * HEAD), bf),
            pltpu.VMEM((width // 128, 128), f32),
            pltpu.VMEM((1, width), f32),
            pltpu.VMEM((3, 4 * chans), f32),
            pltpu.SMEM((head_local,), f32),
            dma((5,)),
            dma((GROUPS,)),
            dma((GROUPS,)),
            dma((3,)),
            dma((2,)),
            dma((GROUPS,)),
            dma((GROUPS, 2 * SPAN)),
            dma((1,)),
            dma((GROUPS,)),
            dma((2,)),
            dma((1,)),
            dma((3,)),
            dma((3, SUBS, 2)),
            dma((6,)),
            dma((2, 2)),
            dma((2, 2)),
            dma((2, 2)),
            dma((2, 2)),
            dma((2,)),
            dma((2,)),
            dma((2, 4)),
            dma((2, 3)),
        ],
        compiler_params=pltpu.CompilerParams(
            collective_id=0, has_side_effects=True, vmem_limit_bytes=48 << 20
        ),
    )(
        *(
            pltpu.with_memory_space_constraint(x, pltpu.HBM)
            for x in (
                tokens[0],
                norm_gain.reshape(width // 128, 128),
                query_weight,
                key_weight,
                value_weight,
                outer_weight,
                inner_weight,
                signal_weight,
                conv_taps,
                sink_logit,
            )
        )
    )
    return (attended[None], conv[None], logs.reshape(1, head_local, rows))


def fits(mesh, args):
    tokens, query_weight, key_weight, outer_weight = (args[i] for i in (0, 2, 3, 5))
    sp, fs, tp = (mesh.shape[a] for a in ("sp", "fs", "tp"))
    rows = tokens.shape[1] // sp
    return (
        fs == 2
        and sp == SPAN
        and tokens.shape[0] == fs
        and tp == 4
        and rows % (2 * WINDOW) == 0
        and rows // WINDOW % 2 == 0
        and rows % (16 * SUBS * tp) == 0
        and key_weight.shape[1] == 2 * HEAD * tp
        and query_weight.shape[1] % (256 * tp) == 0
        and outer_weight.shape[1] == 512 * tp
        and query_weight.shape[1] == 512 * tp
        and query_weight.shape[0] % (16 * sp * fs) == 0
    )


def solution(mesh):
    in_specs = (
        P("fs", "sp", None),
        P(),
        P(("sp", "fs"), "tp"),
        P(("sp", "fs"), "tp"),
        P(("sp", "fs"), "tp"),
        P(("sp", "fs"), "tp"),
        P(("sp", "fs"), "tp"),
        P(("sp", "fs"), "tp"),
        P(None, "tp"),
        P("tp"),
    )
    out_specs = (P("fs", "sp", "tp"), P("fs", "sp", "tp"), P("fs", "tp", "sp"))

    def run(*args):
        body = per_device
        if fits(mesh, args):
            body = functools.partial(fused_device, mesh.shape["tp"])
        return jax.shard_map(
            body, mesh=mesh, in_specs=in_specs, out_specs=out_specs, check_vma=False
        )(*args)

    return run
```

```python
import math

import functools

import jax
import jax.numpy as jnp
from jax import lax
from jax.experimental import pallas as pl
from jax.experimental.pallas import tpu as pltpu
from jax.sharding import PartitionSpec as P

HEAD = 64
WINDOW = 128


EPSILON = 1e-06


def extended(value, sides, width):
    for axis, dim in sides:
        size, length = (lax.axis_size(axis), value.shape[dim])
        up = [(i, (i + 1) % size) for i in range(size - 1)]
        down = [(j, i) for i, j in up]
        last = lax.slice_in_dim(value, length - width, length, axis=dim)
        initial = lax.slice_in_dim(value, 0, width, axis=dim)
        before = lax.ppermute(last, axis, up)
        after = lax.ppermute(initial, axis, down)
        value = jnp.concatenate([before, value, after], axis=dim)
    return value


def normalized(tokens, norm_gain):
    values = tokens.astype(jnp.float32)
    scaling = lax.rsqrt(jnp.mean(values * values, axis=-1, keepdims=True) + EPSILON)
    return (values * scaling * norm_gain).astype(jnp.bfloat16)


def folding(normed):

    def add_portions(running, portions, offset):
        return tuple(
            (jnp.dot(normed, portion, preferred_element_type=jnp.float32) for portion in portions)
        )

    return add_portions


def empty_sums(normed, weights):
    return tuple((jnp.zeros((normed.shape[0], weight.shape[1]), jnp.float32) for weight in weights))


def rounded(results):
    return tuple((result.astype(jnp.bfloat16) for result in results))


def gate_product(inner_gate, signal):
    return (inner_gate.astype(jnp.float32) * signal.astype(jnp.float32)).astype(jnp.bfloat16)


def send_edges(key_proj, value_proj, product):
    stacked = jnp.concatenate([key_proj, value_proj], axis=1)
    window_rows = extended(stacked, (("sp", 0),), WINDOW)
    conv_rows = extended(product, (("sp", 0),), 1)
    return (window_rows, conv_rows)


def banded_attention(queries, window_rows, sink_logit, slopes, first_pos, seq_length):
    tok_count = queries.shape[0]
    kv_cols = window_rows.shape[1] // 2
    kv_heads = kv_cols // HEAD
    group_size = queries.shape[1] // (HEAD * kv_heads)
    block_count = tok_count // WINDOW
    query_blocks = queries.reshape(block_count, WINDOW, kv_heads, group_size, HEAD)
    key_rows = window_rows[:, :kv_cols].reshape(block_count + 2, WINDOW, kv_heads, HEAD)
    value_rows = window_rows[:, kv_cols:].reshape(block_count + 2, WINDOW, kv_heads, HEAD)
    key_span = jnp.concatenate([key_rows[:-2], key_rows[1:-1], key_rows[2:]], axis=1)
    value_span = jnp.concatenate([value_rows[:-2], value_rows[1:-1], value_rows[2:]], axis=1)
    scores = jnp.einsum(
        "bqkgd,bskd->bkgqs", query_blocks, key_span, preferred_element_type=jnp.float32
    ) * (1.0 / math.sqrt(HEAD))
    distance = jnp.arange(WINDOW)[:, None] - jnp.arange(3 * WINDOW)[None, :] + WINDOW
    key_pos = (
        first_pos
        - WINDOW
        + WINDOW * jnp.arange(block_count)[:, None]
        + jnp.arange(3 * WINDOW)[None, :]
    )
    inside = (jnp.abs(distance)[None] <= WINDOW) & ((key_pos >= 0) & (key_pos < seq_length))[
        :, None, :
    ]
    scores = scores - slopes.reshape(kv_heads, group_size, 1, 1) * jnp.abs(distance).astype(
        jnp.float32
    )
    scores = jnp.where(inside[:, None, None], scores, -jnp.inf)
    sink_grid = sink_logit.reshape(kv_heads, group_size, 1, 1)
    row_peak = jnp.maximum(jnp.max(scores, axis=-1, keepdims=True), sink_grid)
    weights = jnp.exp(scores - row_peak)
    row_total = jnp.sum(weights, axis=-1, keepdims=True) + jnp.exp(sink_grid - row_peak)
    weighted = jnp.einsum(
        "bkgqs,bskd->bqkgd",
        weights.astype(jnp.bfloat16),
        value_span,
        preferred_element_type=jnp.float32,
    )
    attended = (
        (weighted / row_total.transpose(0, 3, 1, 2, 4))
        .astype(jnp.bfloat16)
        .reshape(tok_count, kv_heads * group_size * HEAD)
    )
    log_total = (
        (row_peak + jnp.log(row_total))[..., 0]
        .transpose(1, 2, 0, 3)
        .reshape(kv_heads * group_size, tok_count)
    )
    return (attended, log_total)


def per_device(
    tokens,
    norm_gain,
    query_weight,
    key_weight,
    value_weight,
    outer_weight,
    inner_weight,
    signal_weight,
    conv_taps,
    sink_logit,
):
    normed = normalized(tokens[0], norm_gain)
    add_portions = folding(normed)
    all_sums = add_portions(
        empty_sums(
            normed,
            (query_weight, key_weight, value_weight, outer_weight, inner_weight, signal_weight),
        ),
        (
            lax.all_gather(query_weight, ("sp", "fs"), axis=0, tiled=True),
            lax.all_gather(key_weight, ("sp", "fs"), axis=0, tiled=True),
            lax.all_gather(value_weight, ("sp", "fs"), axis=0, tiled=True),
            lax.all_gather(outer_weight, ("sp", "fs"), axis=0, tiled=True),
            lax.all_gather(inner_weight, ("sp", "fs"), axis=0, tiled=True),
            lax.all_gather(signal_weight, ("sp", "fs"), axis=0, tiled=True),
        ),
        jnp.int32(0),
    )
    queries, key_proj, value_proj, outer_gate, inner_gate, signal = rounded(all_sums)
    product = gate_product(inner_gate, signal)
    window_rows, conv_rows = send_edges(key_proj, value_proj, product)
    tok_count = normed.shape[0]
    head_local = queries.shape[1] // HEAD
    head_index = lax.axis_index("tp") * head_local + jnp.arange(1, head_local + 1)
    slopes = jnp.exp2(-8.0 * head_index.astype(jnp.float32) / (head_local * lax.axis_size("tp")))
    first_pos = lax.axis_index("sp") * tok_count
    attended, log_total = banded_attention(
        queries, window_rows, sink_logit, slopes, first_pos, tok_count * lax.axis_size("sp")
    )
    mixed_conv = conv_taps[0] * conv_rows[0:tok_count].astype(jnp.float32)
    mixed_conv = mixed_conv + conv_taps[1] * conv_rows[1 : tok_count + 1].astype(jnp.float32)
    mixed_conv = mixed_conv + conv_taps[2] * conv_rows[2 : tok_count + 2].astype(jnp.float32)
    conv_out = (outer_gate.astype(jnp.float32) * mixed_conv).astype(jnp.bfloat16)
    return (attended[None], conv_out[None], log_total[None])


MESH = pl.DeviceIdType.MESH
GROUPS = 3
SPAN = 4
SUBS = 4
Y_PAIRS = 1
Z_FIRST = 3
FAR = -1e30


def mega_kernel(
    tps,
    tokens,
    gain_in,
    qw,
    kw,
    vw,
    ow,
    iw,
    sw,
    taps_in,
    sinks_in,
    attn_out,
    conv_out,
    log_out,
    toks,
    wts,
    stage_w,
    qs,
    kvs,
    bias,
    sink_row,
    prod,
    outer,
    attn_st,
    log_st,
    conv_st,
    acc,
    kv_raw,
    gain_raw,
    gain,
    taps,
    sinks,
    small_sem,
    load_sem,
    stage_sem,
    misc_sem,
    own_sem,
    y_send,
    w_recv,
    pair_send,
    mid_send,
    tok_y_send,
    tok_z_send,
    tok_t_send,
    tok_recv,
    tok_have,
    kv_send,
    kv_recv,
    pr_send,
    pr_recv,
    ret_send,
    ret_recv,
    conv_send,
    conv_recv,
):
    s, f, t = lax.axis_index("sp"), lax.axis_index("fs"), lax.axis_index("tp")
    other = 1 - f
    core = lax.rem(t, 2)
    outward = 1 - lax.rem(s, 2)
    partner = s + 2 * outward - 1
    facing = SPAN - 1 - s
    far = SPAN - 1 - partner
    is_mid = (s == 1) | (s == SPAN - 2)
    is_end = jnp.logical_not(is_mid)
    low_half = s < SPAN // 2
    pair, diag, mid = (partner, f, t), (partner, other, t), (facing, f, t)
    across = (s, other, t)
    mate_t, beyond_t = t + 1 - 2 * core, lax.rem(t + 2, tps)
    mate, beyond = (s, f, mate_t), (s, f, beyond_t)
    rows = tokens.shape[0]
    depth = qw.shape[0]
    qcols = qs.shape[2]
    heads = qcols // HEAD
    chans = prod.shape[3]
    both_rows = outer.shape[2]
    blocks = rows // WINDOW
    pad = (prod.shape[2] - both_rows) // 2
    sub = rows // SUBS
    part = sub // tps
    up, down = (s + 1, f, t), (s - 1, f, t)
    has_up, has_down = s < SPAN - 1, s > 0
    own_off = jnp.where(low_half, rows, 0)
    end_off = rows - own_off

    barrier = pltpu.get_barrier_semaphore()
    for peer in (pair, diag, across, mate, beyond):
        pl.semaphore_signal(barrier, inc=1, device_id=peer, device_id_type=MESH)

    @pl.when(is_mid)
    def _():
        pl.semaphore_signal(barrier, inc=1, device_id=mid, device_id_type=MESH)

    def block_rows(blk):
        return pl.ds(pl.multiple_of(blk * depth, 16), depth)

    def loads(g, half, dest, sems):
        if g == 0:
            qc = pl.ds(pl.multiple_of(half * qcols, 128), qcols)
            pairs = [(qw.at[:, qc], dest.at[:, pl.ds(0, qcols)])]
        else:
            c = pl.ds(pl.multiple_of(half * (2 * chans) + (g - 1) * chans, 128), chans)
            pairs = [
                (ref.at[:, c], dest.at[:, pl.ds(i * chans, chans)])
                for i, ref in enumerate((iw, sw, ow))
            ]
        return [pltpu.make_async_copy(a, b, sems.at[g]) for a, b in pairs]

    def loaded(g, dest, sems):
        whole = dest.at[:, pl.ds(0, qcols)] if g == 0 else dest
        pltpu.make_async_copy(whole, whole, sems.at[g]).wait()

    mine = s * 2 + f
    theirs = s * 2 + other
    own_dest = [wts.at[g, block_rows(mine)] for g in range(GROUPS)]
    own_loads = [loads(g, f, own_dest[g], load_sem) for g in range(GROUPS)]
    out_loads = [loads(g, other, stage_w.at[g], stage_sem) for g in range(GROUPS)]
    small = [
        pltpu.make_async_copy(a, b, small_sem.at[i])
        for i, (a, b) in enumerate(
            (
                (kw, kv_raw.at[0]),
                (vw, kv_raw.at[1]),
                (gain_in, gain_raw),
                (taps_in, taps),
                (sinks_in, sinks),
            )
        )
    ]
    tok_load = pltpu.make_async_copy(tokens, toks.at[f], misc_sem.at[0])

    def begin(copies):
        for c in copies:
            c.start()

    def finish(copies):
        for c in copies:
            c.wait()

    begin(small[:2] + out_loads[0] + own_loads[0] + small[2:])
    tok_load.start()
    begin(out_loads[1] + own_loads[1] + out_loads[2] + own_loads[2])

    def remote(src, dst, send, recv, peer):
        return pltpu.make_async_remote_copy(
            src_ref=src,
            dst_ref=dst,
            send_sem=send,
            recv_sem=recv,
            device_id=peer,
            device_id_type=MESH,
        )

    def y_copy(g):
        return remote(
            stage_w.at[g], wts.at[g, block_rows(mine)], y_send.at[g], w_recv.at[g, mine], across
        )

    def block_copy(g, blk, send, peer):
        at = wts.at[g, block_rows(blk)]
        return remote(at, at, send, w_recv.at[g, blk], peer)

    def to_pair(g, blk):
        return block_copy(g, blk, pair_send.at[0], pair)

    def to_mid(g, blk):
        return block_copy(g, blk, mid_send.at[g], mid)

    def blocks_sent(send, count):
        at = wts.at[0, pl.ds(0, count * depth)]
        remote(at, at, send, w_recv.at[0, 0], across).wait_send()

    def arrived(g, blk):
        to_pair(g, blk).wait_recv()

    def slot_of(k):
        return (other, 2 + f, 2 + other)[k]

    def piece(slot, j, q):
        place = jnp.where(low_half, SUBS - 1 - j, j)
        return toks.at[slot, pl.ds(pl.multiple_of(place * sub + q * part, 16), part)]

    def tok_y(k, j):
        slot = f if k == 0 else 2 + f
        at = piece(slot, j, beyond_t if k == 2 else t)
        return remote(
            at, at, tok_y_send.at[1 if k else 0], tok_recv.at[2 if k else 0, j, k // 2], across
        )

    def tok_z(k, j):
        seq = f if k == 0 else other
        return remote(
            piece(seq, j, t), piece(2 + seq, j, t), tok_z_send.at[0], tok_recv.at[1 + k, j, 0], pair
        )

    def have_slot(k, j):
        if k < 2:
            return 2 * k + j // (SUBS // 2)
        return 4 + max(0, j - 1)

    def tok_share(k, j, kind):
        at = piece(slot_of(k), j, beyond_t if kind == 2 else t)
        if kind == 1:
            return remote(at, at, tok_t_send.at[k], tok_recv.at[k, j, 1], beyond)
        return remote(at, at, tok_t_send.at[k], tok_have.at[have_slot(k, j)], mate)

    def tok_wait(k, j, kind):
        at = piece(slot_of(k), j, t)
        remote(at, at, tok_t_send.at[k], tok_recv.at[k, j, kind], mate).wait_recv()

    def take(k, j):
        tok_wait(k, j, 0)
        if k < 2 or j >= Y_PAIRS:
            tok_share(k, j, 1).start()
        tok_share(k, j, 0).start()
        if k == 1 and j < Z_FIRST:
            tok_y(1, j).start()

    def hand(k, j):
        tok_wait(k, j, 1)
        tok_share(k, j, 2).start()

    def have(index, pieces):
        at = toks.at[0, pl.ds(0, pieces * part)]
        remote(at, at, tok_t_send.at[0], tok_have.at[index], mate).wait_recv()

    def pieces_sent(send, pieces):
        at = toks.at[0, pl.ds(0, pieces * part)]
        remote(at, at, send, tok_have.at[0], mate).wait_send()

    def norm_own():
        @pl.loop(0, blocks)
        def _(b):
            at = pl.ds(pl.multiple_of(b * WINDOW, WINDOW), WINDOW)
            values = toks[f, at, :].astype(jnp.float32)
            scaling = lax.rsqrt(jnp.mean(values * values, axis=-1, keepdims=True) + EPSILON)
            toks[f, at, :] = (values * scaling * gain[...]).astype(jnp.bfloat16)

    mm_rows = rows // 2

    def make_bias():
        key = lax.broadcasted_iota(jnp.int32, (3 * WINDOW, WINDOW), 0)
        query = lax.broadcasted_iota(jnp.int32, (3 * WINDOW, WINDOW), 1)
        away = jnp.abs(query - key + WINDOW)
        for h in range(heads):
            index = (t * (2 * heads) + f * heads + h + 1).astype(jnp.float32)
            slope = jnp.exp2(jnp.full((1, WINDOW), -8.0 / (2 * heads * tps), jnp.float32) * index)
            cols = pl.ds(h * WINDOW, WINDOW)
            bias[:, cols] = jnp.where(away <= WINDOW, -slope * away.astype(jnp.float32), FAR)
            sink_row[:, cols] = jnp.full((1, WINDOW), sinks[f * heads + h], jnp.float32)

    scale = 1.0 / math.sqrt(HEAD)
    half_k = depth * SPAN
    near_k = pl.multiple_of(jnp.where(low_half, 0, half_k), 128)
    far_k = pl.multiple_of(half_k - near_k, 128)

    def partial(g, slot, at, k_off):
        return jnp.dot(
            toks[slot, pl.ds(at, mm_rows), pl.ds(k_off, half_k)],
            wts[g, pl.ds(k_off, half_k), :],
            preferred_element_type=jnp.float32,
        )

    def sums(g, slot):
        return slot if g == 0 else slot + 4 * g - 2

    def halves_of(b):
        if b is None:
            return lambda body: [body(i) for i in range(2)]
        return lambda body: body(b)

    def near(g, slot, only=None):
        @halves_of(only)
        def _(b):
            at = pl.multiple_of(b * mm_rows, WINDOW)
            acc[sums(g, slot), pl.ds(at, mm_rows), :] = partial(g, slot, at, near_k)

    def total(g, slot, at):
        return acc[sums(g, slot), pl.ds(at, mm_rows), :] + partial(g, slot, at, far_k)

    def project_qkv(seq):
        @pl.loop(0, 2)
        def _(b):
            at = pl.multiple_of(b * mm_rows, WINDOW)
            out = total(0, seq, at)
            qs[seq, pl.ds(at, mm_rows), :] = (out[:, :qcols] * scale).astype(jnp.bfloat16)
            kvs[seq, pl.ds(at + WINDOW, mm_rows), :] = out[:, qcols:].astype(jnp.bfloat16)

    kv_len = kvs.shape[1]

    def kv_copies(seq, slot):
        ref = kvs.at[seq]
        climb = remote(
            ref.at[pl.ds(kv_len - 2 * WINDOW, WINDOW)],
            ref.at[pl.ds(0, WINDOW)],
            kv_send.at[slot, 0],
            kv_recv.at[slot, 0],
            up,
        )
        fall = remote(
            ref.at[pl.ds(WINDOW, WINDOW)],
            ref.at[pl.ds(kv_len - WINDOW, WINDOW)],
            kv_send.at[slot, 1],
            kv_recv.at[slot, 1],
            down,
        )
        return climb, fall

    def kv_start(seq, slot):
        climb, fall = kv_copies(seq, slot)
        blank = jnp.zeros((WINDOW, 2 * HEAD), jnp.bfloat16)

        @pl.when(has_up)
        def _():
            climb.start()

        @pl.when(has_down)
        def _():
            fall.start()

        @pl.when(jnp.logical_not(has_up))
        def _():
            kvs[seq, pl.ds(kv_len - WINDOW, WINDOW), :] = blank

        @pl.when(jnp.logical_not(has_down))
        def _():
            kvs[seq, pl.ds(0, WINDOW), :] = blank

    def kv_wait(seq, slot):
        climb, fall = kv_copies(seq, slot)

        @pl.when(has_up)
        def _():
            climb.wait_send()
            fall.wait_recv()

        @pl.when(has_down)
        def _():
            fall.wait_send()
            climb.wait_recv()

    def attend(seq, first, count, step=1, closed=False):
        def block(i):
            b = first + i * step
            at = pl.multiple_of(b * WINDOW, WINDOW)
            kv = kvs[seq, pl.ds(at, 3 * WINDOW), :]
            keys = kv[:, :HEAD]
            values_t = kv.astype(jnp.float32).T[HEAD:, :].astype(jnp.bfloat16)
            queries = qs[seq, pl.ds(at, WINDOW), :]
            stacked = jnp.concatenate(
                [queries[:, h * HEAD : (h + 1) * HEAD] for h in range(heads)], axis=0
            )
            scores = lax.dot_general(
                keys, stacked, (((1,), (1,)), ((), ())), preferred_element_type=jnp.float32
            )
            scores = scores + bias[...]
            if closed:
                low = jnp.where((b == 0) & (s == 0), FAR, 0.0)
                high = jnp.where((b == blocks - 1) & (s == SPAN - 1), FAR, 0.0)
                scores = jnp.concatenate(
                    [
                        scores[:WINDOW] + low,
                        scores[WINDOW : 2 * WINDOW],
                        scores[2 * WINDOW :] + high,
                    ],
                    axis=0,
                )
            sink = sink_row[...]
            peak = jnp.maximum(jnp.max(scores, axis=0, keepdims=True), sink)
            weights = jnp.exp(scores - peak)
            total = jnp.sum(weights, axis=0, keepdims=True) + jnp.exp(sink - peak)
            mixed = jnp.dot(
                values_t, weights.astype(jnp.bfloat16), preferred_element_type=jnp.float32
            )
            mixed = mixed / total
            logs = peak + jnp.log(total)
            outs = []
            for h in range(heads):
                cols = slice(h * WINDOW, (h + 1) * WINDOW)
                outs.append(mixed[:, cols])
                log_st[seq, pl.ds(h, 1), pl.ds(at, WINDOW)] = logs[:, cols]
            attn_st[seq, pl.ds(at, WINDOW), :] = (
                jnp.concatenate(outs, axis=0).T.astype(jnp.bfloat16)
            )

        @pl.loop(0, count // 2)
        def _(i):
            block(2 * i)
            block(2 * i + 1)

    half_cols = pl.ds(pl.multiple_of(f * qcols, 128), qcols)

    def attn_return(own):
        seq = f if own else other
        pairs = [
            (attn_st.at[seq], attn_out.at[:, half_cols]),
            (log_st.at[seq], log_out.at[f]),
        ]
        if own:
            return [pltpu.make_async_copy(a, b, misc_sem.at[1 + i]) for i, (a, b) in enumerate(pairs)]
        return [
            remote(a, b, ret_send.at[i], ret_recv.at[i], across) for i, (a, b) in enumerate(pairs)
        ]

    def conv_cols(g):
        return pl.ds(pl.multiple_of(f * (2 * chans) + (g - 1) * chans, 128), chans)

    split = mm_rows - pad
    head_b = jnp.where(low_half, 1, 0)
    spans = {
        None: (0, rows),
        "head": (jnp.where(low_half, rows - split, 0), split),
        "tail": (jnp.where(low_half, 0, split), rows - split),
    }

    def conv_return(g, own_seq, own_rows, span=None):
        seq = f if own_seq else other
        off = own_off if own_rows else end_off
        lo, count = spans[span]
        src = conv_st.at[g - 1, seq, pl.ds(pl.multiple_of(off + lo, pad), count)]
        dst = conv_out.at[pl.ds(pl.multiple_of(lo, pad), count), conv_cols(g)]
        if own_seq and own_rows:
            return pltpu.make_async_copy(src, dst, own_sem.at[g - 1])
        if own_seq:
            last = 3 if span == "tail" else 0
            return remote(src, dst, conv_send.at[g - 1, last], conv_recv.at[g - 1, last], pair)
        if own_rows:
            return remote(src, dst, conv_send.at[g - 1, 1], conv_recv.at[g - 1, 1], across)
        last = 1 if span == "tail" else 0
        return remote(
            src, dst, conv_send.at[g - 1, 2 + 2 * last], conv_recv.at[g - 1, 1 + last], diag
        )

    def project_conv(g, seq, own_rows, only=None):
        slot, off = (seq, own_off) if own_rows else (2 + seq, end_off)

        @halves_of(only)
        def _(b):
            at = pl.multiple_of(b * mm_rows, WINDOW)
            to = pl.multiple_of(off + b * mm_rows, WINDOW)
            out = total(g, slot, at)
            inner = out[:, :chans].astype(jnp.bfloat16).astype(jnp.float32)
            signal = out[:, chans : 2 * chans].astype(jnp.bfloat16).astype(jnp.float32)
            prod[g - 1, seq, pl.ds(to + pad, mm_rows), :] = (inner * signal).astype(jnp.bfloat16)
            outer[g - 1, seq, pl.ds(to, mm_rows), :] = out[:, 2 * chans :].astype(jnp.bfloat16)

    def project_tail(g, j):
        at = pl.multiple_of(jnp.where(low_half, SUBS - 1 - j, j) * sub, 16)
        out = jnp.dot(
            toks[2 + other, pl.ds(at, sub), :], wts[g], preferred_element_type=jnp.float32
        )
        inner = out[:, :chans].astype(jnp.bfloat16).astype(jnp.float32)
        signal = out[:, chans : 2 * chans].astype(jnp.bfloat16).astype(jnp.float32)
        to = pl.multiple_of(end_off + at, 16)
        prod[g - 1, other, pl.ds(to + pad, sub), :] = (inner * signal).astype(jnp.bfloat16)
        outer[g - 1, other, pl.ds(to, sub), :] = out[:, 2 * chans :].astype(jnp.bfloat16)

    def pr_copies(g, seq, slot):
        ref = prod.at[g - 1, seq]
        climb = remote(
            ref.at[pl.ds(both_rows, pad)],
            ref.at[pl.ds(0, pad)],
            pr_send.at[g - 1, slot],
            pr_recv.at[g - 1, slot],
            mid,
        )
        fall = remote(
            ref.at[pl.ds(pad, pad)],
            ref.at[pl.ds(both_rows + pad, pad)],
            pr_send.at[g - 1, slot],
            pr_recv.at[g - 1, slot],
            mid,
        )
        return climb, fall

    def pr_blank():
        place = pl.multiple_of(jnp.where(low_half, 0, both_rows + pad), pad)
        blank = jnp.zeros((pad, chans), jnp.bfloat16)
        for g in range(2):
            for seq in range(2):
                prod[g, seq, pl.ds(place, pad), :] = blank

    def pr_start(g, seq, slot):
        climb, fall = pr_copies(g, seq, slot)

        @pl.when(low_half)
        def _():
            climb.start()

        @pl.when(jnp.logical_not(low_half))
        def _():
            fall.start()

    def pr_wait(g, seq, slot):
        climb, fall = pr_copies(g, seq, slot)

        @pl.when(low_half)
        def _():
            climb.wait_send()
            fall.wait_recv()

        @pl.when(jnp.logical_not(low_half))
        def _():
            fall.wait_send()
            climb.wait_recv()

    def mix(g, seq, own_rows, span=None):
        lo, count = spans[span]
        off = pl.multiple_of((own_off if own_rows else end_off) + lo, pad)
        tap = taps[:, conv_cols(g)]
        size = count + 2 * pad
        full = prod[g - 1, seq, pl.ds(off, size), :].astype(jnp.float32)
        before = pltpu.roll(full, 1, 0)[pad : pad + count]
        after = pltpu.roll(full, size - 1, 0)[pad : pad + count]
        mixed = tap[0:1] * before + tap[1:2] * full[pad : pad + count] + tap[2:3] * after
        gate = outer[g - 1, seq, pl.ds(off, count), :].astype(jnp.float32)
        conv_st[g - 1, seq, pl.ds(off, count), :] = (gate * mixed).astype(jnp.bfloat16)

    finish(small[:2])
    keys0, vals0 = kv_raw[0], kv_raw[1]
    halves = [
        jnp.concatenate([w[:, i * HEAD : (i + 1) * HEAD] for w in (keys0, vals0)], axis=1)
        for i in range(2)
    ]
    first = f == 0
    stage_w[0, :, pl.ds(qcols, 2 * HEAD)] = jnp.where(first, halves[1], halves[0])
    wts[0, block_rows(mine), pl.ds(qcols, 2 * HEAD)] = jnp.where(first, halves[0], halves[1])

    pl.semaphore_wait(barrier, jnp.where(is_mid, 6, 5))

    loaded(0, own_dest[0], load_sem)
    to_pair(0, mine).start()

    @pl.when(is_mid)
    def _():
        to_mid(0, mine).start()

    loaded(0, stage_w.at[0], stage_sem)
    loaded(1, stage_w.at[1], stage_sem)

    @pl.when(is_end)
    def _():
        y_copy(0).start()
        y_copy(1).start()

    loaded(1, own_dest[1], load_sem)

    @pl.when(is_mid)
    def _():
        to_mid(1, mine).start()

    finish(small[2:])
    for i in range(gain_raw.shape[0]):
        gain[:, i * 128 : (i + 1) * 128] = gain_raw[i : i + 1, :]
    tok_load.wait()
    norm_own()
    tok_y(0, 0).start()

    @pl.when(is_mid)
    def _():
        y_copy(0).start()

    for j in range(1, SUBS):
        tok_y(0, j).start()

    @pl.when(is_mid)
    def _():
        y_copy(1).start()

    loaded(2, stage_w.at[2], stage_sem)
    y_copy(2).start()
    loaded(2, own_dest[2], load_sem)

    def relay(g, blk, onward):
        arrived(g, blk)
        onward(g, blk).start()

    pt = [partner * 2 + f, partner * 2 + other]
    ct = [facing * 2 + f, facing * 2 + other]
    ft = [far * 2 + f, far * 2 + other]

    def end_program():
        tok_z(0, 0).start()
        make_bias()
        relay(0, theirs, to_pair)
        to_pair(1, mine).start()
        relay(1, theirs, to_pair)
        for j in range(1, SUBS):
            tok_z(0, j).start()
        take(0, 0)
        for blk in pt:
            arrived(0, blk)
        near(0, f)
        take(0, 1)
        hand(0, 0)
        take(0, 2)
        hand(0, 1)
        take(0, 3)
        hand(0, 2)
        have(0, 2 * (SUBS // 2))
        near(0, other, head_b)
        for blk in ct + ft:
            arrived(0, blk)
        project_qkv(f)
        kv_start(f, 0)
        to_pair(2, mine).start()
        hand(0, 3)
        have(1, 2 * (SUBS // 2))
        near(0, other, 1 - head_b)
        project_qkv(other)
        kv_start(other, 1)
        relay(2, theirs, to_pair)
        for j in range(Z_FIRST, SUBS):
            tok_z(1, j).start()
        attend(f, 1, blocks - 2)
        attend(other, 1, blocks - 2)
        kv_wait(f, 0)
        attend(f, 0, 2, blocks - 1, True)
        begin(attn_return(True))
        kv_wait(other, 1)
        attend(other, 0, 2, blocks - 1, True)
        begin(attn_return(False))
        for g in (1, 2):
            for span in (None,) if g == 1 else ("head", "tail"):
                conv_return(g, True, False, span).wait_recv()
            conv_return(g, False, False, "head").wait_recv()
            conv_return(g, False, False, "tail").wait_recv()
        blocks_sent(pair_send.at[0], 2 * GROUPS)
        pieces_sent(tok_z_send.at[0], 2 * SUBS - Z_FIRST)

    def conv_own(g, own_seq):
        seq, slot = (f, 0) if own_seq else (other, 1)
        project_conv(g, seq, True)
        pr_start(g, seq, slot)

    def conv_close(g, own_seq):
        seq, slot = (f, 0) if own_seq else (other, 1)
        pr_wait(g, seq, slot)
        mix(g, seq, True)
        conv_return(g, own_seq, True).start()

    def conv_close_end(g):
        mix(g, f, False)
        conv_return(g, True, False).start()

    def conv_end_close(g, span):
        mix(g, other, False, span)
        conv_return(g, False, False, span).start()

    def mid_program():
        half = (blocks - 2) // 2
        make_bias()
        pr_blank()
        relay(0, ct[0], to_pair)
        relay(0, pt[0], to_mid)
        take(0, 0)
        take(1, 0)
        relay(0, theirs, to_mid)
        to_pair(0, theirs).start()
        relay(0, pt[1], to_mid)
        near(0, f)
        take(0, 1)
        hand(0, 0)
        relay(0, ct[1], to_pair)
        relay(1, pt[0], to_mid)
        take(0, 2)
        relay(0, ft[0], to_pair)
        hand(0, 1)
        have(0, 2 * (SUBS // 2))
        near(0, other, head_b)
        hand(1, 0)
        relay(0, ft[1], to_pair)
        take(0, 3)
        relay(1, pt[1], to_mid)
        project_qkv(f)
        kv_start(f, 0)
        attend(f, 1, half)
        attend(f, 1 + half, half)
        take(1, 1)
        hand(0, 2)
        relay(1, theirs, to_mid)
        to_mid(2, mine).start()
        near(1, f)
        hand(0, 3)
        have(1, 2 * (SUBS // 2))
        near(0, other, 1 - head_b)
        project_qkv(other)
        kv_start(other, 1)
        take(1, 2)
        tok_y(2, 0).start()
        attend(other, 1, half)
        attend(other, 1 + half, half)
        near(1, other)
        relay(2, theirs, to_mid)
        take(1, 3)
        for blk in ct + ft:
            arrived(1, blk)
        conv_own(1, True)
        conv_own(1, False)
        kv_wait(f, 0)
        attend(f, 0, 2, blocks - 1)
        begin(attn_return(True))
        hand(1, 1)
        have(2, 2 * (SUBS // 2))
        near(1, 2 + f, head_b)
        relay(2, pt[0], to_mid)
        take(2, 0)
        take(2, 1)
        project_conv(1, f, False, head_b)
        kv_wait(other, 1)
        attend(other, 0, 2, blocks - 1)
        begin(attn_return(False))
        hand(1, 2)
        hand(1, 3)
        have(3, 2 * (SUBS // 2))
        near(1, 2 + f, 1 - head_b)
        relay(2, pt[1], to_mid)
        take(2, 2)
        project_conv(1, f, False, 1 - head_b)
        conv_close_end(1)
        near(2, f)
        near(2, other)
        near(2, 2 + f)
        conv_close(1, True)
        hand(2, 0)
        hand(2, 1)
        take(2, 3)
        have(4, 4)
        near(1, 2 + other, head_b)
        project_conv(1, other, False, head_b)
        conv_end_close(1, "head")
        conv_close(1, False)
        near(2, 2 + other, head_b)
        for blk in ct + ft:
            arrived(2, blk)
        project_conv(2, f, True, 1 - head_b)
        project_conv(2, f, False, head_b)
        mix(2, f, False, "head")
        conv_return(2, True, False, "head").start()
        project_conv(2, f, False, 1 - head_b)
        mix(2, f, False, "tail")
        conv_return(2, True, False, "tail").start()
        project_conv(2, f, True, head_b)
        pr_start(2, f, 0)
        hand(2, 2)
        conv_own(2, False)
        project_conv(2, other, False, head_b)
        conv_end_close(2, "head")
        have(5, 2)
        project_tail(1, 2)
        hand(2, 3)
        project_tail(2, 2)
        have(6, 2)
        project_tail(1, 3)
        conv_end_close(1, "tail")
        project_tail(2, 3)
        conv_end_close(2, "tail")
        conv_close(2, False)
        conv_close(2, True)
        for g in (1, 2):
            conv_return(g, False, True).wait_recv()
            conv_return(g, True, True).wait()
            conv_return(g, False, True).wait_send()
            for span in (None,) if g == 1 else ("head", "tail"):
                conv_return(g, True, False, span).wait_send()
            conv_return(g, False, False, "head").wait_send()
            conv_return(g, False, False, "tail").wait_send()
            pieces_sent(tok_t_send.at[g], 3 * SUBS if g == 1 else 3 * SUBS - Y_PAIRS)
        blocks_sent(pair_send.at[0], 6)
        for g in range(GROUPS):
            blocks_sent(mid_send.at[g], 4)
        pieces_sent(tok_y_send.at[1], Z_FIRST + Y_PAIRS)

    pl.when(is_end)(end_program)
    pl.when(is_mid)(mid_program)

    for g in range(GROUPS):
        y_copy(g).wait_send()
    pieces_sent(tok_y_send.at[0], SUBS)
    pieces_sent(tok_t_send.at[0], 3 * SUBS)
    for own in (True, False):
        finish(attn_return(own))


def deliver(attended, conv, logs, attn_out, conv_out, log_out, log_buf, sems):
    half = logs.shape[1]
    copies = [
        pltpu.make_async_copy(a, b, sems.at[i])
        for i, (a, b) in enumerate(((attended, attn_out), (conv, conv_out), (log_buf, log_out)))
    ]
    copies[0].start()
    copies[1].start()
    for i in range(2):
        log_buf[pl.ds(i * half, half), :] = logs[i]
    copies[2].start()
    for c in copies:
        c.wait()


def fused_device(
    tps,
    tokens,
    norm_gain,
    query_weight,
    key_weight,
    value_weight,
    outer_weight,
    inner_weight,
    signal_weight,
    conv_taps,
    sink_logit,
):
    rows, width = tokens.shape[1:]
    depth, local = query_weight.shape
    qcols = local // 2
    heads = qcols // HEAD
    chans = outer_weight.shape[1] // 4
    head_local = 2 * heads
    group_cols = qcols + 2 * HEAD
    pad = 16
    bf, f32 = jnp.bfloat16, jnp.float32
    dma = pltpu.SemaphoreType.DMA
    hbm = pl.BlockSpec(memory_space=pltpu.HBM)
    anyspace = pl.BlockSpec(memory_space=pl.ANY)
    attended, conv, logs = pl.pallas_call(
        functools.partial(mega_kernel, tps),
        out_shape=(
            jax.ShapeDtypeStruct((rows, local), bf),
            jax.ShapeDtypeStruct((rows, 4 * chans), bf),
            jax.ShapeDtypeStruct((2, heads, rows), f32),
        ),
        in_specs=[hbm] * 10,
        out_specs=(anyspace, anyspace, anyspace),
        scratch_shapes=[
            pltpu.VMEM((4, rows, width), bf),
            pltpu.VMEM((GROUPS, width, group_cols), bf),
            pltpu.VMEM((GROUPS, depth, group_cols), bf),
            pltpu.VMEM((2, rows, qcols), bf),
            pltpu.VMEM((2, rows + 2 * WINDOW, 2 * HEAD), bf),
            pltpu.VMEM((3 * WINDOW, heads * WINDOW), f32),
            pltpu.VMEM((1, heads * WINDOW), f32),
            pltpu.VMEM((2, 2, 2 * rows + 2 * pad, chans), bf),
            pltpu.VMEM((2, 2, 2 * rows, chans), bf),
            pltpu.VMEM((2, rows, qcols), bf),
            pltpu.VMEM((2, heads, rows), f32),
            pltpu.VMEM((2, 2, 2 * rows, chans), bf),
            pltpu.VMEM((10, rows, group_cols), f32),
            pltpu.VMEM((2, depth, 2 * HEAD), bf),
            pltpu.VMEM((width // 128, 128), f32),
            pltpu.VMEM((1, width), f32),
            pltpu.VMEM((3, 4 * chans), f32),
            pltpu.SMEM((head_local,), f32),
            dma((5,)),
            dma((GROUPS,)),
            dma((GROUPS,)),
            dma((3,)),
            dma((2,)),
            dma((GROUPS,)),
            dma((GROUPS, 2 * SPAN)),
            dma((1,)),
            dma((GROUPS,)),
            dma((2,)),
            dma((1,)),
            dma((3,)),
            dma((3, SUBS, 2)),
            dma((7,)),
            dma((2, 2)),
            dma((2, 2)),
            dma((2, 2)),
            dma((2, 2)),
            dma((2,)),
            dma((2,)),
            dma((2, 5)),
            dma((2, 4)),
        ],
        compiler_params=pltpu.CompilerParams(
            collective_id=0, has_side_effects=True, vmem_limit_bytes=48 << 20
        ),
    )(
        *(
            pltpu.with_memory_space_constraint(x, pltpu.HBM)
            for x in (
                tokens[0],
                norm_gain.reshape(width // 128, 128),
                query_weight,
                key_weight,
                value_weight,
                outer_weight,
                inner_weight,
                signal_weight,
                conv_taps,
                sink_logit,
            )
        )
    )
    vmem = pl.BlockSpec(memory_space=pltpu.VMEM)
    attended, conv, logs = pl.pallas_call(
        deliver,
        out_shape=(
            jax.ShapeDtypeStruct((rows, local), bf),
            jax.ShapeDtypeStruct((rows, 4 * chans), bf),
            jax.ShapeDtypeStruct((head_local, rows), f32),
        ),
        in_specs=[vmem] * 3,
        out_specs=(hbm, hbm, hbm),
        scratch_shapes=[pltpu.VMEM((head_local, rows), f32), dma((3,))],
        compiler_params=pltpu.CompilerParams(vmem_limit_bytes=8 << 20),
    )(attended, conv, logs)
    return (attended[None], conv[None], logs[None])


def fits(mesh, args):
    tokens, query_weight, key_weight, outer_weight = (args[i] for i in (0, 2, 3, 5))
    sp, fs, tp = (mesh.shape[a] for a in ("sp", "fs", "tp"))
    rows = tokens.shape[1] // sp
    return (
        fs == 2
        and sp == SPAN
        and tokens.shape[0] == fs
        and tp == 4
        and rows % (2 * WINDOW) == 0
        and rows // WINDOW % 2 == 0
        and rows % (16 * SUBS * tp) == 0
        and key_weight.shape[1] == 2 * HEAD * tp
        and query_weight.shape[1] % (256 * tp) == 0
        and outer_weight.shape[1] == 512 * tp
        and query_weight.shape[1] == 512 * tp
        and query_weight.shape[0] % (16 * sp * fs) == 0
    )


def solution(mesh):
    in_specs = (
        P("fs", "sp", None),
        P(),
        P(("sp", "fs"), "tp"),
        P(("sp", "fs"), "tp"),
        P(("sp", "fs"), "tp"),
        P(("sp", "fs"), "tp"),
        P(("sp", "fs"), "tp"),
        P(("sp", "fs"), "tp"),
        P(None, "tp"),
        P("tp"),
    )
    out_specs = (P("fs", "sp", "tp"), P("fs", "sp", "tp"), P("fs", "tp", "sp"))

    def run(*args):
        body = per_device
        if fits(mesh, args):
            body = functools.partial(fused_device, mesh.shape["tp"])
        return jax.shard_map(
            body, mesh=mesh, in_specs=in_specs, out_specs=out_specs, check_vma=False
        )(*args)

    return run
```

```python
import math

import functools

import jax
import jax.numpy as jnp
from jax import lax
from jax.experimental import pallas as pl
from jax.experimental.pallas import tpu as pltpu
from jax.sharding import PartitionSpec as P

HEAD = 64
WINDOW = 128


EPSILON = 1e-06


def extended(value, sides, width):
    for axis, dim in sides:
        size, length = (lax.axis_size(axis), value.shape[dim])
        up = [(i, (i + 1) % size) for i in range(size - 1)]
        down = [(j, i) for i, j in up]
        last = lax.slice_in_dim(value, length - width, length, axis=dim)
        initial = lax.slice_in_dim(value, 0, width, axis=dim)
        before = lax.ppermute(last, axis, up)
        after = lax.ppermute(initial, axis, down)
        value = jnp.concatenate([before, value, after], axis=dim)
    return value


def normalized(tokens, norm_gain):
    values = tokens.astype(jnp.float32)
    scaling = lax.rsqrt(jnp.mean(values * values, axis=-1, keepdims=True) + EPSILON)
    return (values * scaling * norm_gain).astype(jnp.bfloat16)


def folding(normed):

    def add_portions(running, portions, offset):
        return tuple(
            (jnp.dot(normed, portion, preferred_element_type=jnp.float32) for portion in portions)
        )

    return add_portions


def empty_sums(normed, weights):
    return tuple((jnp.zeros((normed.shape[0], weight.shape[1]), jnp.float32) for weight in weights))


def rounded(results):
    return tuple((result.astype(jnp.bfloat16) for result in results))


def gate_product(inner_gate, signal):
    return (inner_gate.astype(jnp.float32) * signal.astype(jnp.float32)).astype(jnp.bfloat16)


def send_edges(key_proj, value_proj, product):
    stacked = jnp.concatenate([key_proj, value_proj], axis=1)
    window_rows = extended(stacked, (("sp", 0),), WINDOW)
    conv_rows = extended(product, (("sp", 0),), 1)
    return (window_rows, conv_rows)


def banded_attention(queries, window_rows, sink_logit, slopes, first_pos, seq_length):
    tok_count = queries.shape[0]
    kv_cols = window_rows.shape[1] // 2
    kv_heads = kv_cols // HEAD
    group_size = queries.shape[1] // (HEAD * kv_heads)
    block_count = tok_count // WINDOW
    query_blocks = queries.reshape(block_count, WINDOW, kv_heads, group_size, HEAD)
    key_rows = window_rows[:, :kv_cols].reshape(block_count + 2, WINDOW, kv_heads, HEAD)
    value_rows = window_rows[:, kv_cols:].reshape(block_count + 2, WINDOW, kv_heads, HEAD)
    key_span = jnp.concatenate([key_rows[:-2], key_rows[1:-1], key_rows[2:]], axis=1)
    value_span = jnp.concatenate([value_rows[:-2], value_rows[1:-1], value_rows[2:]], axis=1)
    scores = jnp.einsum(
        "bqkgd,bskd->bkgqs", query_blocks, key_span, preferred_element_type=jnp.float32
    ) * (1.0 / math.sqrt(HEAD))
    distance = jnp.arange(WINDOW)[:, None] - jnp.arange(3 * WINDOW)[None, :] + WINDOW
    key_pos = (
        first_pos
        - WINDOW
        + WINDOW * jnp.arange(block_count)[:, None]
        + jnp.arange(3 * WINDOW)[None, :]
    )
    inside = (jnp.abs(distance)[None] <= WINDOW) & ((key_pos >= 0) & (key_pos < seq_length))[
        :, None, :
    ]
    scores = scores - slopes.reshape(kv_heads, group_size, 1, 1) * jnp.abs(distance).astype(
        jnp.float32
    )
    scores = jnp.where(inside[:, None, None], scores, -jnp.inf)
    sink_grid = sink_logit.reshape(kv_heads, group_size, 1, 1)
    row_peak = jnp.maximum(jnp.max(scores, axis=-1, keepdims=True), sink_grid)
    weights = jnp.exp(scores - row_peak)
    row_total = jnp.sum(weights, axis=-1, keepdims=True) + jnp.exp(sink_grid - row_peak)
    weighted = jnp.einsum(
        "bkgqs,bskd->bqkgd",
        weights.astype(jnp.bfloat16),
        value_span,
        preferred_element_type=jnp.float32,
    )
    attended = (
        (weighted / row_total.transpose(0, 3, 1, 2, 4))
        .astype(jnp.bfloat16)
        .reshape(tok_count, kv_heads * group_size * HEAD)
    )
    log_total = (
        (row_peak + jnp.log(row_total))[..., 0]
        .transpose(1, 2, 0, 3)
        .reshape(kv_heads * group_size, tok_count)
    )
    return (attended, log_total)


def per_device(
    tokens,
    norm_gain,
    query_weight,
    key_weight,
    value_weight,
    outer_weight,
    inner_weight,
    signal_weight,
    conv_taps,
    sink_logit,
):
    normed = normalized(tokens[0], norm_gain)
    add_portions = folding(normed)
    all_sums = add_portions(
        empty_sums(
            normed,
            (query_weight, key_weight, value_weight, outer_weight, inner_weight, signal_weight),
        ),
        (
            lax.all_gather(query_weight, ("sp", "fs"), axis=0, tiled=True),
            lax.all_gather(key_weight, ("sp", "fs"), axis=0, tiled=True),
            lax.all_gather(value_weight, ("sp", "fs"), axis=0, tiled=True),
            lax.all_gather(outer_weight, ("sp", "fs"), axis=0, tiled=True),
            lax.all_gather(inner_weight, ("sp", "fs"), axis=0, tiled=True),
            lax.all_gather(signal_weight, ("sp", "fs"), axis=0, tiled=True),
        ),
        jnp.int32(0),
    )
    queries, key_proj, value_proj, outer_gate, inner_gate, signal = rounded(all_sums)
    product = gate_product(inner_gate, signal)
    window_rows, conv_rows = send_edges(key_proj, value_proj, product)
    tok_count = normed.shape[0]
    head_local = queries.shape[1] // HEAD
    head_index = lax.axis_index("tp") * head_local + jnp.arange(1, head_local + 1)
    slopes = jnp.exp2(-8.0 * head_index.astype(jnp.float32) / (head_local * lax.axis_size("tp")))
    first_pos = lax.axis_index("sp") * tok_count
    attended, log_total = banded_attention(
        queries, window_rows, sink_logit, slopes, first_pos, tok_count * lax.axis_size("sp")
    )
    mixed_conv = conv_taps[0] * conv_rows[0:tok_count].astype(jnp.float32)
    mixed_conv = mixed_conv + conv_taps[1] * conv_rows[1 : tok_count + 1].astype(jnp.float32)
    mixed_conv = mixed_conv + conv_taps[2] * conv_rows[2 : tok_count + 2].astype(jnp.float32)
    conv_out = (outer_gate.astype(jnp.float32) * mixed_conv).astype(jnp.bfloat16)
    return (attended[None], conv_out[None], log_total[None])


MESH = pl.DeviceIdType.MESH
GROUPS = 3
SPAN = 4
SUBS = 4
Y_PAIRS = 1
Z_FIRST = 3
FAR = -1e30


def mega_kernel(
    tps,
    tokens,
    gain_in,
    qw,
    kw,
    vw,
    ow,
    iw,
    sw,
    taps_in,
    sinks_in,
    attn_out,
    conv_out,
    log_out,
    toks,
    wts,
    stage_w,
    qs,
    kvs,
    bias,
    sink_row,
    prod,
    outer,
    attn_st,
    log_st,
    conv_st,
    acc,
    kv_raw,
    gain_raw,
    gain,
    taps,
    sinks,
    small_sem,
    load_sem,
    stage_sem,
    misc_sem,
    own_sem,
    y_send,
    w_recv,
    pair_send,
    mid_send,
    tok_y_send,
    tok_z_send,
    tok_t_send,
    tok_recv,
    tok_have,
    kv_send,
    kv_recv,
    pr_send,
    pr_recv,
    ret_send,
    ret_recv,
    conv_send,
    conv_recv,
):
    s, f, t = lax.axis_index("sp"), lax.axis_index("fs"), lax.axis_index("tp")
    other = 1 - f
    core = lax.rem(t, 2)
    outward = 1 - lax.rem(s, 2)
    partner = s + 2 * outward - 1
    facing = SPAN - 1 - s
    far = SPAN - 1 - partner
    is_mid = (s == 1) | (s == SPAN - 2)
    is_end = jnp.logical_not(is_mid)
    low_half = s < SPAN // 2
    pair, diag, mid = (partner, f, t), (partner, other, t), (facing, f, t)
    across = (s, other, t)
    mate_t, beyond_t = t + 1 - 2 * core, lax.rem(t + 2, tps)
    mate, beyond = (s, f, mate_t), (s, f, beyond_t)
    rows = tokens.shape[0]
    depth = qw.shape[0]
    qcols = qs.shape[2]
    heads = qcols // HEAD
    chans = prod.shape[3]
    both_rows = outer.shape[2]
    blocks = rows // WINDOW
    pad = (prod.shape[2] - both_rows) // 2
    sub = rows // SUBS
    part = sub // tps
    up, down = (s + 1, f, t), (s - 1, f, t)
    has_up, has_down = s < SPAN - 1, s > 0
    own_off = jnp.where(low_half, rows, 0)
    end_off = rows - own_off

    barrier = pltpu.get_barrier_semaphore()
    for peer in (pair, diag, across, mate, beyond):
        pl.semaphore_signal(barrier, inc=1, device_id=peer, device_id_type=MESH)

    @pl.when(is_mid)
    def _():
        pl.semaphore_signal(barrier, inc=1, device_id=mid, device_id_type=MESH)

    def block_rows(blk):
        return pl.ds(pl.multiple_of(blk * depth, 16), depth)

    def loads(g, half, dest, sems):
        if g == 0:
            qc = pl.ds(pl.multiple_of(half * qcols, 128), qcols)
            pairs = [(qw.at[:, qc], dest.at[:, pl.ds(0, qcols)])]
        else:
            c = pl.ds(pl.multiple_of(half * (2 * chans) + (g - 1) * chans, 128), chans)
            pairs = [
                (ref.at[:, c], dest.at[:, pl.ds(i * chans, chans)])
                for i, ref in enumerate((iw, sw, ow))
            ]
        return [pltpu.make_async_copy(a, b, sems.at[g]) for a, b in pairs]

    def loaded(g, dest, sems):
        whole = dest.at[:, pl.ds(0, qcols)] if g == 0 else dest
        pltpu.make_async_copy(whole, whole, sems.at[g]).wait()

    mine = s * 2 + f
    theirs = s * 2 + other
    own_dest = [wts.at[g, block_rows(mine)] for g in range(GROUPS)]
    own_loads = [loads(g, f, own_dest[g], load_sem) for g in range(GROUPS)]
    out_loads = [loads(g, other, stage_w.at[g], stage_sem) for g in range(GROUPS)]
    small = [
        pltpu.make_async_copy(a, b, small_sem.at[i])
        for i, (a, b) in enumerate(
            (
                (kw, kv_raw.at[0]),
                (vw, kv_raw.at[1]),
                (gain_in, gain_raw),
                (taps_in, taps),
                (sinks_in, sinks),
            )
        )
    ]
    tok_load = pltpu.make_async_copy(tokens, toks.at[f], misc_sem.at[0])

    def begin(copies):
        for c in copies:
            c.start()

    def finish(copies):
        for c in copies:
            c.wait()

    begin(small[:2] + out_loads[0] + own_loads[0] + small[2:])
    tok_load.start()
    begin(out_loads[1] + own_loads[1] + out_loads[2] + own_loads[2])

    def remote(src, dst, send, recv, peer):
        return pltpu.make_async_remote_copy(
            src_ref=src,
            dst_ref=dst,
            send_sem=send,
            recv_sem=recv,
            device_id=peer,
            device_id_type=MESH,
        )

    def y_copy(g):
        return remote(
            stage_w.at[g], wts.at[g, block_rows(mine)], y_send.at[g], w_recv.at[g, mine], across
        )

    def block_copy(g, blk, send, peer):
        at = wts.at[g, block_rows(blk)]
        return remote(at, at, send, w_recv.at[g, blk], peer)

    def to_pair(g, blk):
        return block_copy(g, blk, pair_send.at[0], pair)

    def to_mid(g, blk):
        return block_copy(g, blk, mid_send.at[g], mid)

    def blocks_sent(send, count):
        at = wts.at[0, pl.ds(0, count * depth)]
        remote(at, at, send, w_recv.at[0, 0], across).wait_send()

    def arrived(g, blk):
        to_pair(g, blk).wait_recv()

    def slot_of(k):
        return (other, 2 + f, 2 + other)[k]

    def piece(slot, j, q):
        place = jnp.where(low_half, SUBS - 1 - j, j)
        return toks.at[slot, pl.ds(pl.multiple_of(place * sub + q * part, 16), part)]

    def tok_y(k, j):
        slot = f if k == 0 else 2 + f
        at = piece(slot, j, beyond_t if k == 2 else t)
        return remote(
            at, at, tok_y_send.at[1 if k else 0], tok_recv.at[2 if k else 0, j, k // 2], across
        )

    def tok_z(k, j):
        seq = f if k == 0 else other
        return remote(
            piece(seq, j, t), piece(2 + seq, j, t), tok_z_send.at[0], tok_recv.at[1 + k, j, 0], pair
        )

    def have_slot(k, j):
        if k < 2:
            return 2 * k + j // (SUBS // 2)
        return 4 + max(0, j - 1)

    def tok_share(k, j, kind):
        at = piece(slot_of(k), j, beyond_t if kind == 2 else t)
        if kind == 1:
            return remote(at, at, tok_t_send.at[k], tok_recv.at[k, j, 1], beyond)
        return remote(at, at, tok_t_send.at[k], tok_have.at[have_slot(k, j)], mate)

    def tok_wait(k, j, kind):
        at = piece(slot_of(k), j, t)
        remote(at, at, tok_t_send.at[k], tok_recv.at[k, j, kind], mate).wait_recv()

    def take(k, j):
        tok_wait(k, j, 0)
        if k < 2 or j >= Y_PAIRS:
            tok_share(k, j, 1).start()
        tok_share(k, j, 0).start()
        if k == 1 and j < Z_FIRST:
            tok_y(1, j).start()

    def hand(k, j):
        tok_wait(k, j, 1)
        tok_share(k, j, 2).start()

    def have(index, pieces):
        at = toks.at[0, pl.ds(0, pieces * part)]
        remote(at, at, tok_t_send.at[0], tok_have.at[index], mate).wait_recv()

    def pieces_sent(send, pieces):
        at = toks.at[0, pl.ds(0, pieces * part)]
        remote(at, at, send, tok_have.at[0], mate).wait_send()

    def norm_own():
        @pl.loop(0, blocks)
        def _(b):
            at = pl.ds(pl.multiple_of(b * WINDOW, WINDOW), WINDOW)
            values = toks[f, at, :].astype(jnp.float32)
            scaling = lax.rsqrt(jnp.mean(values * values, axis=-1, keepdims=True) + EPSILON)
            toks[f, at, :] = (values * scaling * gain[...]).astype(jnp.bfloat16)

    mm_rows = rows // 2

    def make_bias():
        key = lax.broadcasted_iota(jnp.int32, (3 * WINDOW, WINDOW), 0)
        query = lax.broadcasted_iota(jnp.int32, (3 * WINDOW, WINDOW), 1)
        away = jnp.abs(query - key + WINDOW)
        for h in range(heads):
            index = (t * (2 * heads) + f * heads + h + 1).astype(jnp.float32)
            slope = jnp.exp2(jnp.full((1, WINDOW), -8.0 / (2 * heads * tps), jnp.float32) * index)
            cols = pl.ds(h * WINDOW, WINDOW)
            bias[:, cols] = jnp.where(away <= WINDOW, -slope * away.astype(jnp.float32), FAR)
            sink_row[:, cols] = jnp.full((1, WINDOW), sinks[f * heads + h], jnp.float32)

    scale = 1.0 / math.sqrt(HEAD)
    half_k = depth * SPAN
    near_k = pl.multiple_of(jnp.where(low_half, 0, half_k), 128)
    far_k = pl.multiple_of(half_k - near_k, 128)

    def partial(g, slot, at, k_off):
        return jnp.dot(
            toks[slot, pl.ds(at, mm_rows), pl.ds(k_off, half_k)],
            wts[g, pl.ds(k_off, half_k), :],
            preferred_element_type=jnp.float32,
        )

    def sums(g, slot):
        return slot if g == 0 else slot + 4 * g - 2

    def halves_of(b):
        if b is None:
            return lambda body: [body(i) for i in range(2)]
        return lambda body: body(b)

    def near(g, slot, only=None):
        @halves_of(only)
        def _(b):
            at = pl.multiple_of(b * mm_rows, WINDOW)
            acc[sums(g, slot), pl.ds(at, mm_rows), :] = partial(g, slot, at, near_k)

    def total(g, slot, at):
        return acc[sums(g, slot), pl.ds(at, mm_rows), :] + partial(g, slot, at, far_k)

    def project_qkv(seq):
        @pl.loop(0, 2)
        def _(b):
            at = pl.multiple_of(b * mm_rows, WINDOW)
            out = total(0, seq, at)
            qs[seq, pl.ds(at, mm_rows), :] = (out[:, :qcols] * scale).astype(jnp.bfloat16)
            kvs[seq, pl.ds(at + WINDOW, mm_rows), :] = out[:, qcols:].astype(jnp.bfloat16)

    kv_len = kvs.shape[1]

    def kv_copies(seq, slot):
        ref = kvs.at[seq]
        climb = remote(
            ref.at[pl.ds(kv_len - 2 * WINDOW, WINDOW)],
            ref.at[pl.ds(0, WINDOW)],
            kv_send.at[slot, 0],
            kv_recv.at[slot, 0],
            up,
        )
        fall = remote(
            ref.at[pl.ds(WINDOW, WINDOW)],
            ref.at[pl.ds(kv_len - WINDOW, WINDOW)],
            kv_send.at[slot, 1],
            kv_recv.at[slot, 1],
            down,
        )
        return climb, fall

    def kv_start(seq, slot):
        climb, fall = kv_copies(seq, slot)
        blank = jnp.zeros((WINDOW, 2 * HEAD), jnp.bfloat16)

        @pl.when(has_up)
        def _():
            climb.start()

        @pl.when(has_down)
        def _():
            fall.start()

        @pl.when(jnp.logical_not(has_up))
        def _():
            kvs[seq, pl.ds(kv_len - WINDOW, WINDOW), :] = blank

        @pl.when(jnp.logical_not(has_down))
        def _():
            kvs[seq, pl.ds(0, WINDOW), :] = blank

    def kv_wait(seq, slot):
        climb, fall = kv_copies(seq, slot)

        @pl.when(has_up)
        def _():
            climb.wait_send()
            fall.wait_recv()

        @pl.when(has_down)
        def _():
            fall.wait_send()
            climb.wait_recv()

    def attend(seq, first, count, step=1, closed=False):
        def block(i):
            b = first + i * step
            at = pl.multiple_of(b * WINDOW, WINDOW)
            kv = kvs[seq, pl.ds(at, 3 * WINDOW), :]
            keys = kv[:, :HEAD]
            values_t = kv.astype(jnp.float32).T[HEAD:, :].astype(jnp.bfloat16)
            queries = qs[seq, pl.ds(at, WINDOW), :]
            stacked = jnp.concatenate(
                [queries[:, h * HEAD : (h + 1) * HEAD] for h in range(heads)], axis=0
            )
            scores = lax.dot_general(
                keys, stacked, (((1,), (1,)), ((), ())), preferred_element_type=jnp.float32
            )
            scores = scores + bias[...]
            if closed:
                low = jnp.where((b == 0) & (s == 0), FAR, 0.0)
                high = jnp.where((b == blocks - 1) & (s == SPAN - 1), FAR, 0.0)
                scores = jnp.concatenate(
                    [
                        scores[:WINDOW] + low,
                        scores[WINDOW : 2 * WINDOW],
                        scores[2 * WINDOW :] + high,
                    ],
                    axis=0,
                )
            sink = sink_row[...]
            peak = jnp.maximum(jnp.max(scores, axis=0, keepdims=True), sink)
            weights = jnp.exp(scores - peak)
            total = jnp.sum(weights, axis=0, keepdims=True) + jnp.exp(sink - peak)
            mixed = jnp.dot(
                values_t, weights.astype(jnp.bfloat16), preferred_element_type=jnp.float32
            )
            mixed = mixed / total
            logs = peak + jnp.log(total)
            outs = []
            for h in range(heads):
                cols = slice(h * WINDOW, (h + 1) * WINDOW)
                outs.append(mixed[:, cols])
                log_st[seq, pl.ds(h, 1), pl.ds(at, WINDOW)] = logs[:, cols]
            attn_st[seq, pl.ds(at, WINDOW), :] = (
                jnp.concatenate(outs, axis=0).T.astype(jnp.bfloat16)
            )

        @pl.loop(0, count // 2)
        def _(i):
            block(2 * i)
            block(2 * i + 1)

    half_cols = pl.ds(pl.multiple_of(f * qcols, 128), qcols)

    def attn_return(own):
        seq = f if own else other
        pairs = [
            (attn_st.at[seq], attn_out.at[:, half_cols]),
            (log_st.at[seq], log_out.at[f]),
        ]
        if own:
            return [pltpu.make_async_copy(a, b, misc_sem.at[1 + i]) for i, (a, b) in enumerate(pairs)]
        return [
            remote(a, b, ret_send.at[i], ret_recv.at[i], across) for i, (a, b) in enumerate(pairs)
        ]

    def conv_cols(g):
        return pl.ds(pl.multiple_of(f * (2 * chans) + (g - 1) * chans, 128), chans)

    split = mm_rows - pad
    head_b = jnp.where(low_half, 1, 0)
    spans = {
        None: (0, rows),
        "head": (jnp.where(low_half, rows - split, 0), split),
        "tail": (jnp.where(low_half, 0, split), rows - split),
        "far": (jnp.where(low_half, 0, rows - split), split),
        "rest": (jnp.where(low_half, split, 0), rows - split),
    }

    def conv_return(g, own_seq, own_rows, span=None):
        seq = f if own_seq else other
        off = own_off if own_rows else end_off
        lo, count = spans[span]
        src = conv_st.at[g - 1, seq, pl.ds(pl.multiple_of(off + lo, pad), count)]
        dst = conv_out.at[pl.ds(pl.multiple_of(lo, pad), count), conv_cols(g)]
        if own_seq and own_rows:
            return pltpu.make_async_copy(src, dst, own_sem.at[g - 1])
        if own_seq:
            last = 3 if span == "rest" else 0
            return remote(src, dst, conv_send.at[g - 1, last], conv_recv.at[g - 1, last], pair)
        if own_rows:
            return remote(src, dst, conv_send.at[g - 1, 1], conv_recv.at[g - 1, 1], across)
        last = 1 if span == "tail" else 0
        return remote(
            src, dst, conv_send.at[g - 1, 2 + 2 * last], conv_recv.at[g - 1, 1 + last], diag
        )

    def project_conv(g, seq, own_rows, only=None):
        slot, off = (seq, own_off) if own_rows else (2 + seq, end_off)

        @halves_of(only)
        def _(b):
            at = pl.multiple_of(b * mm_rows, WINDOW)
            to = pl.multiple_of(off + b * mm_rows, WINDOW)
            out = total(g, slot, at)
            inner = out[:, :chans].astype(jnp.bfloat16).astype(jnp.float32)
            signal = out[:, chans : 2 * chans].astype(jnp.bfloat16).astype(jnp.float32)
            prod[g - 1, seq, pl.ds(to + pad, mm_rows), :] = (inner * signal).astype(jnp.bfloat16)
            outer[g - 1, seq, pl.ds(to, mm_rows), :] = out[:, 2 * chans :].astype(jnp.bfloat16)

    def project_tail(g, j):
        at = pl.multiple_of(jnp.where(low_half, SUBS - 1 - j, j) * sub, 16)
        out = jnp.dot(
            toks[2 + other, pl.ds(at, sub), :], wts[g], preferred_element_type=jnp.float32
        )
        inner = out[:, :chans].astype(jnp.bfloat16).astype(jnp.float32)
        signal = out[:, chans : 2 * chans].astype(jnp.bfloat16).astype(jnp.float32)
        to = pl.multiple_of(end_off + at, 16)
        prod[g - 1, other, pl.ds(to + pad, sub), :] = (inner * signal).astype(jnp.bfloat16)
        outer[g - 1, other, pl.ds(to, sub), :] = out[:, 2 * chans :].astype(jnp.bfloat16)

    def pr_copies(g, seq, slot):
        ref = prod.at[g - 1, seq]
        climb = remote(
            ref.at[pl.ds(both_rows, pad)],
            ref.at[pl.ds(0, pad)],
            pr_send.at[g - 1, slot],
            pr_recv.at[g - 1, slot],
            mid,
        )
        fall = remote(
            ref.at[pl.ds(pad, pad)],
            ref.at[pl.ds(both_rows + pad, pad)],
            pr_send.at[g - 1, slot],
            pr_recv.at[g - 1, slot],
            mid,
        )
        return climb, fall

    def pr_blank():
        place = pl.multiple_of(jnp.where(low_half, 0, both_rows + pad), pad)
        blank = jnp.zeros((pad, chans), jnp.bfloat16)
        for g in range(2):
            for seq in range(2):
                prod[g, seq, pl.ds(place, pad), :] = blank

    def pr_start(g, seq, slot):
        climb, fall = pr_copies(g, seq, slot)

        @pl.when(low_half)
        def _():
            climb.start()

        @pl.when(jnp.logical_not(low_half))
        def _():
            fall.start()

    def pr_wait(g, seq, slot):
        climb, fall = pr_copies(g, seq, slot)

        @pl.when(low_half)
        def _():
            climb.wait_send()
            fall.wait_recv()

        @pl.when(jnp.logical_not(low_half))
        def _():
            fall.wait_send()
            climb.wait_recv()

    def mix(g, seq, own_rows, span=None):
        lo, count = spans[span]
        off = pl.multiple_of((own_off if own_rows else end_off) + lo, pad)
        tap = taps[:, conv_cols(g)]
        size = count + 2 * pad
        full = prod[g - 1, seq, pl.ds(off, size), :].astype(jnp.float32)
        before = pltpu.roll(full, 1, 0)[pad : pad + count]
        after = pltpu.roll(full, size - 1, 0)[pad : pad + count]
        mixed = tap[0:1] * before + tap[1:2] * full[pad : pad + count] + tap[2:3] * after
        gate = outer[g - 1, seq, pl.ds(off, count), :].astype(jnp.float32)
        conv_st[g - 1, seq, pl.ds(off, count), :] = (gate * mixed).astype(jnp.bfloat16)

    finish(small[:2])
    keys0, vals0 = kv_raw[0], kv_raw[1]
    halves = [
        jnp.concatenate([w[:, i * HEAD : (i + 1) * HEAD] for w in (keys0, vals0)], axis=1)
        for i in range(2)
    ]
    first = f == 0
    stage_w[0, :, pl.ds(qcols, 2 * HEAD)] = jnp.where(first, halves[1], halves[0])
    wts[0, block_rows(mine), pl.ds(qcols, 2 * HEAD)] = jnp.where(first, halves[0], halves[1])

    pl.semaphore_wait(barrier, jnp.where(is_mid, 6, 5))

    loaded(0, own_dest[0], load_sem)
    to_pair(0, mine).start()

    @pl.when(is_mid)
    def _():
        to_mid(0, mine).start()

    loaded(0, stage_w.at[0], stage_sem)
    loaded(1, stage_w.at[1], stage_sem)

    @pl.when(is_end)
    def _():
        y_copy(0).start()
        y_copy(1).start()

    loaded(1, own_dest[1], load_sem)

    @pl.when(is_mid)
    def _():
        to_mid(1, mine).start()

    finish(small[2:])
    for i in range(gain_raw.shape[0]):
        gain[:, i * 128 : (i + 1) * 128] = gain_raw[i : i + 1, :]
    tok_load.wait()
    norm_own()
    tok_y(0, 0).start()

    @pl.when(is_mid)
    def _():
        y_copy(0).start()

    for j in range(1, SUBS):
        tok_y(0, j).start()

    @pl.when(is_mid)
    def _():
        y_copy(1).start()

    loaded(2, stage_w.at[2], stage_sem)
    y_copy(2).start()
    loaded(2, own_dest[2], load_sem)

    def relay(g, blk, onward):
        arrived(g, blk)
        onward(g, blk).start()

    pt = [partner * 2 + f, partner * 2 + other]
    ct = [facing * 2 + f, facing * 2 + other]
    ft = [far * 2 + f, far * 2 + other]

    def end_program():
        tok_z(0, 0).start()
        make_bias()
        relay(0, theirs, to_pair)
        to_pair(1, mine).start()
        relay(1, theirs, to_pair)
        for j in range(1, SUBS):
            tok_z(0, j).start()
        take(0, 0)
        for blk in pt:
            arrived(0, blk)
        near(0, f)
        take(0, 1)
        hand(0, 0)
        take(0, 2)
        hand(0, 1)
        take(0, 3)
        hand(0, 2)
        have(0, 2 * (SUBS // 2))
        near(0, other, head_b)
        for blk in ct + ft:
            arrived(0, blk)
        project_qkv(f)
        kv_start(f, 0)
        to_pair(2, mine).start()
        hand(0, 3)
        have(1, 2 * (SUBS // 2))
        near(0, other, 1 - head_b)
        project_qkv(other)
        kv_start(other, 1)
        relay(2, theirs, to_pair)
        for j in range(Z_FIRST, SUBS):
            tok_z(1, j).start()
        attend(f, 1, blocks - 2)
        attend(other, 1, blocks - 2)
        kv_wait(f, 0)
        attend(f, 0, 2, blocks - 1, True)
        begin(attn_return(True))
        kv_wait(other, 1)
        attend(other, 0, 2, blocks - 1, True)
        begin(attn_return(False))
        for g in (1, 2):
            for span in (None,) if g == 1 else ("far", "rest"):
                conv_return(g, True, False, span).wait_recv()
            conv_return(g, False, False, "head").wait_recv()
            conv_return(g, False, False, "tail").wait_recv()
        blocks_sent(pair_send.at[0], 2 * GROUPS)
        pieces_sent(tok_z_send.at[0], 2 * SUBS - Z_FIRST)

    def conv_own(g, own_seq):
        seq, slot = (f, 0) if own_seq else (other, 1)
        project_conv(g, seq, True)
        pr_start(g, seq, slot)

    def conv_close(g, own_seq):
        seq, slot = (f, 0) if own_seq else (other, 1)
        pr_wait(g, seq, slot)
        mix(g, seq, True)
        conv_return(g, own_seq, True).start()

    def conv_close_end(g):
        mix(g, f, False)
        conv_return(g, True, False).start()

    def conv_end_close(g, span):
        mix(g, other, False, span)
        conv_return(g, False, False, span).start()

    def mid_program():
        half = (blocks - 2) // 2
        make_bias()
        pr_blank()
        relay(0, ct[0], to_pair)
        relay(0, pt[0], to_mid)
        take(0, 0)
        take(1, 0)
        relay(0, theirs, to_mid)
        to_pair(0, theirs).start()
        relay(0, pt[1], to_mid)
        near(0, f)
        take(0, 1)
        hand(0, 0)
        relay(0, ct[1], to_pair)
        relay(1, pt[0], to_mid)
        take(0, 2)
        relay(0, ft[0], to_pair)
        hand(0, 1)
        have(0, 2 * (SUBS // 2))
        near(0, other, head_b)
        hand(1, 0)
        relay(0, ft[1], to_pair)
        take(0, 3)
        relay(1, pt[1], to_mid)
        project_qkv(f)
        kv_start(f, 0)
        attend(f, 1, half)
        attend(f, 1 + half, half)
        take(1, 1)
        hand(0, 2)
        relay(1, theirs, to_mid)
        to_mid(2, mine).start()
        near(1, f)
        hand(0, 3)
        have(1, 2 * (SUBS // 2))
        near(0, other, 1 - head_b)
        project_qkv(other)
        kv_start(other, 1)
        take(1, 2)
        tok_y(2, 0).start()
        attend(other, 1, half)
        attend(other, 1 + half, half)
        near(1, other)
        relay(2, theirs, to_mid)
        take(1, 3)
        for blk in ct + ft:
            arrived(1, blk)
        conv_own(1, True)
        conv_own(1, False)
        kv_wait(f, 0)
        attend(f, 0, 2, blocks - 1)
        begin(attn_return(True))
        hand(1, 1)
        have(2, 2 * (SUBS // 2))
        near(1, 2 + f, head_b)
        relay(2, pt[0], to_mid)
        take(2, 0)
        take(2, 1)
        project_conv(1, f, False, head_b)
        kv_wait(other, 1)
        attend(other, 0, 2, blocks - 1)
        begin(attn_return(False))
        hand(1, 2)
        hand(1, 3)
        have(3, 2 * (SUBS // 2))
        near(1, 2 + f, 1 - head_b)
        relay(2, pt[1], to_mid)
        take(2, 2)
        project_conv(1, f, False, 1 - head_b)
        conv_close_end(1)
        near(2, f)
        near(2, other)
        take(2, 3)
        near(2, 2 + f)
        hand(2, 0)
        conv_close(1, True)
        hand(2, 1)
        have(4, 4)
        near(1, 2 + other, head_b)
        project_conv(1, other, False, head_b)
        conv_end_close(1, "head")
        conv_close(1, False)
        near(2, 2 + other, head_b)
        for blk in ct + ft:
            arrived(2, blk)
        project_conv(2, f, False, 1 - head_b)
        mix(2, f, False, "far")
        conv_return(2, True, False, "far").start()
        project_conv(2, f, True, 1 - head_b)
        project_conv(2, f, False, head_b)
        mix(2, f, False, "rest")
        conv_return(2, True, False, "rest").start()
        hand(2, 2)
        conv_own(2, False)
        project_conv(2, other, False, head_b)
        conv_end_close(2, "head")
        hand(2, 3)
        project_conv(2, f, True, head_b)
        pr_start(2, f, 0)
        have(5, 2)
        project_tail(1, 2)
        have(6, 2)
        project_tail(1, 3)
        conv_end_close(1, "tail")
        conv_close(2, False)
        project_tail(2, 2)
        project_tail(2, 3)
        conv_end_close(2, "tail")
        conv_close(2, True)
        for g in (1, 2):
            conv_return(g, False, True).wait_recv()
            conv_return(g, True, True).wait()
            conv_return(g, False, True).wait_send()
            for span in (None,) if g == 1 else ("far", "rest"):
                conv_return(g, True, False, span).wait_send()
            conv_return(g, False, False, "head").wait_send()
            conv_return(g, False, False, "tail").wait_send()
            pieces_sent(tok_t_send.at[g], 3 * SUBS if g == 1 else 3 * SUBS - Y_PAIRS)
        blocks_sent(pair_send.at[0], 6)
        for g in range(GROUPS):
            blocks_sent(mid_send.at[g], 4)
        pieces_sent(tok_y_send.at[1], Z_FIRST + Y_PAIRS)

    pl.when(is_end)(end_program)
    pl.when(is_mid)(mid_program)

    for g in range(GROUPS):
        y_copy(g).wait_send()
    pieces_sent(tok_y_send.at[0], SUBS)
    pieces_sent(tok_t_send.at[0], 3 * SUBS)
    for own in (True, False):
        finish(attn_return(own))


def deliver(attended, conv, logs, attn_out, conv_out, log_out, log_buf, sems):
    half = logs.shape[1]
    copies = [
        pltpu.make_async_copy(a, b, sems.at[i])
        for i, (a, b) in enumerate(((attended, attn_out), (conv, conv_out), (log_buf, log_out)))
    ]
    copies[0].start()
    copies[1].start()
    for i in range(2):
        log_buf[pl.ds(i * half, half), :] = logs[i]
    copies[2].start()
    for c in copies:
        c.wait()


def fused_device(
    tps,
    tokens,
    norm_gain,
    query_weight,
    key_weight,
    value_weight,
    outer_weight,
    inner_weight,
    signal_weight,
    conv_taps,
    sink_logit,
):
    rows, width = tokens.shape[1:]
    depth, local = query_weight.shape
    qcols = local // 2
    heads = qcols // HEAD
    chans = outer_weight.shape[1] // 4
    head_local = 2 * heads
    group_cols = qcols + 2 * HEAD
    pad = 16
    bf, f32 = jnp.bfloat16, jnp.float32
    dma = pltpu.SemaphoreType.DMA
    hbm = pl.BlockSpec(memory_space=pltpu.HBM)
    anyspace = pl.BlockSpec(memory_space=pl.ANY)
    attended, conv, logs = pl.pallas_call(
        functools.partial(mega_kernel, tps),
        out_shape=(
            jax.ShapeDtypeStruct((rows, local), bf),
            jax.ShapeDtypeStruct((rows, 4 * chans), bf),
            jax.ShapeDtypeStruct((2, heads, rows), f32),
        ),
        in_specs=[hbm] * 10,
        out_specs=(anyspace, anyspace, anyspace),
        scratch_shapes=[
            pltpu.VMEM((4, rows, width), bf),
            pltpu.VMEM((GROUPS, width, group_cols), bf),
            pltpu.VMEM((GROUPS, depth, group_cols), bf),
            pltpu.VMEM((2, rows, qcols), bf),
            pltpu.VMEM((2, rows + 2 * WINDOW, 2 * HEAD), bf),
            pltpu.VMEM((3 * WINDOW, heads * WINDOW), f32),
            pltpu.VMEM((1, heads * WINDOW), f32),
            pltpu.VMEM((2, 2, 2 * rows + 2 * pad, chans), bf),
            pltpu.VMEM((2, 2, 2 * rows, chans), bf),
            pltpu.VMEM((2, rows, qcols), bf),
            pltpu.VMEM((2, heads, rows), f32),
            pltpu.VMEM((2, 2, 2 * rows, chans), bf),
            pltpu.VMEM((10, rows, group_cols), f32),
            pltpu.VMEM((2, depth, 2 * HEAD), bf),
            pltpu.VMEM((width // 128, 128), f32),
            pltpu.VMEM((1, width), f32),
            pltpu.VMEM((3, 4 * chans), f32),
            pltpu.SMEM((head_local,), f32),
            dma((5,)),
            dma((GROUPS,)),
            dma((GROUPS,)),
            dma((3,)),
            dma((2,)),
            dma((GROUPS,)),
            dma((GROUPS, 2 * SPAN)),
            dma((1,)),
            dma((GROUPS,)),
            dma((2,)),
            dma((1,)),
            dma((3,)),
            dma((3, SUBS, 2)),
            dma((7,)),
            dma((2, 2)),
            dma((2, 2)),
            dma((2, 2)),
            dma((2, 2)),
            dma((2,)),
            dma((2,)),
            dma((2, 5)),
            dma((2, 4)),
        ],
        compiler_params=pltpu.CompilerParams(
            collective_id=0, has_side_effects=True, vmem_limit_bytes=48 << 20
        ),
    )(
        *(
            pltpu.with_memory_space_constraint(x, pltpu.HBM)
            for x in (
                tokens[0],
                norm_gain.reshape(width // 128, 128),
                query_weight,
                key_weight,
                value_weight,
                outer_weight,
                inner_weight,
                signal_weight,
                conv_taps,
                sink_logit,
            )
        )
    )
    vmem = pl.BlockSpec(memory_space=pltpu.VMEM)
    attended, conv, logs = pl.pallas_call(
        deliver,
        out_shape=(
            jax.ShapeDtypeStruct((rows, local), bf),
            jax.ShapeDtypeStruct((rows, 4 * chans), bf),
            jax.ShapeDtypeStruct((head_local, rows), f32),
        ),
        in_specs=[vmem] * 3,
        out_specs=(hbm, hbm, hbm),
        scratch_shapes=[pltpu.VMEM((head_local, rows), f32), dma((3,))],
        compiler_params=pltpu.CompilerParams(vmem_limit_bytes=8 << 20),
    )(attended, conv, logs)
    return (attended[None], conv[None], logs[None])


def fits(mesh, args):
    tokens, query_weight, key_weight, outer_weight = (args[i] for i in (0, 2, 3, 5))
    sp, fs, tp = (mesh.shape[a] for a in ("sp", "fs", "tp"))
    rows = tokens.shape[1] // sp
    return (
        fs == 2
        and sp == SPAN
        and tokens.shape[0] == fs
        and tp == 4
        and rows % (2 * WINDOW) == 0
        and rows // WINDOW % 2 == 0
        and rows % (16 * SUBS * tp) == 0
        and key_weight.shape[1] == 2 * HEAD * tp
        and query_weight.shape[1] % (256 * tp) == 0
        and outer_weight.shape[1] == 512 * tp
        and query_weight.shape[1] == 512 * tp
        and query_weight.shape[0] % (16 * sp * fs) == 0
    )


def solution(mesh):
    in_specs = (
        P("fs", "sp", None),
        P(),
        P(("sp", "fs"), "tp"),
        P(("sp", "fs"), "tp"),
        P(("sp", "fs"), "tp"),
        P(("sp", "fs"), "tp"),
        P(("sp", "fs"), "tp"),
        P(("sp", "fs"), "tp"),
        P(None, "tp"),
        P("tp"),
    )
    out_specs = (P("fs", "sp", "tp"), P("fs", "sp", "tp"), P("fs", "tp", "sp"))

    def run(*args):
        body = per_device
        if fits(mesh, args):
            body = functools.partial(fused_device, mesh.shape["tp"])
        return jax.shard_map(
            body, mesh=mesh, in_specs=in_specs, out_specs=out_specs, check_vma=False
        )(*args)

    return run
```

```python
import math

import functools

import jax
import jax.numpy as jnp
from jax import lax
from jax.experimental import pallas as pl
from jax.experimental.pallas import tpu as pltpu
from jax.sharding import PartitionSpec as P

HEAD = 64
WINDOW = 128


EPSILON = 1e-06


def extended(value, sides, width):
    for axis, dim in sides:
        size, length = (lax.axis_size(axis), value.shape[dim])
        up = [(i, (i + 1) % size) for i in range(size - 1)]
        down = [(j, i) for i, j in up]
        last = lax.slice_in_dim(value, length - width, length, axis=dim)
        initial = lax.slice_in_dim(value, 0, width, axis=dim)
        before = lax.ppermute(last, axis, up)
        after = lax.ppermute(initial, axis, down)
        value = jnp.concatenate([before, value, after], axis=dim)
    return value


def normalized(tokens, norm_gain):
    values = tokens.astype(jnp.float32)
    scaling = lax.rsqrt(jnp.mean(values * values, axis=-1, keepdims=True) + EPSILON)
    return (values * scaling * norm_gain).astype(jnp.bfloat16)


def folding(normed):

    def add_portions(running, portions, offset):
        return tuple(
            (jnp.dot(normed, portion, preferred_element_type=jnp.float32) for portion in portions)
        )

    return add_portions


def empty_sums(normed, weights):
    return tuple((jnp.zeros((normed.shape[0], weight.shape[1]), jnp.float32) for weight in weights))


def rounded(results):
    return tuple((result.astype(jnp.bfloat16) for result in results))


def gate_product(inner_gate, signal):
    return (inner_gate.astype(jnp.float32) * signal.astype(jnp.float32)).astype(jnp.bfloat16)


def send_edges(key_proj, value_proj, product):
    stacked = jnp.concatenate([key_proj, value_proj], axis=1)
    window_rows = extended(stacked, (("sp", 0),), WINDOW)
    conv_rows = extended(product, (("sp", 0),), 1)
    return (window_rows, conv_rows)


def banded_attention(queries, window_rows, sink_logit, slopes, first_pos, seq_length):
    tok_count = queries.shape[0]
    kv_cols = window_rows.shape[1] // 2
    kv_heads = kv_cols // HEAD
    group_size = queries.shape[1] // (HEAD * kv_heads)
    block_count = tok_count // WINDOW
    query_blocks = queries.reshape(block_count, WINDOW, kv_heads, group_size, HEAD)
    key_rows = window_rows[:, :kv_cols].reshape(block_count + 2, WINDOW, kv_heads, HEAD)
    value_rows = window_rows[:, kv_cols:].reshape(block_count + 2, WINDOW, kv_heads, HEAD)
    key_span = jnp.concatenate([key_rows[:-2], key_rows[1:-1], key_rows[2:]], axis=1)
    value_span = jnp.concatenate([value_rows[:-2], value_rows[1:-1], value_rows[2:]], axis=1)
    scores = jnp.einsum(
        "bqkgd,bskd->bkgqs", query_blocks, key_span, preferred_element_type=jnp.float32
    ) * (1.0 / math.sqrt(HEAD))
    distance = jnp.arange(WINDOW)[:, None] - jnp.arange(3 * WINDOW)[None, :] + WINDOW
    key_pos = (
        first_pos
        - WINDOW
        + WINDOW * jnp.arange(block_count)[:, None]
        + jnp.arange(3 * WINDOW)[None, :]
    )
    inside = (jnp.abs(distance)[None] <= WINDOW) & ((key_pos >= 0) & (key_pos < seq_length))[
        :, None, :
    ]
    scores = scores - slopes.reshape(kv_heads, group_size, 1, 1) * jnp.abs(distance).astype(
        jnp.float32
    )
    scores = jnp.where(inside[:, None, None], scores, -jnp.inf)
    sink_grid = sink_logit.reshape(kv_heads, group_size, 1, 1)
    row_peak = jnp.maximum(jnp.max(scores, axis=-1, keepdims=True), sink_grid)
    weights = jnp.exp(scores - row_peak)
    row_total = jnp.sum(weights, axis=-1, keepdims=True) + jnp.exp(sink_grid - row_peak)
    weighted = jnp.einsum(
        "bkgqs,bskd->bqkgd",
        weights.astype(jnp.bfloat16),
        value_span,
        preferred_element_type=jnp.float32,
    )
    attended = (
        (weighted / row_total.transpose(0, 3, 1, 2, 4))
        .astype(jnp.bfloat16)
        .reshape(tok_count, kv_heads * group_size * HEAD)
    )
    log_total = (
        (row_peak + jnp.log(row_total))[..., 0]
        .transpose(1, 2, 0, 3)
        .reshape(kv_heads * group_size, tok_count)
    )
    return (attended, log_total)


def per_device(
    tokens,
    norm_gain,
    query_weight,
    key_weight,
    value_weight,
    outer_weight,
    inner_weight,
    signal_weight,
    conv_taps,
    sink_logit,
):
    normed = normalized(tokens[0], norm_gain)
    add_portions = folding(normed)
    all_sums = add_portions(
        empty_sums(
            normed,
            (query_weight, key_weight, value_weight, outer_weight, inner_weight, signal_weight),
        ),
        (
            lax.all_gather(query_weight, ("sp", "fs"), axis=0, tiled=True),
            lax.all_gather(key_weight, ("sp", "fs"), axis=0, tiled=True),
            lax.all_gather(value_weight, ("sp", "fs"), axis=0, tiled=True),
            lax.all_gather(outer_weight, ("sp", "fs"), axis=0, tiled=True),
            lax.all_gather(inner_weight, ("sp", "fs"), axis=0, tiled=True),
            lax.all_gather(signal_weight, ("sp", "fs"), axis=0, tiled=True),
        ),
        jnp.int32(0),
    )
    queries, key_proj, value_proj, outer_gate, inner_gate, signal = rounded(all_sums)
    product = gate_product(inner_gate, signal)
    window_rows, conv_rows = send_edges(key_proj, value_proj, product)
    tok_count = normed.shape[0]
    head_local = queries.shape[1] // HEAD
    head_index = lax.axis_index("tp") * head_local + jnp.arange(1, head_local + 1)
    slopes = jnp.exp2(-8.0 * head_index.astype(jnp.float32) / (head_local * lax.axis_size("tp")))
    first_pos = lax.axis_index("sp") * tok_count
    attended, log_total = banded_attention(
        queries, window_rows, sink_logit, slopes, first_pos, tok_count * lax.axis_size("sp")
    )
    mixed_conv = conv_taps[0] * conv_rows[0:tok_count].astype(jnp.float32)
    mixed_conv = mixed_conv + conv_taps[1] * conv_rows[1 : tok_count + 1].astype(jnp.float32)
    mixed_conv = mixed_conv + conv_taps[2] * conv_rows[2 : tok_count + 2].astype(jnp.float32)
    conv_out = (outer_gate.astype(jnp.float32) * mixed_conv).astype(jnp.bfloat16)
    return (attended[None], conv_out[None], log_total[None])


MESH = pl.DeviceIdType.MESH
GROUPS = 3
SPAN = 4
SUBS = 4
Y_PAIRS = 1
Z_FIRST = 3
FAR = -1e30


def mega_kernel(
    tps,
    tokens,
    gain_in,
    qw,
    kw,
    vw,
    ow,
    iw,
    sw,
    taps_in,
    sinks_in,
    attn_out,
    conv_out,
    log_out,
    toks,
    wts,
    stage_w,
    qs,
    kvs,
    bias,
    sink_row,
    prod,
    outer,
    attn_st,
    log_st,
    conv_st,
    acc,
    kv_raw,
    gain_raw,
    gain,
    taps,
    sinks,
    small_sem,
    load_sem,
    stage_sem,
    misc_sem,
    own_sem,
    y_send,
    w_recv,
    pair_send,
    mid_send,
    tok_y_send,
    tok_z_send,
    tok_t_send,
    tok_recv,
    tok_have,
    kv_send,
    kv_recv,
    pr_send,
    pr_recv,
    ret_send,
    ret_recv,
    conv_send,
    conv_recv,
):
    s, f, t = lax.axis_index("sp"), lax.axis_index("fs"), lax.axis_index("tp")
    other = 1 - f
    core = lax.rem(t, 2)
    outward = 1 - lax.rem(s, 2)
    partner = s + 2 * outward - 1
    facing = SPAN - 1 - s
    far = SPAN - 1 - partner
    is_mid = (s == 1) | (s == SPAN - 2)
    is_end = jnp.logical_not(is_mid)
    low_half = s < SPAN // 2
    pair, diag, mid = (partner, f, t), (partner, other, t), (facing, f, t)
    across = (s, other, t)
    mate_t, beyond_t = t + 1 - 2 * core, lax.rem(t + 2, tps)
    mate, beyond = (s, f, mate_t), (s, f, beyond_t)
    rows = tokens.shape[0]
    depth = qw.shape[0]
    qcols = qs.shape[2]
    heads = qcols // HEAD
    chans = prod.shape[3]
    both_rows = outer.shape[2]
    blocks = rows // WINDOW
    pad = (prod.shape[2] - both_rows) // 2
    sub = rows // SUBS
    part = sub // tps
    up, down = (s + 1, f, t), (s - 1, f, t)
    has_up, has_down = s < SPAN - 1, s > 0
    own_off = jnp.where(low_half, rows, 0)
    end_off = rows - own_off

    barrier = pltpu.get_barrier_semaphore()
    for peer in (pair, diag, across, mate, beyond):
        pl.semaphore_signal(barrier, inc=1, device_id=peer, device_id_type=MESH)

    @pl.when(is_mid)
    def _():
        pl.semaphore_signal(barrier, inc=1, device_id=mid, device_id_type=MESH)

    def block_rows(blk):
        return pl.ds(pl.multiple_of(blk * depth, 16), depth)

    def loads(g, half, dest, sems):
        if g == 0:
            qc = pl.ds(pl.multiple_of(half * qcols, 128), qcols)
            pairs = [(qw.at[:, qc], dest.at[:, pl.ds(0, qcols)])]
        else:
            c = pl.ds(pl.multiple_of(half * (2 * chans) + (g - 1) * chans, 128), chans)
            pairs = [
                (ref.at[:, c], dest.at[:, pl.ds(i * chans, chans)])
                for i, ref in enumerate((iw, sw, ow))
            ]
        return [pltpu.make_async_copy(a, b, sems.at[g]) for a, b in pairs]

    def loaded(g, dest, sems):
        whole = dest.at[:, pl.ds(0, qcols)] if g == 0 else dest
        pltpu.make_async_copy(whole, whole, sems.at[g]).wait()

    mine = s * 2 + f
    theirs = s * 2 + other
    own_dest = [wts.at[g, block_rows(mine)] for g in range(GROUPS)]
    own_loads = [loads(g, f, own_dest[g], load_sem) for g in range(GROUPS)]
    out_loads = [loads(g, other, stage_w.at[g], stage_sem) for g in range(GROUPS)]
    small = [
        pltpu.make_async_copy(a, b, small_sem.at[i])
        for i, (a, b) in enumerate(
            (
                (kw, kv_raw.at[0]),
                (vw, kv_raw.at[1]),
                (gain_in, gain_raw),
                (taps_in, taps),
                (sinks_in, sinks),
            )
        )
    ]
    tok_load = pltpu.make_async_copy(tokens, toks.at[f], misc_sem.at[0])

    def begin(copies):
        for c in copies:
            c.start()

    def finish(copies):
        for c in copies:
            c.wait()

    begin(small[:2] + out_loads[0] + own_loads[0] + small[2:])
    tok_load.start()
    begin(out_loads[1] + own_loads[1] + out_loads[2] + own_loads[2])

    def remote(src, dst, send, recv, peer):
        return pltpu.make_async_remote_copy(
            src_ref=src,
            dst_ref=dst,
            send_sem=send,
            recv_sem=recv,
            device_id=peer,
            device_id_type=MESH,
        )

    def arrive_sem(g, blk, crosses=False):
        if g == 0:
            return w_recv.at[blk]
        if crosses:
            return w_recv.at[4 * SPAN + g - 1]
        return w_recv.at[2 * SPAN + SPAN * (g - 1) + lax.rem(blk, SPAN)]

    def y_copy(g):
        return remote(
            stage_w.at[g], wts.at[g, block_rows(mine)], y_send.at[0], arrive_sem(g, mine), across
        )

    def block_copy(g, blk, send, peer, crosses=False):
        at = wts.at[g, block_rows(blk)]
        return remote(at, at, send, arrive_sem(g, blk, crosses), peer)

    def to_pair(g, blk):
        return block_copy(g, blk, pair_send.at[0], pair)

    def to_mid(g, blk):
        return block_copy(g, blk, mid_send.at[0], mid, True)

    def blocks_sent(send, count):
        at = wts.at[0, pl.ds(0, count * depth)]
        remote(at, at, send, w_recv.at[0], across).wait_send()

    def arrived(g, blk):
        to_pair(g, blk).wait_recv()

    def far_arrived(g):
        at = wts.at[g, pl.ds(0, SPAN * depth)]
        remote(at, at, mid_send.at[0], arrive_sem(g, 0, True), mid).wait_recv()

    def slot_of(k):
        return (other, 2 + f, 2 + other)[k]

    def piece(slot, j, q):
        place = jnp.where(low_half, SUBS - 1 - j, j)
        return toks.at[slot, pl.ds(pl.multiple_of(place * sub + q * part, 16), part)]

    def tok_y(k, j):
        slot = f if k == 0 else 2 + f
        at = piece(slot, j, beyond_t if k == 2 else t)
        return remote(
            at, at, tok_y_send.at[1 if k else 0], tok_recv.at[2 if k else 0, j, k // 2], across
        )

    def tok_z(k, j):
        seq = f if k == 0 else other
        return remote(
            piece(seq, j, t), piece(2 + seq, j, t), tok_z_send.at[0], tok_recv.at[1 + k, j, 0], pair
        )

    def have_slot(k, j):
        if k < 2:
            return 2 * k + j // (SUBS // 2)
        return 4 + max(0, j - 1)

    def tok_share(k, j, kind):
        at = piece(slot_of(k), j, beyond_t if kind == 2 else t)
        if kind == 1:
            return remote(at, at, tok_t_send.at[k], tok_recv.at[k, j, 1], beyond)
        return remote(at, at, tok_t_send.at[k], tok_have.at[have_slot(k, j)], mate)

    def tok_wait(k, j, kind):
        at = piece(slot_of(k), j, t)
        remote(at, at, tok_t_send.at[k], tok_recv.at[k, j, kind], mate).wait_recv()

    def take(k, j):
        tok_wait(k, j, 0)
        if k < 2 or j >= Y_PAIRS:
            tok_share(k, j, 1).start()
        tok_share(k, j, 0).start()
        if k == 1 and j < Z_FIRST:
            tok_y(1, j).start()

    def hand(k, j):
        tok_wait(k, j, 1)
        tok_share(k, j, 2).start()

    def have(index, pieces):
        at = toks.at[0, pl.ds(0, pieces * part)]
        remote(at, at, tok_t_send.at[0], tok_have.at[index], mate).wait_recv()

    def pieces_sent(send, pieces):
        at = toks.at[0, pl.ds(0, pieces * part)]
        remote(at, at, send, tok_have.at[0], mate).wait_send()

    def norm_own():
        @pl.loop(0, blocks)
        def _(b):
            at = pl.ds(pl.multiple_of(b * WINDOW, WINDOW), WINDOW)
            values = toks[f, at, :].astype(jnp.float32)
            scaling = lax.rsqrt(jnp.mean(values * values, axis=-1, keepdims=True) + EPSILON)
            toks[f, at, :] = (values * scaling * gain[...]).astype(jnp.bfloat16)

    mm_rows = rows // 2

    def make_bias():
        key = lax.broadcasted_iota(jnp.int32, (3 * WINDOW, WINDOW), 0)
        query = lax.broadcasted_iota(jnp.int32, (3 * WINDOW, WINDOW), 1)
        away = jnp.abs(query - key + WINDOW)
        for h in range(heads):
            index = (t * (2 * heads) + f * heads + h + 1).astype(jnp.float32)
            slope = jnp.exp2(jnp.full((1, WINDOW), -8.0 / (2 * heads * tps), jnp.float32) * index)
            cols = pl.ds(h * WINDOW, WINDOW)
            bias[:, cols] = jnp.where(away <= WINDOW, -slope * away.astype(jnp.float32), FAR)
            sink_row[:, cols] = jnp.full((1, WINDOW), sinks[f * heads + h], jnp.float32)

    scale = 1.0 / math.sqrt(HEAD)
    half_k = depth * SPAN
    near_k = pl.multiple_of(jnp.where(low_half, 0, half_k), 128)
    far_k = pl.multiple_of(half_k - near_k, 128)

    def partial(g, slot, at, k_off):
        return jnp.dot(
            toks[slot, pl.ds(at, mm_rows), pl.ds(k_off, half_k)],
            wts[g, pl.ds(k_off, half_k), :],
            preferred_element_type=jnp.float32,
        )

    def sums(g, slot):
        return slot if g == 0 else slot + 4 * g - 2

    def halves_of(b):
        if b is None:
            return lambda body: [body(i) for i in range(2)]
        return lambda body: body(b)

    def near(g, slot, only=None):
        @halves_of(only)
        def _(b):
            at = pl.multiple_of(b * mm_rows, WINDOW)
            acc[sums(g, slot), pl.ds(at, mm_rows), :] = partial(g, slot, at, near_k)

    def total(g, slot, at):
        return acc[sums(g, slot), pl.ds(at, mm_rows), :] + partial(g, slot, at, far_k)

    def project_qkv(seq):
        @pl.loop(0, 2)
        def _(b):
            at = pl.multiple_of(b * mm_rows, WINDOW)
            out = total(0, seq, at)
            qs[seq, pl.ds(at, mm_rows), :] = (out[:, :qcols] * scale).astype(jnp.bfloat16)
            kvs[seq, pl.ds(at + WINDOW, mm_rows), :] = out[:, qcols:].astype(jnp.bfloat16)

    kv_len = kvs.shape[1]

    def kv_copies(seq, slot):
        ref = kvs.at[seq]
        climb = remote(
            ref.at[pl.ds(kv_len - 2 * WINDOW, WINDOW)],
            ref.at[pl.ds(0, WINDOW)],
            kv_send.at[slot, 0],
            kv_recv.at[slot, 0],
            up,
        )
        fall = remote(
            ref.at[pl.ds(WINDOW, WINDOW)],
            ref.at[pl.ds(kv_len - WINDOW, WINDOW)],
            kv_send.at[slot, 1],
            kv_recv.at[slot, 1],
            down,
        )
        return climb, fall

    def kv_start(seq, slot):
        climb, fall = kv_copies(seq, slot)
        blank = jnp.zeros((WINDOW, 2 * HEAD), jnp.bfloat16)

        @pl.when(has_up)
        def _():
            climb.start()

        @pl.when(has_down)
        def _():
            fall.start()

        @pl.when(jnp.logical_not(has_up))
        def _():
            kvs[seq, pl.ds(kv_len - WINDOW, WINDOW), :] = blank

        @pl.when(jnp.logical_not(has_down))
        def _():
            kvs[seq, pl.ds(0, WINDOW), :] = blank

    def kv_wait(seq, slot):
        climb, fall = kv_copies(seq, slot)

        @pl.when(has_up)
        def _():
            climb.wait_send()
            fall.wait_recv()

        @pl.when(has_down)
        def _():
            fall.wait_send()
            climb.wait_recv()

    def attend(seq, first, count, step=1, closed=False):
        def block(i):
            b = first + i * step
            at = pl.multiple_of(b * WINDOW, WINDOW)
            kv = kvs[seq, pl.ds(at, 3 * WINDOW), :]
            keys = kv[:, :HEAD]
            values_t = kv.astype(jnp.float32).T[HEAD:, :].astype(jnp.bfloat16)
            queries = qs[seq, pl.ds(at, WINDOW), :]
            stacked = jnp.concatenate(
                [queries[:, h * HEAD : (h + 1) * HEAD] for h in range(heads)], axis=0
            )
            scores = lax.dot_general(
                keys, stacked, (((1,), (1,)), ((), ())), preferred_element_type=jnp.float32
            )
            scores = scores + bias[...]
            if closed:
                low = jnp.where((b == 0) & (s == 0), FAR, 0.0)
                high = jnp.where((b == blocks - 1) & (s == SPAN - 1), FAR, 0.0)
                scores = jnp.concatenate(
                    [
                        scores[:WINDOW] + low,
                        scores[WINDOW : 2 * WINDOW],
                        scores[2 * WINDOW :] + high,
                    ],
                    axis=0,
                )
            sink = sink_row[...]
            peak = jnp.maximum(jnp.max(scores, axis=0, keepdims=True), sink)
            weights = jnp.exp(scores - peak)
            total = jnp.sum(weights, axis=0, keepdims=True) + jnp.exp(sink - peak)
            mixed = jnp.dot(
                values_t, weights.astype(jnp.bfloat16), preferred_element_type=jnp.float32
            )
            mixed = mixed / total
            logs = peak + jnp.log(total)
            outs = []
            for h in range(heads):
                cols = slice(h * WINDOW, (h + 1) * WINDOW)
                outs.append(mixed[:, cols])
                log_st[seq, pl.ds(h, 1), pl.ds(at, WINDOW)] = logs[:, cols]
            attn_st[seq, pl.ds(at, WINDOW), :] = (
                jnp.concatenate(outs, axis=0).T.astype(jnp.bfloat16)
            )

        @pl.loop(0, count // 2)
        def _(i):
            block(2 * i)
            block(2 * i + 1)

    half_cols = pl.ds(pl.multiple_of(f * qcols, 128), qcols)

    def attn_return(own):
        seq = f if own else other
        pairs = [
            (attn_st.at[seq], attn_out.at[:, half_cols]),
            (log_st.at[seq], log_out.at[f]),
        ]
        if own:
            return [pltpu.make_async_copy(a, b, misc_sem.at[1 + i]) for i, (a, b) in enumerate(pairs)]
        return [
            remote(a, b, ret_send.at[i], ret_recv.at[i], across) for i, (a, b) in enumerate(pairs)
        ]

    def conv_cols(g):
        return pl.ds(pl.multiple_of(f * (2 * chans) + (g - 1) * chans, 128), chans)

    split = mm_rows - pad
    head_b = jnp.where(low_half, 1, 0)
    spans = {
        None: (0, rows),
        "head": (jnp.where(low_half, rows - split, 0), split),
        "tail": (jnp.where(low_half, 0, split), rows - split),
        "far": (jnp.where(low_half, 0, rows - split), split),
        "rest": (jnp.where(low_half, split, 0), rows - split),
    }

    def conv_return(g, own_seq, own_rows, span=None):
        seq = f if own_seq else other
        off = own_off if own_rows else end_off
        lo, count = spans[span]
        src = conv_st.at[g - 1, seq, pl.ds(pl.multiple_of(off + lo, pad), count)]
        dst = conv_out.at[pl.ds(pl.multiple_of(lo, pad), count), conv_cols(g)]
        if own_seq and own_rows:
            return pltpu.make_async_copy(src, dst, own_sem.at[g - 1])
        if own_seq:
            last = 3 if span == "rest" else 0
            return remote(src, dst, conv_send.at[g - 1], conv_recv.at[g - 1, last], pair)
        if own_rows:
            return remote(src, dst, conv_send.at[g - 1], conv_recv.at[g - 1, 1], across)
        last = 1 if span == "tail" else 0
        return remote(
            src, dst, conv_send.at[g - 1], conv_recv.at[g - 1, 1 + last], diag
        )

    def project_conv(g, seq, own_rows, only=None):
        slot, off = (seq, own_off) if own_rows else (2 + seq, end_off)

        @halves_of(only)
        def _(b):
            at = pl.multiple_of(b * mm_rows, WINDOW)
            to = pl.multiple_of(off + b * mm_rows, WINDOW)
            out = total(g, slot, at)
            inner = out[:, :chans].astype(jnp.bfloat16).astype(jnp.float32)
            signal = out[:, chans : 2 * chans].astype(jnp.bfloat16).astype(jnp.float32)
            prod[g - 1, seq, pl.ds(to + pad, mm_rows), :] = (inner * signal).astype(jnp.bfloat16)
            outer[g - 1, seq, pl.ds(to, mm_rows), :] = out[:, 2 * chans :].astype(jnp.bfloat16)

    def project_tail(g, j):
        at = pl.multiple_of(jnp.where(low_half, SUBS - 1 - j, j) * sub, 16)
        out = jnp.dot(
            toks[2 + other, pl.ds(at, sub), :], wts[g], preferred_element_type=jnp.float32
        )
        inner = out[:, :chans].astype(jnp.bfloat16).astype(jnp.float32)
        signal = out[:, chans : 2 * chans].astype(jnp.bfloat16).astype(jnp.float32)
        to = pl.multiple_of(end_off + at, 16)
        prod[g - 1, other, pl.ds(to + pad, sub), :] = (inner * signal).astype(jnp.bfloat16)
        outer[g - 1, other, pl.ds(to, sub), :] = out[:, 2 * chans :].astype(jnp.bfloat16)

    def pr_copies(g, seq, slot):
        ref = prod.at[g - 1, seq]
        climb = remote(
            ref.at[pl.ds(both_rows, pad)],
            ref.at[pl.ds(0, pad)],
            pr_send.at[g - 1, slot],
            pr_recv.at[g - 1, slot],
            mid,
        )
        fall = remote(
            ref.at[pl.ds(pad, pad)],
            ref.at[pl.ds(both_rows + pad, pad)],
            pr_send.at[g - 1, slot],
            pr_recv.at[g - 1, slot],
            mid,
        )
        return climb, fall

    def pr_blank():
        place = pl.multiple_of(jnp.where(low_half, 0, both_rows + pad), pad)
        blank = jnp.zeros((pad, chans), jnp.bfloat16)
        for g in range(2):
            for seq in range(2):
                prod[g, seq, pl.ds(place, pad), :] = blank

    def pr_start(g, seq, slot):
        climb, fall = pr_copies(g, seq, slot)

        @pl.when(low_half)
        def _():
            climb.start()

        @pl.when(jnp.logical_not(low_half))
        def _():
            fall.start()

    def pr_wait(g, seq, slot):
        climb, fall = pr_copies(g, seq, slot)

        @pl.when(low_half)
        def _():
            climb.wait_send()
            fall.wait_recv()

        @pl.when(jnp.logical_not(low_half))
        def _():
            fall.wait_send()
            climb.wait_recv()

    def mix(g, seq, own_rows, span=None):
        lo, count = spans[span]
        off = pl.multiple_of((own_off if own_rows else end_off) + lo, pad)
        tap = taps[:, conv_cols(g)]
        size = count + 2 * pad
        full = prod[g - 1, seq, pl.ds(off, size), :].astype(jnp.float32)
        before = pltpu.roll(full, 1, 0)[pad : pad + count]
        after = pltpu.roll(full, size - 1, 0)[pad : pad + count]
        mixed = tap[0:1] * before + tap[1:2] * full[pad : pad + count] + tap[2:3] * after
        gate = outer[g - 1, seq, pl.ds(off, count), :].astype(jnp.float32)
        conv_st[g - 1, seq, pl.ds(off, count), :] = (gate * mixed).astype(jnp.bfloat16)

    finish(small[:2])
    keys0, vals0 = kv_raw[0], kv_raw[1]
    halves = [
        jnp.concatenate([w[:, i * HEAD : (i + 1) * HEAD] for w in (keys0, vals0)], axis=1)
        for i in range(2)
    ]
    first = f == 0
    stage_w[0, :, pl.ds(qcols, 2 * HEAD)] = jnp.where(first, halves[1], halves[0])
    wts[0, block_rows(mine), pl.ds(qcols, 2 * HEAD)] = jnp.where(first, halves[0], halves[1])

    pl.semaphore_wait(barrier, jnp.where(is_mid, 6, 5))

    loaded(0, own_dest[0], load_sem)
    to_pair(0, mine).start()

    @pl.when(is_mid)
    def _():
        to_mid(0, mine).start()

    loaded(0, stage_w.at[0], stage_sem)
    loaded(1, stage_w.at[1], stage_sem)

    @pl.when(is_end)
    def _():
        y_copy(0).start()
        y_copy(1).start()

    loaded(1, own_dest[1], load_sem)

    @pl.when(is_mid)
    def _():
        to_mid(1, mine).start()

    finish(small[2:])
    for i in range(gain_raw.shape[0]):
        gain[:, i * 128 : (i + 1) * 128] = gain_raw[i : i + 1, :]
    tok_load.wait()
    norm_own()
    tok_y(0, 0).start()

    @pl.when(is_mid)
    def _():
        y_copy(0).start()

    for j in range(1, SUBS):
        tok_y(0, j).start()

    @pl.when(is_mid)
    def _():
        y_copy(1).start()

    loaded(2, stage_w.at[2], stage_sem)
    y_copy(2).start()
    loaded(2, own_dest[2], load_sem)

    def relay(g, blk, onward):
        arrived(g, blk)
        onward(g, blk).start()

    pt = [partner * 2 + f, partner * 2 + other]
    ct = [facing * 2 + f, facing * 2 + other]
    ft = [far * 2 + f, far * 2 + other]

    def end_program():
        tok_z(0, 0).start()
        make_bias()
        relay(0, theirs, to_pair)
        to_pair(1, mine).start()
        relay(1, theirs, to_pair)
        for j in range(1, SUBS):
            tok_z(0, j).start()
        take(0, 0)
        for blk in pt:
            arrived(0, blk)
        near(0, f)
        take(0, 1)
        hand(0, 0)
        take(0, 2)
        hand(0, 1)
        take(0, 3)
        hand(0, 2)
        have(0, 2 * (SUBS // 2))
        near(0, other, head_b)
        for blk in ct + ft:
            arrived(0, blk)
        project_qkv(f)
        kv_start(f, 0)
        to_pair(2, mine).start()
        hand(0, 3)
        have(1, 2 * (SUBS // 2))
        near(0, other, 1 - head_b)
        project_qkv(other)
        kv_start(other, 1)
        relay(2, theirs, to_pair)
        for j in range(Z_FIRST, SUBS):
            tok_z(1, j).start()
        attend(f, 1, blocks - 2)
        attend(other, 1, blocks - 2)
        kv_wait(f, 0)
        attend(f, 0, 2, blocks - 1, True)
        begin(attn_return(True))
        kv_wait(other, 1)
        attend(other, 0, 2, blocks - 1, True)
        begin(attn_return(False))
        for g in (1, 2):
            for span in (None,) if g == 1 else ("far", "rest"):
                conv_return(g, True, False, span).wait_recv()
            conv_return(g, False, False, "head").wait_recv()
            conv_return(g, False, False, "tail").wait_recv()
        blocks_sent(pair_send.at[0], 2 * GROUPS)
        pieces_sent(tok_z_send.at[0], 2 * SUBS - Z_FIRST)

    def conv_own(g, own_seq):
        seq, slot = (f, 0) if own_seq else (other, 1)
        project_conv(g, seq, True)
        pr_start(g, seq, slot)

    def conv_close(g, own_seq):
        seq, slot = (f, 0) if own_seq else (other, 1)
        pr_wait(g, seq, slot)
        mix(g, seq, True)
        conv_return(g, own_seq, True).start()

    def conv_close_end(g):
        mix(g, f, False)
        conv_return(g, True, False).start()

    def conv_end_close(g, span):
        mix(g, other, False, span)
        conv_return(g, False, False, span).start()

    def mid_program():
        half = (blocks - 2) // 2
        make_bias()
        pr_blank()
        relay(0, ct[0], to_pair)
        relay(0, pt[0], to_mid)
        take(0, 0)
        take(1, 0)
        relay(0, theirs, to_mid)
        to_pair(0, theirs).start()
        relay(0, pt[1], to_mid)
        near(0, f)
        take(0, 1)
        hand(0, 0)
        relay(0, ct[1], to_pair)
        relay(1, pt[0], to_mid)
        take(0, 2)
        relay(0, ft[0], to_pair)
        hand(0, 1)
        have(0, 2 * (SUBS // 2))
        near(0, other, head_b)
        hand(1, 0)
        relay(0, ft[1], to_pair)
        take(0, 3)
        relay(1, pt[1], to_mid)
        project_qkv(f)
        kv_start(f, 0)
        attend(f, 1, half)
        attend(f, 1 + half, half)
        take(1, 1)
        hand(0, 2)
        relay(1, theirs, to_mid)
        to_mid(2, mine).start()
        near(1, f)
        hand(0, 3)
        have(1, 2 * (SUBS // 2))
        near(0, other, 1 - head_b)
        project_qkv(other)
        kv_start(other, 1)
        take(1, 2)
        tok_y(2, 0).start()
        attend(other, 1, half)
        attend(other, 1 + half, half)
        near(1, other)
        relay(2, theirs, to_mid)
        take(1, 3)
        far_arrived(1)
        conv_own(1, True)
        conv_own(1, False)
        kv_wait(f, 0)
        attend(f, 0, 2, blocks - 1)
        begin(attn_return(True))
        hand(1, 1)
        have(2, 2 * (SUBS // 2))
        near(1, 2 + f, head_b)
        relay(2, pt[0], to_mid)
        take(2, 0)
        take(2, 1)
        project_conv(1, f, False, head_b)
        kv_wait(other, 1)
        attend(other, 0, 2, blocks - 1)
        begin(attn_return(False))
        hand(1, 2)
        hand(1, 3)
        have(3, 2 * (SUBS // 2))
        near(1, 2 + f, 1 - head_b)
        relay(2, pt[1], to_mid)
        take(2, 2)
        project_conv(1, f, False, 1 - head_b)
        conv_close_end(1)
        near(2, f)
        near(2, other)
        take(2, 3)
        near(2, 2 + f)
        hand(2, 0)
        conv_close(1, True)
        hand(2, 1)
        have(4, 4)
        near(1, 2 + other, head_b)
        project_conv(1, other, False, head_b)
        conv_end_close(1, "head")
        conv_close(1, False)
        near(2, 2 + other, head_b)
        far_arrived(2)
        project_conv(2, f, False, 1 - head_b)
        mix(2, f, False, "far")
        conv_return(2, True, False, "far").start()
        project_conv(2, f, True, 1 - head_b)
        project_conv(2, f, False, head_b)
        mix(2, f, False, "rest")
        conv_return(2, True, False, "rest").start()
        hand(2, 2)
        conv_own(2, False)
        project_conv(2, other, False, head_b)
        conv_end_close(2, "head")
        hand(2, 3)
        project_conv(2, f, True, head_b)
        pr_start(2, f, 0)
        have(5, 2)
        project_tail(1, 2)
        have(6, 2)
        project_tail(1, 3)
        conv_end_close(1, "tail")
        conv_close(2, False)
        project_tail(2, 2)
        project_tail(2, 3)
        conv_end_close(2, "tail")
        conv_close(2, True)
        for g in (1, 2):
            conv_return(g, False, True).wait_recv()
            conv_return(g, True, True).wait()
            sent = conv_st.at[0, :, pl.ds(0, 3 * rows // 2)]
            remote(sent, sent, conv_send.at[g - 1], conv_recv.at[g - 1, 1], across).wait_send()
            pieces_sent(tok_t_send.at[g], 3 * SUBS if g == 1 else 3 * SUBS - Y_PAIRS)
        blocks_sent(pair_send.at[0], 6)
        sent = wts.at[pl.ds(0, 2), pl.ds(0, 2 * GROUPS * depth)]
        remote(sent, sent, mid_send.at[0], w_recv.at[0], across).wait_send()
        pieces_sent(tok_y_send.at[1], Z_FIRST + Y_PAIRS)

    pl.when(is_end)(end_program)
    pl.when(is_mid)(mid_program)

    blocks_sent(y_send.at[0], GROUPS)
    pieces_sent(tok_y_send.at[0], SUBS)
    pieces_sent(tok_t_send.at[0], 3 * SUBS)
    for own in (True, False):
        finish(attn_return(own))


def deliver(attended, conv, logs, attn_out, conv_out, log_out, log_buf, sems):
    half = logs.shape[1]
    copies = [
        pltpu.make_async_copy(a, b, sems.at[i])
        for i, (a, b) in enumerate(((attended, attn_out), (conv, conv_out), (log_buf, log_out)))
    ]
    copies[0].start()
    copies[1].start()
    for i in range(2):
        log_buf[pl.ds(i * half, half), :] = logs[i]
    copies[2].start()
    for c in copies:
        c.wait()


def fused_device(
    tps,
    tokens,
    norm_gain,
    query_weight,
    key_weight,
    value_weight,
    outer_weight,
    inner_weight,
    signal_weight,
    conv_taps,
    sink_logit,
):
    rows, width = tokens.shape[1:]
    depth, local = query_weight.shape
    qcols = local // 2
    heads = qcols // HEAD
    chans = outer_weight.shape[1] // 4
    head_local = 2 * heads
    group_cols = qcols + 2 * HEAD
    pad = 16
    bf, f32 = jnp.bfloat16, jnp.float32
    dma = pltpu.SemaphoreType.DMA
    hbm = pl.BlockSpec(memory_space=pltpu.HBM)
    anyspace = pl.BlockSpec(memory_space=pl.ANY)
    attended, conv, logs = pl.pallas_call(
        functools.partial(mega_kernel, tps),
        out_shape=(
            jax.ShapeDtypeStruct((rows, local), bf),
            jax.ShapeDtypeStruct((rows, 4 * chans), bf),
            jax.ShapeDtypeStruct((2, heads, rows), f32),
        ),
        in_specs=[hbm] * 10,
        out_specs=(anyspace, anyspace, anyspace),
        scratch_shapes=[
            pltpu.VMEM((4, rows, width), bf),
            pltpu.VMEM((GROUPS, width, group_cols), bf),
            pltpu.VMEM((GROUPS, depth, group_cols), bf),
            pltpu.VMEM((2, rows, qcols), bf),
            pltpu.VMEM((2, rows + 2 * WINDOW, 2 * HEAD), bf),
            pltpu.VMEM((3 * WINDOW, heads * WINDOW), f32),
            pltpu.VMEM((1, heads * WINDOW), f32),
            pltpu.VMEM((2, 2, 2 * rows + 2 * pad, chans), bf),
            pltpu.VMEM((2, 2, 2 * rows, chans), bf),
            pltpu.VMEM((2, rows, qcols), bf),
            pltpu.VMEM((2, heads, rows), f32),
            pltpu.VMEM((2, 2, 2 * rows, chans), bf),
            pltpu.VMEM((10, rows, group_cols), f32),
            pltpu.VMEM((2, depth, 2 * HEAD), bf),
            pltpu.VMEM((width // 128, 128), f32),
            pltpu.VMEM((1, width), f32),
            pltpu.VMEM((3, 4 * chans), f32),
            pltpu.SMEM((head_local,), f32),
            dma((5,)),
            dma((GROUPS,)),
            dma((GROUPS,)),
            dma((3,)),
            dma((2,)),
            dma((1,)),
            dma((4 * SPAN + GROUPS - 1,)),
            dma((1,)),
            dma((1,)),
            dma((2,)),
            dma((1,)),
            dma((3,)),
            dma((3, SUBS, 2)),
            dma((7,)),
            dma((2, 2)),
            dma((2, 2)),
            dma((2, 2)),
            dma((2, 2)),
            dma((2,)),
            dma((2,)),
            dma((2,)),
            dma((2, 4)),
        ],
        compiler_params=pltpu.CompilerParams(
            collective_id=0, has_side_effects=True, vmem_limit_bytes=48 << 20
        ),
    )(
        *(
            pltpu.with_memory_space_constraint(x, pltpu.HBM)
            for x in (
                tokens[0],
                norm_gain.reshape(width // 128, 128),
                query_weight,
                key_weight,
                value_weight,
                outer_weight,
                inner_weight,
                signal_weight,
                conv_taps,
                sink_logit,
            )
        )
    )
    vmem = pl.BlockSpec(memory_space=pltpu.VMEM)
    attended, conv, logs = pl.pallas_call(
        deliver,
        out_shape=(
            jax.ShapeDtypeStruct((rows, local), bf),
            jax.ShapeDtypeStruct((rows, 4 * chans), bf),
            jax.ShapeDtypeStruct((head_local, rows), f32),
        ),
        in_specs=[vmem] * 3,
        out_specs=(hbm, hbm, hbm),
        scratch_shapes=[pltpu.VMEM((head_local, rows), f32), dma((3,))],
        compiler_params=pltpu.CompilerParams(vmem_limit_bytes=8 << 20),
    )(attended, conv, logs)
    return (attended[None], conv[None], logs[None])


def fits(mesh, args):
    tokens, query_weight, key_weight, outer_weight = (args[i] for i in (0, 2, 3, 5))
    sp, fs, tp = (mesh.shape[a] for a in ("sp", "fs", "tp"))
    rows = tokens.shape[1] // sp
    return (
        fs == 2
        and sp == SPAN
        and tokens.shape[0] == fs
        and tp == 4
        and rows % (2 * WINDOW) == 0
        and rows // WINDOW % 2 == 0
        and rows % (16 * SUBS * tp) == 0
        and key_weight.shape[1] == 2 * HEAD * tp
        and query_weight.shape[1] % (256 * tp) == 0
        and outer_weight.shape[1] == 512 * tp
        and query_weight.shape[1] == 512 * tp
        and query_weight.shape[0] % (16 * sp * fs) == 0
    )


def solution(mesh):
    in_specs = (
        P("fs", "sp", None),
        P(),
        P(("sp", "fs"), "tp"),
        P(("sp", "fs"), "tp"),
        P(("sp", "fs"), "tp"),
        P(("sp", "fs"), "tp"),
        P(("sp", "fs"), "tp"),
        P(("sp", "fs"), "tp"),
        P(None, "tp"),
        P("tp"),
    )
    out_specs = (P("fs", "sp", "tp"), P("fs", "sp", "tp"), P("fs", "tp", "sp"))

    def run(*args):
        body = per_device
        if fits(mesh, args):
            body = functools.partial(fused_device, mesh.shape["tp"])
        return jax.shard_map(
            body, mesh=mesh, in_specs=in_specs, out_specs=out_specs, check_vma=False
        )(*args)

    return run
```
